512 devices in a mesh: sp: 64 (over z, y), tp: 8 (over x, core).
Axes of the slice: x: 4, y: 4, z: 16, core: 2. Of those that a mesh axis runs over, the one named last changes fastest.
Arguments:
- hidden_in: bfloat16 [16384, 2048], P('sp', 'tp'), may hold values from -6 to 6
- w_query_rec: bfloat16 [2048, 2048], P('sp', 'tp'), may hold values from -0.125 to 0.125
- w_forget: bfloat16 [2048, 2048], P('sp', 'tp'), may hold values from -0.125 to 0.125
- w_input: bfloat16 [2048, 2048], P('sp', 'tp'), may hold values from -0.125 to 0.125
- forget_gap: float32 [2048], P('tp'), may hold values from 1e-05 to 0.08
- decay_extra: float32 [16384, 16], P('sp', 'tp'), may hold values from -0.75 to 0
- rec_gain: float32 [128], replicated, may hold values from 0.1 to 1.9
- w_q_down: bfloat16 [2048, 512], P(None, 'tp'), may hold values from -0.125 to 0.125
- w_kv_down: bfloat16 [2048, 256], P(None, 'tp'), may hold values from -0.125 to 0.125
- w_key_rope: bfloat16 [2048, 32], replicated, may hold values from -0.125 to 0.125
- q_gain: float32 [512], replicated, may hold values from 1.4 to 7
- kv_gain: float32 [256], replicated, may hold values from 1.4 to 7
- w_q_nope: bfloat16 [512, 1024], P(None, 'tp'), may hold values from -0.25 to 0.25
- w_q_rope: bfloat16 [512, 512], P(None, 'tp'), may hold values from -0.25 to 0.25
- w_k_up: bfloat16 [256, 1024], P(None, 'tp'), may hold values from -0.375 to 0.375
- w_v_up: bfloat16 [256, 1024], P(None, 'tp'), may hold values from -0.375 to 0.375
- w_out_rec: bfloat16 [2048, 2048], P('tp'), may hold values from -0.109375 to 0.109375
- w_out_att: bfloat16 [1024, 2048], P('tp'), may hold values from -0.109375 to 0.109375
Outputs:
- mixed_out: bfloat16 [16384, 2048], P(('sp', 'tp'))
The draws below stay inside these ranges and needn't reach their ends.
All inputs are finite; a program needn't handle non-finite values.
Results may differ from the reference program's by a relative error of at most 0.02.
The reference program's roundings to bfloat16 on the way count: a program that leaves them out, or rounds other values in their place, can miss the bound.
Values may be sent and summed in bfloat16 or wider, within the bound.
A program may use at most 128 MiB of HBM per device.

```python
import math
import jax
import jax.numpy as jnp
from jax import lax

D = 2048
RECURRENT_HEADS = 16
HG_KDIM = 128
HG_VDIM = 128
HG_BLOCK = 64
MLA_HEADS = 16
NOPE = 64
ROPE = 32
MLA_V = 64
Q_RANK = 512
KV_RANK = 256
TOK_DEV = 256
SEQUENCE_TOKENS = 16384


def draw_forget_gap(key, part):
    first_key, key_second_draw, key_third_draw = jax.random.split(jax.random.fold_in(key, 11), 3)
    fast_share = 0.5
    fast_heads = jax.random.uniform(first_key, (RECURRENT_HEADS, 1)) < fast_share
    slow_gap = jnp.exp(jax.random.uniform(key_second_draw, (RECURRENT_HEADS, HG_KDIM), jnp.float32, jnp.log(1e-05), jnp.log(0.0001)))
    fast_gap = jnp.exp(jax.random.uniform(key_third_draw, (RECURRENT_HEADS, HG_KDIM), jnp.float32, jnp.log(0.03), jnp.log(0.08)))
    return jnp.where(fast_heads, fast_gap, slow_gap).reshape(RECURRENT_HEADS * HG_KDIM).astype(jnp.float32)


def draw_decay_extra(key, part):
    first_key, key_second_draw, key_third_draw = jax.random.split(jax.random.fold_in(key, 23), 3)
    block_count = SEQUENCE_TOKENS // TOK_DEV
    forget_base_rate = jnp.exp(jax.random.uniform(first_key, (block_count, 1, RECURRENT_HEADS), jnp.float32, jnp.log(0.2), 0.0)) / SEQUENCE_TOKENS
    forget_base_rate = jnp.broadcast_to(forget_base_rate, (block_count, TOK_DEV, RECURRENT_HEADS)).reshape(SEQUENCE_TOKENS, RECURRENT_HEADS)
    spike_events = jax.random.uniform(key_second_draw, (SEQUENCE_TOKENS, RECURRENT_HEADS)) < 3.0 / SEQUENCE_TOKENS
    spike_depth = jax.random.uniform(key_third_draw, (SEQUENCE_TOKENS, RECURRENT_HEADS), jnp.float32, jnp.log(0.5), jnp.log(0.8))
    return (jnp.where(spike_events, spike_depth, 0.0) - forget_base_rate).astype(jnp.float32)


def draw_q_gain(key, part):
    values = jax.random.uniform(jax.random.fold_in(key, 31), (Q_RANK,), jnp.float32, 1.4, 2.6)
    return values.astype(jnp.float32)


def draw_kv_gain(key, part):
    values = jax.random.uniform(jax.random.fold_in(key, 37), (KV_RANK,), jnp.float32, 1.4, 2.6)
    return values.astype(jnp.float32)


def level_of(key, dims, shards, low, high):
    def one(dim, parts):
        heights = jax.random.uniform(jax.random.fold_in(jax.random.fold_in(key, 6), dim), (parts,), jnp.float32, low / len(shards), high / len(shards))
        return jnp.repeat(jnp.exp(heights), dims[dim] // parts).reshape((-1,) + (1,) * (len(dims) - dim - 1))

    loudness = one(*shards[0])
    for cut in shards[1:]:
        loudness = loudness * one(*cut)
    return loudness


def scatter_about(key, dims, deviation, bound, cuts=(), kind=jnp.bfloat16):
    drawn = deviation * jax.random.normal(key, dims, jnp.float32)
    if cuts:
        drawn = drawn * level_of(key, dims, cuts, -0.22, 0.18)
    return jnp.clip(drawn, -bound, bound).astype(kind)


def setup_inputs(seed: int = 0) -> dict:
    arg_keys = jax.random.split(jax.random.key(seed), 19)
    return {
        "hidden_in": scatter_about(arg_keys[0], (SEQUENCE_TOKENS, D), 1.0, 6.0, ((0, 64), (1, 8))),
        "w_query_rec": scatter_about(arg_keys[1], (D, RECURRENT_HEADS * HG_KDIM), D ** -0.5, 0.125, ((0, 64), (1, 8))),
        "w_forget": scatter_about(arg_keys[2], (D, RECURRENT_HEADS * HG_KDIM), D ** -0.5, 0.125, ((0, 64), (1, 8))),
        "w_input": scatter_about(arg_keys[3], (D, RECURRENT_HEADS * HG_VDIM), D ** -0.5, 0.125, ((0, 64), (1, 8))),
        "forget_gap": draw_forget_gap(jax.random.fold_in(arg_keys[18], 71), 0),
        "decay_extra": draw_decay_extra(jax.random.fold_in(arg_keys[18], 71), 0),
        "rec_gain": jnp.clip(1.0 + 0.18 * jax.random.normal(arg_keys[6], (HG_VDIM,), jnp.float32), 0.1, 1.9),
        "w_q_down": scatter_about(arg_keys[7], (D, Q_RANK), D ** -0.5, 0.125, ((1, 8),)),
        "w_kv_down": scatter_about(arg_keys[8], (D, KV_RANK), D ** -0.5, 0.125, ((1, 8),)),
        "w_key_rope": scatter_about(arg_keys[9], (D, ROPE), D ** -0.5, 0.125),
        "q_gain": draw_q_gain(jax.random.fold_in(arg_keys[18], 71), 0),
        "kv_gain": draw_kv_gain(jax.random.fold_in(arg_keys[18], 71), 0),
        "w_q_nope": scatter_about(arg_keys[12], (Q_RANK, MLA_HEADS * NOPE), Q_RANK ** -0.5, 0.25, ((1, 8),)),
        "w_q_rope": scatter_about(arg_keys[13], (Q_RANK, MLA_HEADS * ROPE), Q_RANK ** -0.5, 0.25, ((1, 8),)),
        "w_k_up": scatter_about(arg_keys[14], (KV_RANK, MLA_HEADS * NOPE), KV_RANK ** -0.5, 0.375, ((1, 8),)),
        "w_v_up": scatter_about(arg_keys[15], (KV_RANK, MLA_HEADS * MLA_V), KV_RANK ** -0.5, 0.375, ((1, 8),)),
        "w_out_rec": scatter_about(arg_keys[16], (RECURRENT_HEADS * HG_VDIM, D), (RECURRENT_HEADS * HG_VDIM + MLA_HEADS * MLA_V) ** -0.5, 0.109375, ((0, 8),)),
        "w_out_att": scatter_about(arg_keys[17], (MLA_HEADS * MLA_V, D), (RECURRENT_HEADS * HG_VDIM + MLA_HEADS * MLA_V) ** -0.5, 0.109375, ((0, 8),)),
    }


NORM_EPS = 1e-06
ROPE_BASE = 10000.0
NEG_BIG = -1e+30

def rms_scale(values):
    return values * lax.rsqrt(lax.optimization_barrier(jnp.mean(values * values, axis=-1, keepdims=True)) + NORM_EPS)

def rotate_half(values, cosine, sine_table):
    half_width = values.shape[-1] // 2
    lower_half = values[..., :half_width]
    upper_half = values[..., half_width:]
    return jnp.concatenate([lower_half * cosine - upper_half * sine_table, lower_half * sine_table + upper_half * cosine], axis=-1)

def rotary_tables(row_count, offset, rot_width):
    positions = jnp.arange(row_count, dtype=jnp.float32) + offset
    frequency = 1.0 / ROPE_BASE ** (jnp.arange(0, rot_width, 2, dtype=jnp.float32) / rot_width)
    angles = positions[:, None] * frequency[None, :]
    return (jnp.cos(angles), jnp.sin(angles))

def block_step(rec_state, inputs):
    queries, key_in, values, log_forget = inputs
    cumulative = jnp.cumsum(log_forget, axis=1)
    log_gaps = cumulative[:, :, None, :] - cumulative[:, None, :, :]
    block_len = queries.shape[1]
    lower_mask = jnp.tril(jnp.ones((block_len, block_len), jnp.float32))
    decays = jnp.exp(jnp.minimum(log_gaps, 0.0)) * lower_mask[None, :, :, None]
    scores = jnp.einsum('htsd,hsd->hts', queries[:, :, None, :] * decays, key_in, precision=lax.Precision.HIGHEST)
    block_out = jnp.einsum('hts,hsv->htv', scores, values, precision=lax.Precision.HIGHEST) + jnp.einsum('htd,hdv->htv', queries * jnp.exp(cumulative), rec_state, precision=lax.Precision.HIGHEST)
    last_cumul = cumulative[:, -1:, :]
    rec_state = jnp.exp(last_cumul[:, 0, :])[..., None] * rec_state + jnp.einsum('hsd,hsv->hdv', key_in * jnp.exp(last_cumul - cumulative), values, precision=lax.Precision.HIGHEST)
    return (rec_state, block_out)

def recurrence(queries, key_in, values, log_forget):
    seq_total, head_count, key_width = queries.shape
    block_count = seq_total // HG_BLOCK

    def to_blocks(tensor):
        return tensor.reshape(block_count, HG_BLOCK, head_count, tensor.shape[-1]).transpose(0, 2, 1, 3)
    initial = jnp.zeros((head_count, key_width, values.shape[-1]), jnp.float32)
    _, outputs = lax.scan(block_step, initial, (to_blocks(queries), to_blocks(key_in), to_blocks(values), to_blocks(log_forget)))
    return outputs.transpose(0, 2, 1, 3).reshape(seq_total, head_count, values.shape[-1])

def score_block(q_nope, q_rope, k_nope, k_rope, values, q_start, k_start):
    score_scale = 1.0 / math.sqrt(NOPE + ROPE)
    scores = (jnp.einsum('qhd,khd->hqk', q_nope.astype(jnp.float32), k_nope.astype(jnp.float32)) + jnp.einsum('qhr,kr->hqk', q_rope.astype(jnp.float32), k_rope.astype(jnp.float32))) * score_scale
    q_pos = q_start + jnp.arange(q_nope.shape[0], dtype=jnp.int32)
    k_pos = k_start + jnp.arange(k_nope.shape[0], dtype=jnp.int32)
    allowed = k_pos[None, :] <= q_pos[:, None]
    scores = jnp.where(allowed[None], scores, NEG_BIG)
    block_peak = lax.optimization_barrier(jnp.max(scores, axis=-1))
    weights = jnp.where(allowed[None], jnp.exp(scores - block_peak[..., None]), 0.0)
    block_total = lax.optimization_barrier(jnp.sum(weights, axis=-1))
    weights16 = weights.astype(jnp.bfloat16)
    block_sum = jnp.einsum('hqk,khv->hqv', weights16.astype(jnp.float32), values.astype(jnp.float32))
    return (block_peak, block_total, block_sum)

def merge_terms(earlier, later_part):
    top = jnp.maximum(earlier[0], later_part[0])
    old_factor = jnp.exp(earlier[0] - top)
    new_factor = jnp.exp(later_part[0] - top)
    return (top, earlier[1] * old_factor + later_part[1] * new_factor, earlier[2] * old_factor[..., None] + later_part[2] * new_factor[..., None])

def reference(hidden_in, w_query_rec, w_forget, w_input, forget_gap, decay_extra, rec_gain, w_q_down, w_kv_down, w_key_rope, q_gain, kv_gain, w_q_nope, w_q_rope, w_k_up, w_v_up, w_out_rec, w_out_att):
    seq_total = hidden_in.shape[0]

    def project_input(weight):
        return jnp.dot(hidden_in, weight, preferred_element_type=jnp.float32).astype(jnp.bfloat16)
    rec_query = project_input(w_query_rec).astype(jnp.float32).reshape(seq_total, RECURRENT_HEADS, HG_KDIM)
    forget_pre = project_input(w_forget).astype(jnp.float32).reshape(seq_total, RECURRENT_HEADS, HG_KDIM)
    rec_value = project_input(w_input).astype(jnp.float32).reshape(seq_total, RECURRENT_HEADS, HG_VDIM)
    gap_rows = forget_gap.reshape(RECURRENT_HEADS, HG_KDIM)
    closing = jax.nn.sigmoid(-forget_pre)
    key_in = gap_rows * closing
    log_forget = jnp.log1p(-gap_rows * closing) + decay_extra[:, :, None]
    rec_raw = recurrence(rec_query, key_in, rec_value, log_forget)
    rec_out = (rms_scale(rec_raw) * rec_gain).astype(jnp.bfloat16).reshape(seq_total, RECURRENT_HEADS * HG_VDIM)
    q_latent = project_input(w_q_down)
    kv_latent = project_input(w_kv_down)
    q_normed = (rms_scale(q_latent.astype(jnp.float32)) * q_gain).astype(jnp.bfloat16)
    latent = (rms_scale(kv_latent.astype(jnp.float32)) * kv_gain).astype(jnp.bfloat16)
    cosine, sine_table = rotary_tables(seq_total, 0.0, ROPE)
    key_rope = rotate_half(jnp.dot(hidden_in, w_key_rope, preferred_element_type=jnp.float32), cosine, sine_table).astype(jnp.bfloat16)
    q_nope = jnp.dot(q_normed, w_q_nope, preferred_element_type=jnp.float32).astype(jnp.bfloat16)
    q_nope = q_nope.reshape(seq_total, MLA_HEADS, NOPE)
    q_rope = jnp.dot(q_normed, w_q_rope, preferred_element_type=jnp.float32).reshape(seq_total, MLA_HEADS, ROPE)
    q_rope = rotate_half(q_rope, cosine[:, None, :], sine_table[:, None, :]).astype(jnp.bfloat16)
    k_nope = jnp.dot(latent, w_k_up, preferred_element_type=jnp.float32).astype(jnp.bfloat16)
    k_nope = k_nope.reshape(seq_total, MLA_HEADS, NOPE)
    att_value = jnp.dot(latent, w_v_up, preferred_element_type=jnp.float32).astype(jnp.bfloat16)
    att_value = att_value.reshape(seq_total, MLA_HEADS, MLA_V)
    block_len = TOK_DEV
    block_count = seq_total // block_len

    def per_query(query_block):
        q_start = (query_block * block_len).astype(jnp.int32)
        query_nope = lax.dynamic_slice_in_dim(q_nope, q_start, block_len, 0)
        query_rope = lax.dynamic_slice_in_dim(q_rope, q_start, block_len, 0)

        def inner(key_block, running):
            k_start = (key_block * block_len).astype(jnp.int32)
            partials = score_block(query_nope, query_rope, lax.dynamic_slice_in_dim(k_nope, k_start, block_len, 0), lax.dynamic_slice_in_dim(key_rope, k_start, block_len, 0), lax.dynamic_slice_in_dim(att_value, k_start, block_len, 0), q_start, k_start)
            return merge_terms(running, partials)
        initial = (jnp.full((MLA_HEADS, block_len), NEG_BIG, jnp.float32), jnp.zeros((MLA_HEADS, block_len), jnp.float32), jnp.zeros((MLA_HEADS, block_len, MLA_V), jnp.float32))
        top, total_w, accum = lax.fori_loop(jnp.int32(0), query_block + 1, inner, initial)
        result = accum / total_w[..., None]
        return result.transpose(1, 0, 2).reshape(block_len, MLA_HEADS * MLA_V).astype(jnp.bfloat16)
    att_out = lax.map(per_query, jnp.arange(block_count, dtype=jnp.int32)).reshape(seq_total, MLA_HEADS * MLA_V)
    mixed_out = jnp.dot(rec_out, w_out_rec, preferred_element_type=jnp.float32) + jnp.dot(att_out, w_out_att, preferred_element_type=jnp.float32)
    return mixed_out.astype(jnp.bfloat16)
```

```python
import functools
import math

import jax
import jax.numpy as jnp
from jax import lax
from jax.experimental import pallas as pl
from jax.experimental.pallas import tpu as pltpu
from jax.sharding import PartitionSpec as P

HEAD = 128
NOPE = 64
ROPE = 32
NORM_EPS = 1e-06
ROPE_BASE = 10000.0
NEG_BIG = -1e30
NY = 4
CHUNK = 512
MESH = pl.DeviceIdType.MESH
F32 = jnp.float32
BF16 = jnp.bfloat16
NT = (((1,), (1,)), ((), ()))
TN = (((0,), (0,)), ((), ()))
VM = pltpu.VMEM
DMA = pltpu.SemaphoreType.DMA


def dot(a, b):
    return jnp.dot(a, b, preferred_element_type=F32)


def dotg(a, b, dims):
    return lax.dot_general(a, b, dims, preferred_element_type=F32)


def remote(src, dst, ssem, rsem, dev):
    return pltpu.make_async_remote_copy(
        src_ref=src, dst_ref=dst, send_sem=ssem, recv_sem=rsem, device_id=dev, device_id_type=MESH
    )


def take_bytes(ref, count, sem):
    part = ref.at[pl.ds(0, count)]
    pltpu.make_async_copy(part, part, sem).wait()


def lanes_of(shape):
    return lax.broadcasted_iota(jnp.int32, shape, len(shape) - 1)


class Line:
    def __init__(self, ref, ssem, rsem, nx):
        self.ref, self.ssem, self.rsem, self.nx = ref, ssem, rsem, nx
        tp = lax.axis_index("tp")
        self.tp, self.core, self.x = tp, lax.rem(tp, 2), tp // 2
        self.sib = self.x * 2 + 1 - self.core

    def at_x(self, dx):
        return lax.rem(self.x + dx + self.nx, self.nx) * 2 + self.core

    def copy(self, slot, to, k):
        piece = self.ref.at[slot]
        return remote(piece, piece, self.ssem, self.rsem.at[k], {"tp": to})

    def start(self):
        for d in range(1, self.nx):
            self.copy(self.tp, self.at_x(d), d - 1).start()
        self.copy(self.tp, self.sib, self.nx - 1).start()

    def forward(self):
        for d in range(1, self.nx):
            slot = self.at_x(-d)
            self.copy(slot, self.tp, d - 1).wait_recv()
            self.copy(slot, self.sib, self.nx - 1 + d).start()

    def finish(self):
        for d in range(self.nx):
            x = lax.rem(self.x - d + self.nx, self.nx)
            self.copy(x * 2 + 1 - self.core, self.tp, self.nx - 1 + d).wait_recv()

    def drain(self):
        take_bytes(self.ref, 2 * self.nx - 1, self.ssem)


class Plane:
    def __init__(self, ref, ssem, zsem, ysem, nz):
        self.ref, self.ssem, self.zsem, self.ysem, self.nz = ref, ssem, zsem, ysem, nz
        self.sp = lax.axis_index("sp")
        self.z, self.y = self.sp // NY, lax.rem(self.sp, NY)
        self.up, self.down = nz // 2, nz // 2 - 1

    def slot(self, dz, dy):
        z = lax.rem(self.z + dz + self.nz, self.nz)
        return z * NY + lax.rem(self.y + dy + NY, NY)

    def copy(self, slot, to, sem):
        piece = self.ref.at[slot]
        return remote(piece, piece, self.ssem, sem, {"sp": to})

    def ways(self, t):
        if t <= self.up:
            yield 1, t - 1, t < self.up
        if t <= self.down:
            yield -1, self.up + t - 1, t < self.down

    def drain(self):
        take_bytes(self.ref, self.nz * NY - 1, self.ssem)


class PlaneZY(Plane):
    def spread(self, slot):
        for d in range(1, NY):
            self.copy(slot, self.slot(0, d), self.ysem).start()

    def start(self):
        for way, k, _ in self.ways(1):
            self.copy(self.sp, self.slot(way, 0), self.zsem.at[k]).start()
        self.spread(self.sp)

    def step(self, t):
        for way, k, more in self.ways(t):
            slot = self.slot(-way * t, 0)
            self.copy(slot, self.sp, self.zsem.at[k]).wait_recv()
            if more:
                self.copy(slot, self.slot(way, 0), self.zsem.at[k + 1]).start()
            self.spread(slot)

    def finish(self):
        take_bytes(self.ref, self.nz * (NY - 1), self.ysem)


class PlaneYZ(Plane):
    def start(self):
        for d in range(1, NY):
            self.copy(self.sp, self.slot(0, d), self.ysem.at[d - 1]).start()
        self.launch(0)

    def launch(self, d):
        for way, k, _ in self.ways(1):
            self.copy(self.slot(0, -d), self.slot(way, 0), self.zsem.at[k, d]).start()

    def begin(self):
        for d in range(1, NY):
            self.copy(self.slot(0, -d), self.sp, self.ysem.at[d - 1]).wait_recv()
            self.launch(d)

    def step(self, t):
        for d in range(NY):
            for way, k, more in self.ways(t):
                slot = self.slot(-way * t, -d)
                self.copy(slot, self.sp, self.zsem.at[k, d]).wait_recv()
                if more:
                    self.copy(slot, self.slot(way, 0), self.zsem.at[k + 1, d]).start()


def gather_kernel(
    nz, nx, hid, wq, wf, wi, wqd, wkvd, wkr, wku, wvu, wqn, wqr, qg, kvg, kcos, ksin,
    left, qn, lat, kvw, qw,
    hall, wa, wb, rall, wr,
    loc, hs, hr, ks, kr, qs, qr, rs, rr, was, waz, way_, wbs, wbz, wby, ls, lz, ly,
):
    tpn, spn = 2 * nx, nz * NY
    tp, sp = lax.axis_index("tp"), lax.axis_index("sp")
    toks, feat = hid.shape
    tt = lat.shape[1]
    line_h, line_k = Line(hall, hs, hr, nx), Line(kvw, ks, kr, nx)
    line_q, line_r = Line(qw, qs, qr, nx), Line(rall, rs, rr, nx)
    plane_a = PlaneYZ(wa, was, waz, way_, nz)
    plane_b = PlaneZY(wb, wbs, wbz, wby, nz)
    plane_l = PlaneYZ(lat, ls, lz, ly, nz)

    barrier = pltpu.get_barrier_semaphore()
    greet = [{"tp": line_h.at_x(d)} for d in range(1, nx)] + [{"tp": line_h.sib}]
    greet += [{"sp": plane_a.slot(0, d)} for d in range(1, NY)]
    greet += [{"sp": plane_a.slot(1, 0)}, {"sp": plane_a.slot(-1, 0)}]
    for dev in greet:
        pl.semaphore_signal(barrier, inc=1, device_id=dev, device_id_type=MESH)

    own = [
        pltpu.make_async_copy(hid, hall.at[tp], loc.at[0]),
        pltpu.make_async_copy(wq, wa.at[sp], loc.at[1]),
        pltpu.make_async_copy(wf, wb.at[sp, :, pl.ds(0, wf.shape[1])], loc.at[2]),
        pltpu.make_async_copy(wi, wb.at[sp, :, pl.ds(wf.shape[1], wi.shape[1])], loc.at[3]),
        pltpu.make_async_copy(wku, kvw.at[tp, :, pl.ds(0, 128)], loc.at[4]),
        pltpu.make_async_copy(wvu, kvw.at[tp, :, pl.ds(128, 128)], loc.at[5]),
        pltpu.make_async_copy(wqn, qw.at[tp, :, pl.ds(0, 128)], loc.at[6]),
    ]
    for c in own:
        c.start()
    qw[tp, :, 128:256] = jnp.zeros((qw.shape[1], 128), BF16)
    qw[tp, :, 128:192] = wqr[...]
    wr[:, 0:64] = wqd[...]
    wr[:, 64:96] = wkvd[...]
    wr[:, 96:128] = wkr[...]
    for c in own:
        c.wait()
    pl.semaphore_wait(barrier, len(greet))

    line_h.start()
    plane_a.start()
    plane_b.start()
    line_k.start()
    plane_a.begin()

    def wstep(t):
        plane_b.step(t)
        plane_a.step(t)

    def lora():
        line_h.finish()
        acc = dot(hall[0], wr[0:feat, :])
        for i in range(1, tpn):
            acc = acc + dot(hall[i], wr[i * feat : (i + 1) * feat, :])
        rall[tp] = acc.astype(BF16)
        line_r.start()
        first = pl.multiple_of(tp * tt, tt)
        mine = dot(hall[0, pl.ds(first, tt), :], wr[0:feat, :])
        for i in range(1, tpn):
            mine = mine + dot(hall[i, pl.ds(first, tt), :], wr[i * feat : (i + 1) * feat, :])
        lane = lanes_of((tt, 128))
        other = jnp.where(
            lax.rem(lane, 32) < 16, pltpu.roll(mine, 128 - 16, 1), pltpu.roll(mine, 16, 1)
        )
        turned = mine * kcos[...] + other * ksin[...]
        both = jnp.where(
            lane < 32,
            pltpu.roll(turned, 32, 1),
            jnp.where(lane < 64, pltpu.roll(turned, 64, 1), 0.0),
        )
        lat[sp, :, 256:384] = both.astype(BF16)

    def latents():
        line_r.finish()
        lane = lanes_of((toks, 128))
        total = jnp.zeros((toks, 128), F32)
        for i in range(tpn):
            piece = rall[i].astype(F32)
            total = total + jnp.where(lane < 64, piece * piece, 0.0)
        width = 64 * tpn
        scale = lax.rsqrt(jnp.sum(total, axis=1, keepdims=True) / width + NORM_EPS)
        for j in range(width // 128):
            one, two = rall[2 * j].astype(F32), rall[2 * j + 1].astype(F32)
            tile = jnp.where(lane < 64, one, pltpu.roll(two, 64, 1))
            cols = slice(128 * j, 128 * (j + 1))
            qn[:, cols] = (tile * scale * qg[:, cols]).astype(BF16)
        first = pl.multiple_of(tp * tt, tt)
        lane = lanes_of((tt, 128))
        tiles = []
        total = jnp.zeros((tt, 128), F32)
        width = 32 * tpn
        for j in range(2):
            tile = jnp.zeros((tt, 128), F32)
            for k in range(4):
                if 4 * j + k >= tpn:
                    continue
                piece = rall[4 * j + k, pl.ds(first, tt), :].astype(F32)
                moved = pltpu.roll(piece, (32 * k - 64) % 128, 1) if k != 2 else piece
                tile = jnp.where((lane >= 32 * k) & (lane < 32 * (k + 1)), moved, tile)
            tiles.append(tile)
            total = total + tile * tile
        scale = lax.rsqrt(jnp.sum(total, axis=1, keepdims=True) / width + NORM_EPS)
        for j in range(2):
            cols = slice(128 * j, 128 * (j + 1))
            lat[sp, :, cols] = (tiles[j] * scale * kvg[:, cols]).astype(BF16)

    def project(w, cols, at):
        per = spn // tpn
        acc = None
        for i in range(tpn):
            block = w[i * per : (i + 1) * per, :, cols].reshape(feat, 256)
            part = dot(hall[i], block)
            acc = part if acc is None else acc + part
        left[:, at : at + 256] = acc.astype(BF16)

    last = nz // 2
    jobs = {
        2: [line_h.forward],
        3: [lora],
        4: [line_k.forward, line_r.forward],
        5: [latents, plane_l.start, line_q.start],
        6: [plane_l.begin],
    }
    lsteps = list(range(1, last + 1))
    for t in range(1, max(last, 6) + 1):
        if t <= last:
            wstep(t)
        for job in jobs.get(t, []):
            job()
        if t > 6:
            plane_l.step(lsteps.pop(0))
    plane_b.finish()
    tail = [
        lambda: project(wb, slice(0, 256), 256),
        lambda: project(wb, slice(256, 512), 512),
        lambda: project(wa, slice(0, 256), 0),
        line_q.forward,
    ]
    while lsteps or tail:
        if lsteps:
            plane_l.step(lsteps.pop(0))
        if tail:
            tail.pop(0)()
    line_k.finish()
    line_q.finish()
    for part in (line_h, line_k, line_q, line_r, plane_a, plane_b, plane_l):
        part.drain()


def scan_kernel(
    nz, leftr, gap, dex, lout, qx, into,
    stb, decb, ys, yd, zb, zdb, zs, zd, ib,
    ys_s, ys_r, yd_s, yd_r, zs_s, zs_r, zd_s, zd_r, i_s, i_r,
):
    sp = lax.axis_index("sp")
    z, y = sp // NY, lax.rem(sp, NY)
    toks = leftr.shape[0]
    half = toks // 2
    vs = HEAD // NY

    def at_y(d):
        return z * NY + lax.rem(y + d + NY, NY)

    def at_z(d):
        return lax.rem(z + d + nz, nz) * NY + y

    barrier = pltpu.get_barrier_semaphore()
    for d in range(1, NY):
        pl.semaphore_signal(barrier, inc=1, device_id={"sp": at_y(d)}, device_id_type=MESH)
    for d in range(1, nz):
        pl.semaphore_signal(barrier, inc=1, device_id={"sp": at_z(d)}, device_id_type=MESH)

    pre = leftr[:, 256:512].astype(F32)
    key = gap[...] * (1.0 / (1.0 + jnp.exp(pre)))
    series = jnp.full(key.shape, 1.0 / 11.0, F32)
    for n in range(10, 0, -1):
        series = series * key + 1.0 / n
    lane = lanes_of((toks, 256))
    logf = jnp.where(lane < 128, dex[:, 0:1], dex[:, 1:2]) - series * key
    rows = lax.broadcasted_iota(jnp.int32, (toks, toks), 0)
    lower = jnp.where(rows >= lanes_of((toks, toks)), 1.0, 0.0).astype(F32)
    cum = jnp.dot(lower, logf, preferred_element_type=F32, precision=lax.Precision.HIGHEST)
    qx[...] = (leftr[:, 0:256].astype(F32) * jnp.exp(cum)).astype(BF16)
    tri = lax.broadcasted_iota(jnp.int32, (half, half), 0) >= lanes_of((half, half))
    for h in range(2):
        cols = slice(HEAD * h, HEAD * (h + 1))
        c, k = cum[:, cols], key[:, cols]
        q = leftr[:, cols].astype(F32)
        v = leftr[:, 512 + HEAD * h : 512 + HEAD * (h + 1)]
        edge, last = c[half - 1 : half], c[toks - 1 : toks]
        outs = []
        for b in range(2):
            r = slice(half * b, half * (b + 1))
            mid = c[half * b + half // 2 - 1 : half * b + half // 2]
            qd = (q[r] * jnp.exp(c[r] - mid)).astype(BF16)
            kd = (k[r] * jnp.exp(mid - c[r])).astype(BF16)
            a = jnp.where(tri, dotg(qd, kd, NT), 0.0).astype(BF16)
            outs.append(dot(a, v[r]))
        s0 = dotg(v[:half], (k[:half] * jnp.exp(edge - c[:half])).astype(BF16), TN)
        qe = (q[half:] * jnp.exp(c[half:] - edge)).astype(BF16)
        lout[0:half, cols] = outs[0]
        lout[half:toks, cols] = outs[1] + dotg(qe, s0.astype(BF16), NT)
        st = dotg(v, (k * jnp.exp(last - c)).astype(BF16), TN)
        stb[h] = st.astype(BF16)
        decb[h : h + 1, :] = jnp.exp(last)
    pl.semaphore_wait(barrier, NY - 1 + nz - 1)

    def ycopy(d):
        to = lax.rem(y + d + NY, NY)
        mine = stb.at[:, pl.ds(pl.multiple_of(to * vs, vs), vs), :]
        dev = {"sp": at_y(d)}
        return (
            remote(mine, ys.at[y], ys_s.at[d - 1], ys_r.at[d - 1], dev),
            remote(decb, yd.at[y], yd_s.at[d - 1], yd_r.at[d - 1], dev),
        )

    def yarrive(d):
        src = lax.rem(y - d + NY, NY)
        dev = {"sp": sp}
        remote(ys.at[src], ys.at[src], ys_s.at[d - 1], ys_r.at[d - 1], dev).wait_recv()
        remote(yd.at[src], yd.at[src], yd_s.at[d - 1], yd_r.at[d - 1], dev).wait_recv()

    for d in range(1, NY):
        for c in ycopy(d):
            c.start()
    for h in range(2):
        ys[y, h] = stb[h, pl.ds(pl.multiple_of(y * vs, vs), vs), :]
    yd[y] = decb[...]
    for d in range(1, NY):
        yarrive(d)
    before, spans = [], []
    state = [jnp.zeros((vs, HEAD), F32) for _ in range(2)]
    span = [jnp.ones((1, HEAD), F32) for _ in range(2)]
    for j in range(NY):
        before.append(list(state))
        spans.append(list(span))
        for h in range(2):
            decay = yd[j, h : h + 1, :]
            state[h] = decay * state[h] + ys[j, h].astype(F32)
            span[h] = span[h] * decay
    for h in range(2):
        zb[h] = state[h].astype(BF16)
        zdb[h : h + 1, :] = span[h]

    def zcopy(d):
        dev = {"sp": (z + d) * NY + y}
        return (
            remote(zb, zs.at[z], zs_s.at[d - 1], zs_r.at[z], dev),
            remote(zdb, zd.at[z], zd_s.at[d - 1], zd_r.at[z], dev),
        )

    for d in range(1, nz):

        @pl.when(z + d < nz)
        def _():
            for c in zcopy(d):
                c.start()

    def earlier(j, carry):
        dev = {"sp": sp}
        remote(zs.at[j], zs.at[j], zs_s.at[0], zs_r.at[j], dev).wait_recv()
        remote(zd.at[j], zd.at[j], zd_s.at[0], zd_r.at[j], dev).wait_recv()
        return tuple(zd[j, h : h + 1, :] * carry[h] + zs[j, h].astype(F32) for h in range(2))

    zero = jnp.zeros((vs, HEAD), F32)
    carry = lax.fori_loop(0, z, earlier, (zero, zero))
    for j in range(NY):
        for h in range(2):
            ib[j, h] = (spans[j][h] * carry[h] + before[j][h]).astype(BF16)

    def icopy(d):
        to = lax.rem(y + d + NY, NY)
        spot = into.at[:, pl.ds(pl.multiple_of(y * vs, vs), vs), :]
        return remote(ib.at[to], spot, i_s.at[d - 1], i_r.at[d - 1], {"sp": at_y(d)})

    for d in range(1, NY):
        icopy(d).start()
    for h in range(2):
        into[h, pl.ds(pl.multiple_of(y * vs, vs), vs), :] = ib[y, h]
    for d in range(1, NY):
        src = lax.rem(y - d + NY, NY)
        spot = into.at[:, pl.ds(pl.multiple_of(src * vs, vs), vs), :]
        remote(spot, spot, i_s.at[d - 1], i_r.at[d - 1], {"sp": sp}).wait_recv()
    for d in range(1, NY):
        for c in ycopy(d):
            c.wait_send()
        icopy(d).wait_send()
    for d in range(1, nz):

        @pl.when(z + d < nz)
        def _():
            for c in zcopy(d):
                c.wait_send()


def attend_kernel(tpn, spn, qn, lat, kvw, qw, qcos, qsin, o, stats, qblk, msc, acc):
    sp, tp = lax.axis_index("sp"), lax.axis_index("tp")
    toks = qn.shape[0]
    tt = lat.shape[1]
    per = CHUNK // tt
    scale = 1.0 / math.sqrt(NOPE + ROPE)
    lane = lanes_of((toks, 128))
    stats_tile = jnp.zeros((toks, 128), F32)
    whole = sp // per

    def pair(p, stats_tile):
        q = dot(qn[...], qw[p])
        flat, turn = q[:, :128], q[:, 128:]
        other = jnp.where(
            lax.rem(lane, 32) < 16, pltpu.roll(turn, 128 - 16, 1), pltpu.roll(turn, 16, 1)
        )
        turn = turn * qcos[...] + other * qsin[...]
        qblk[0:toks, 0:128] = jnp.where(lane < 64, flat, 0.0).astype(BF16)
        qblk[toks:, 0:128] = jnp.where(lane < 64, 0.0, flat).astype(BF16)
        qblk[0:toks, 128:256] = jnp.where(lane < 32, turn, 0.0).astype(BF16)
        qblk[toks:, 128:256] = jnp.where((lane >= 32) & (lane < 64), turn, 0.0).astype(BF16)
        msc[...] = jnp.full((2 * toks, 128), NEG_BIG, F32)
        acc[...] = jnp.zeros((2 * toks, 256), F32)

        def chunk(j, masked):
            part = lat[pl.ds(j * per, per)].reshape(CHUNK, 384)
            kv = dot(part[:, : kvw.shape[1]], kvw[p]).astype(BF16)
            keys = jnp.concatenate([kv[:, :128], part[:, 256:]], axis=1)
            vals = jnp.concatenate([kv[:, 128:], jnp.ones((CHUNK, 128), BF16)], axis=1)
            for h in range(2):
                r = slice(h * toks, (h + 1) * toks)
                s = dotg(qblk[r, :], keys, NT)
                if masked:
                    at = lanes_of((toks, CHUNK))
                    kpos = (j * per + at // tt) * toks + tp * tt + lax.rem(at, tt)
                    qpos = sp * toks + lax.broadcasted_iota(jnp.int32, (toks, CHUNK), 0)
                    ok = kpos <= qpos
                    s = jnp.where(ok, s, NEG_BIG)
                old = msc[r, 0:1]
                new = jnp.maximum(old, jnp.max(s, axis=1, keepdims=True))
                w = jnp.exp((s - new) * scale)
                if masked:
                    w = jnp.where(ok, w, 0.0)
                fade = jnp.exp((old - new) * scale)
                acc[r, :] = acc[r, :] * fade + dot(w.astype(BF16), vals)
                msc[r, :] = jnp.broadcast_to(new, (toks, 128))

        @pl.loop(0, whole)
        def _(j):
            chunk(j, False)

        chunk(whole, True)
        outs = []
        for h in range(2):
            r = slice(h * toks, (h + 1) * toks)
            total = acc[r, 128:256]
            some = total > 0.0
            safe = jnp.where(some, total, 1.0)
            outs.append(acc[r, 0:128] / safe)
            lse = jnp.where(some, msc[r, :] * scale + jnp.log(safe), NEG_BIG)
            stats_tile = jnp.where(lane == 8 * p + h, lse, stats_tile)
        o[p] = jnp.where(lane < 64, outs[0], outs[1]).astype(BF16)
        return stats_tile

    stats_tile = lax.fori_loop(0, tpn, pair, stats_tile)
    stats[...] = jnp.transpose(stats_tile)[: stats.shape[0]]


def merge_kernel(
    nx, o, stats, lout, qx, into, gain, wor, woa, out,
    orecv, srecv, mixed, pairs, got_pair, sums, got,
    o_s, o_r, s_s, s_r, p_s, p_r, f_s, f_r,
):
    tpn = 2 * nx
    tp = lax.axis_index("tp")
    x, core = tp // 2, lax.rem(tp, 2)
    sib = x * 2 + 1 - core
    toks = lout.shape[0]
    tt = toks // tpn
    barrier = pltpu.get_barrier_semaphore()

    def at(d):
        return lax.rem(tp + d + tpn, tpn)

    for d in range(1, tpn):
        pl.semaphore_signal(barrier, inc=1, device_id={"tp": at(d)}, device_id_type=MESH)
    pl.semaphore_wait(barrier, tpn - 1)

    def parts(d):
        to = at(d)
        return (
            remote(o.at[to], orecv.at[tp], o_s.at[d - 1], o_r.at[d - 1], {"tp": to}),
            remote(stats.at[to], srecv.at[tp], s_s.at[d - 1], s_r.at[d - 1], {"tp": to}),
        )

    for d in range(1, tpn):
        for c in parts(d):
            c.start()
    orecv[tp] = o[tp]
    srecv[tp] = stats[tp]

    cols = []
    for h in range(2):
        c = slice(HEAD * h, HEAD * (h + 1))
        raw = lout[:, c] + dotg(qx[:, c], into[h], NT)
        norm = lax.rsqrt(jnp.mean(raw * raw, axis=1, keepdims=True) + NORM_EPS)
        cols.append((raw * norm * gain[...]).astype(BF16))
    rec = jnp.concatenate(cols, axis=1)
    width = wor.shape[1]
    step = 512
    for n in range(0, width, step):
        mixed[:, n : n + step] = dot(rec, wor[:, n : n + step])

    for d in range(1, tpn):
        src = at(-d)
        dev = {"tp": tp}
        remote(orecv.at[src], orecv.at[src], o_s.at[d - 1], o_r.at[d - 1], dev).wait_recv()
        remote(srecv.at[src], srecv.at[src], s_s.at[d - 1], s_r.at[d - 1], dev).wait_recv()
    rowsT = srecv[...].reshape(8 * tpn, toks)
    if 8 * tpn < 128:
        rowsT = jnp.concatenate([rowsT, jnp.zeros((128 - 8 * tpn, toks), F32)], axis=0)
    lse = jnp.transpose(rowsT)
    lane = lanes_of((toks, 128))
    top = [
        functools.reduce(jnp.maximum, [lse[:, 8 * i + h : 8 * i + h + 1] for i in range(tpn)])
        for h in range(2)
    ]
    total = jnp.zeros((toks, 128), F32)
    merged = jnp.zeros((toks, 128), F32)
    for i in range(tpn):
        both = [jnp.exp(lse[:, 8 * i + h : 8 * i + h + 1] - top[h]) for h in range(2)]
        weight = jnp.where(lane < 64, both[0], both[1])
        total = total + weight
        merged = merged + weight * orecv[i].astype(F32)
    att = (merged / total).astype(BF16)
    for n in range(0, width, step):
        mixed[:, n : n + step] += dot(att, woa[:, n : n + step])

    for i in range(nx):
        first = pl.multiple_of((2 * i + 1 - core) * tt, tt)
        pairs[i] = mixed[pl.ds(first, tt), :].astype(BF16)
    pair = remote(pairs, got_pair, p_s, p_r, {"tp": sib})
    pair.start()
    pair.wait_recv()

    def mine(i):
        first = pl.multiple_of((2 * i + core) * tt, tt)
        return mixed[pl.ds(first, tt), :] + got_pair[i].astype(F32)

    def final(d):
        i = lax.rem(x + d, nx)
        return remote(sums.at[d - 1], got.at[d - 1], f_s.at[d - 1], f_r.at[d - 1], {"tp": i * 2 + core})

    for d in range(1, nx):
        sums[d - 1] = mine(lax.rem(x + d, nx)).astype(BF16)
        final(d).start()
    total = mine(x)
    for d in range(1, nx):
        final(d).wait_recv()
        total = total + got[d - 1].astype(F32)
    out[...] = total.astype(BF16)
    pair.wait_send()
    for d in range(1, nx):
        final(d).wait_send()
    for d in range(1, tpn):
        for c in parts(d):
            c.wait_send()


def call(kernel, name, ins, outs, scratch, cid=None):
    params = {"vmem_limit_bytes": 60 * 2**20}
    if cid is not None:
        params |= {"collective_id": cid, "has_side_effects": True}
    return pl.pallas_call(
        kernel,
        out_shape=[jax.ShapeDtypeStruct(s, d) for s, d in outs],
        in_specs=[pl.BlockSpec(memory_space=VM)] * ins,
        out_specs=[pl.BlockSpec(memory_space=VM)] * len(outs),
        scratch_shapes=scratch,
        compiler_params=pltpu.CompilerParams(**params),
        name=name,
    )


def shards(
    nz, nx,
    hidden_in, w_query_rec, w_forget, w_input, forget_gap, decay_extra, rec_gain,
    w_q_down, w_kv_down, w_key_rope, q_gain, kv_gain, w_q_nope, w_q_rope, w_k_up, w_v_up,
    w_out_rec, w_out_att,
):
    tpn, spn = 2 * nx, nz * NY
    toks, feat = hidden_in.shape
    tt = toks // tpn
    rw = w_query_rec.shape[0]
    qrank = w_q_down.shape[1] * tpn
    sp, tp = lax.axis_index("sp"), lax.axis_index("tp")

    position = (sp * toks + jnp.arange(toks)).astype(F32)
    lane = jnp.arange(128)
    frequency = 1.0 / ROPE_BASE ** (jnp.arange(0, ROPE, 2, dtype=F32) / ROPE)
    angle = position[:, None] * frequency[None, :]
    sign = jnp.where(lane % 32 < 16, -1.0, 1.0).astype(F32)
    qcos = jnp.tile(jnp.cos(angle), (1, 8))
    qsin = jnp.tile(jnp.sin(angle), (1, 8)) * sign[None, :]
    kcos = lax.dynamic_slice_in_dim(qcos, tp * tt, tt, 0)
    ksin = lax.dynamic_slice_in_dim(qsin, tp * tt, tt, 0)
    kvg = jnp.pad(kv_gain, (0, 256 - kv_gain.shape[0]))

    line = [DMA(()), DMA((2 * nx - 1,))]
    yz = [DMA(()), DMA((nz - 1, NY)), DMA((NY - 1,))]
    left, qn, lat, kvw, qw = call(
        functools.partial(gather_kernel, nz, nx),
        "gather",
        15,
        [
            ((toks, 768), BF16),
            ((toks, qrank), BF16),
            ((spn, tt, 384), BF16),
            ((tpn, w_k_up.shape[0], 256), BF16),
            ((tpn, qrank, 256), BF16),
        ],
        [
            VM((tpn, toks, feat), BF16),
            VM((spn, rw, 256), BF16),
            VM((spn, rw, 512), BF16),
            VM((tpn, toks, 128), BF16),
            VM((tpn * feat, 128), BF16),
            DMA((7,)),
            *line, *line, *line, *line,
            *yz, DMA(()), DMA((nz - 1,)), DMA(()), *yz,
        ],
        cid=0,
    )(
        hidden_in, w_query_rec, w_forget, w_input, w_q_down, w_kv_down, w_key_rope,
        w_k_up, w_v_up, w_q_nope, w_q_rope, q_gain[None], kvg[None], kcos, ksin,
    )

    vs = HEAD // NY
    lout, qx, into = call(
        functools.partial(scan_kernel, nz),
        "scan",
        3,
        [((toks, 256), F32), ((toks, 256), BF16), ((2, HEAD, HEAD), BF16)],
        [
            VM((2, HEAD, HEAD), BF16),
            VM((8, HEAD), F32),
            VM((NY, 2, vs, HEAD), BF16),
            VM((NY, 8, HEAD), F32),
            VM((2, vs, HEAD), BF16),
            VM((8, HEAD), F32),
            VM((nz, 2, vs, HEAD), BF16),
            VM((nz, 8, HEAD), F32),
            VM((NY, 2, vs, HEAD), BF16),
            *([DMA((NY - 1,))] * 4),
            DMA((nz - 1,)), DMA((nz,)), DMA((nz - 1,)), DMA((nz,)),
            *([DMA((NY - 1,))] * 2),
        ],
        cid=1,
    )(left, forget_gap[None], decay_extra)

    o, stats = call(
        functools.partial(attend_kernel, tpn, spn),
        "attend",
        6,
        [((tpn, toks, 128), BF16), ((8 * tpn, toks), F32)],
        [VM((2 * toks, 256), BF16), VM((2 * toks, 128), F32), VM((2 * toks, 256), F32)],
    )(qn, lat, kvw, qw, qcos, qsin)

    (out,) = call(
        functools.partial(merge_kernel, nx),
        "merge",
        8,
        [((tt, w_out_rec.shape[1]), BF16)],
        [
            VM((tpn, toks, 128), BF16),
            VM((tpn, 8, toks), F32),
            VM((toks, w_out_rec.shape[1]), F32),
            VM((nx, tt, w_out_rec.shape[1]), BF16),
            VM((nx, tt, w_out_rec.shape[1]), BF16),
            VM((max(nx - 1, 1), tt, w_out_rec.shape[1]), BF16),
            VM((max(nx - 1, 1), tt, w_out_rec.shape[1]), BF16),
            *([DMA((tpn - 1,))] * 4),
            DMA(()), DMA(()),
            *([DMA((max(nx - 1, 1),))] * 2),
        ],
        cid=2,
    )(o, stats.reshape(tpn, 8, toks), lout, qx, into, rec_gain[None], w_out_rec, w_out_att)
    return out


def solution(mesh):
    placed = (
        P("sp", "tp"),
        P("sp", "tp"),
        P("sp", "tp"),
        P("sp", "tp"),
        P("tp"),
        P("sp", "tp"),
        P(),
        P(None, "tp"),
        P(None, "tp"),
        P(),
        P(),
        P(),
        P(None, "tp"),
        P(None, "tp"),
        P(None, "tp"),
        P(None, "tp"),
        P("tp", None),
        P("tp", None),
    )
    nz, nx = mesh.shape["sp"] // NY, mesh.shape["tp"] // 2
    return jax.shard_map(
        functools.partial(shards, nz, nx),
        mesh=mesh,
        in_specs=placed,
        out_specs=P(("sp", "tp"), None),
        check_vma=False,
    )
```

```python
import functools
import math

import jax
import jax.numpy as jnp
from jax import lax
from jax.experimental import pallas as pl
from jax.experimental.pallas import tpu as pltpu
from jax.sharding import PartitionSpec as P

HEAD = 128
NOPE = 64
ROPE = 32
NORM_EPS = 1e-06
ROPE_BASE = 10000.0
NEG_BIG = -1e30
NY = 4
CHUNK = 512
SPLIT = 4
FULL_GREET = False
MESH = pl.DeviceIdType.MESH
F32 = jnp.float32
BF16 = jnp.bfloat16
NT = (((1,), (1,)), ((), ()))
TN = (((0,), (0,)), ((), ()))
VM = pltpu.VMEM
DMA = pltpu.SemaphoreType.DMA


def dot(a, b):
    return jnp.dot(a, b, preferred_element_type=F32)


def dotg(a, b, dims):
    return lax.dot_general(a, b, dims, preferred_element_type=F32)


def remote(src, dst, ssem, rsem, dev):
    return pltpu.make_async_remote_copy(
        src_ref=src, dst_ref=dst, send_sem=ssem, recv_sem=rsem, device_id=dev, device_id_type=MESH
    )


def take_bytes(ref, count, sem):
    part = ref.at[pl.ds(0, count)]
    pltpu.make_async_copy(part, part, sem).wait()


def lanes_of(shape):
    return lax.broadcasted_iota(jnp.int32, shape, len(shape) - 1)


class Line:
    def __init__(self, ref, ssem, rsem, nx):
        self.ref, self.ssem, self.rsem, self.nx = ref, ssem, rsem, nx
        tp = lax.axis_index("tp")
        self.tp, self.core, self.x = tp, lax.rem(tp, 2), tp // 2
        self.sib = self.x * 2 + 1 - self.core

    def at_x(self, dx):
        return lax.rem(self.x + dx + self.nx, self.nx) * 2 + self.core

    def copy(self, slot, to, k):
        piece = self.ref.at[slot]
        return remote(piece, piece, self.ssem, self.rsem.at[k], {"tp": to})

    def start(self):
        for d in range(1, self.nx):
            self.copy(self.tp, self.at_x(d), d - 1).start()
        self.copy(self.tp, self.sib, self.nx - 1).start()

    def forward(self):
        for d in range(1, self.nx):
            slot = self.at_x(-d)
            self.copy(slot, self.tp, d - 1).wait_recv()
            self.copy(slot, self.sib, self.nx - 1 + d).start()

    def finish(self):
        for d in range(self.nx):
            x = lax.rem(self.x - d + self.nx, self.nx)
            self.copy(x * 2 + 1 - self.core, self.tp, self.nx - 1 + d).wait_recv()

    def drain(self):
        take_bytes(self.ref, 2 * self.nx - 1, self.ssem)


class Plane:
    def __init__(self, ref, ssem, zsem, ysem, nz):
        self.ref, self.ssem, self.zsem, self.ysem, self.nz = ref, ssem, zsem, ysem, nz
        self.sp = lax.axis_index("sp")
        self.z, self.y = self.sp // NY, lax.rem(self.sp, NY)
        self.limit = {1: nz // 2, -1: nz // 2 - 1}
        self.steps = (nz // 2 + 1) // 2

    def slot(self, dz, dy):
        z = lax.rem(self.z + dz + self.nz, self.nz)
        return z * NY + lax.rem(self.y + dy + NY, NY)

    def copy(self, slot, to, sem):
        piece = self.ref.at[slot]
        return remote(piece, piece, self.ssem, sem, {"sp": to})

    def next_of(self, way, d):
        return [c for c in (d + 2, d + 1) if d % 2 == 0 and c <= self.limit[way]]

    def key(self, way, d):
        return d - 1 if way == 1 else self.limit[1] + d - 1

    def arrivals(self, t):
        return [(w, d) for d in (2 * t - 1, 2 * t) for w in (1, -1) if d <= self.limit[w]]

    def drain(self):
        take_bytes(self.ref, self.nz * NY - 1, self.ssem)


class PlaneZY(Plane):
    def hand_on(self, way, d):
        for c in self.next_of(way, d):
            self.copy(self.slot(-way * d, 0), self.slot(way * (c - d), 0), self.zsem.at[self.key(way, c)]).start()

    def spread(self, slot):
        for d in range(1, NY):
            self.copy(slot, self.slot(0, d), self.ysem).start()

    def start(self):
        self.hand_on(1, 0)
        self.hand_on(-1, 0)
        self.spread(self.sp)

    def step(self, t):
        for way, d in self.arrivals(t):
            slot = self.slot(-way * d, 0)
            self.copy(slot, self.sp, self.zsem.at[self.key(way, d)]).wait_recv()
            self.hand_on(way, d)
            self.spread(slot)

    def finish(self):
        take_bytes(self.ref, self.nz * (NY - 1), self.ysem)


class PlaneYZ(Plane):
    def hand_on(self, way, d, j):
        for c in self.next_of(way, d):
            sem = self.zsem.at[self.key(way, c), j]
            self.copy(self.slot(-way * d, -j), self.slot(way * (c - d), 0), sem).start()

    def start(self):
        for d in range(1, NY):
            self.copy(self.sp, self.slot(0, d), self.ysem.at[d - 1]).start()
        self.hand_on(1, 0, 0)
        self.hand_on(-1, 0, 0)

    def begin(self):
        for j in range(1, NY):
            self.copy(self.slot(0, -j), self.sp, self.ysem.at[j - 1]).wait_recv()
            self.hand_on(1, 0, j)
            self.hand_on(-1, 0, j)

    def step(self, t):
        for way, d in self.arrivals(t):
            for j in range(NY):
                slot = self.slot(-way * d, -j)
                self.copy(slot, self.sp, self.zsem.at[self.key(way, d), j]).wait_recv()
                self.hand_on(way, d, j)


class Scan:
    def __init__(self, nz, left, gap, dext, lout, qx, into, key, cum, stb, decb, ys, yd, zb, zdb, zs, zd, ib, sems):
        self.nz = nz
        self.left, self.gap, self.dext, self.lout, self.qx, self.into = left, gap, dext, lout, qx, into
        self.key, self.cum = key, cum
        self.stb, self.decb, self.ys, self.yd = stb, decb, ys, yd
        self.zb, self.zdb, self.zs, self.zd, self.ib = zb, zdb, zs, zd, ib
        self.ys_s, self.ys_r, self.yd_s, self.yd_r, self.zs_s, self.zs_r, self.zd_s, self.zd_r, self.i_s, self.i_r = sems
        self.sp = lax.axis_index("sp")
        self.z, self.y = self.sp // NY, lax.rem(self.sp, NY)
        self.vs = HEAD // NY

    def at_y(self, d):
        return self.z * NY + self.other(d)

    def other(self, d):
        return lax.rem(self.y + d + NY, NY)

    def rows(self, ref, j):
        return ref.at[:, pl.ds(pl.multiple_of(j * self.vs, self.vs), self.vs), :]

    def prepare(self):
        toks = self.left.shape[0]
        pre = self.left[:, 256:512].astype(F32)
        key = self.gap[...] * (1.0 / (1.0 + jnp.exp(pre)))
        series = jnp.full(key.shape, 1.0 / 11.0, F32)
        for n in range(10, 0, -1):
            series = series * key + 1.0 / n
        extra = [jnp.transpose(jnp.broadcast_to(self.dext[h : h + 1, :], (HEAD, toks))) for h in range(2)]
        logf = jnp.concatenate(extra, axis=1) - series * key
        rows = lax.broadcasted_iota(jnp.int32, (toks, toks), 0)
        lower = jnp.where(rows >= lanes_of((toks, toks)), 1.0, 0.0).astype(F32)
        cum = jnp.dot(lower, logf, preferred_element_type=F32, precision=lax.Precision.HIGHEST)
        self.qx[...] = (self.left[:, 0:256].astype(F32) * jnp.exp(cum)).astype(BF16)
        self.key[...] = key
        self.cum[...] = cum

    def local(self):
        toks = self.left.shape[0]
        half = toks // 2
        tri = lax.broadcasted_iota(jnp.int32, (half, half), 0) >= lanes_of((half, half))
        for h in range(2):
            cols = slice(HEAD * h, HEAD * (h + 1))
            c, k = self.cum[:, cols], self.key[:, cols]
            v = self.left[:, 512 + HEAD * h : 512 + HEAD * (h + 1)]
            last = c[toks - 1 : toks]
            self.stb[h] = dotg(v, (k * jnp.exp(last - c)).astype(BF16), TN).astype(BF16)
            self.decb[h : h + 1, :] = jnp.exp(last)
        for d in range(1, NY):
            for c in self.ycopy(d):
                c.start()
        for h in range(2):
            cols = slice(HEAD * h, HEAD * (h + 1))
            c, k = self.cum[:, cols], self.key[:, cols]
            q = self.left[:, cols].astype(F32)
            v = self.left[:, 512 + HEAD * h : 512 + HEAD * (h + 1)]
            edge = c[half - 1 : half]
            outs = []
            for b in range(2):
                r = slice(half * b, half * (b + 1))
                mid = c[half * b + half // 2 - 1 : half * b + half // 2]
                qd = (q[r] * jnp.exp(c[r] - mid)).astype(BF16)
                kd = (k[r] * jnp.exp(mid - c[r])).astype(BF16)
                a = jnp.where(tri, dotg(qd, kd, NT), 0.0).astype(BF16)
                outs.append(dot(a, v[r]))
            s0 = dotg(v[:half], (k[:half] * jnp.exp(edge - c[:half])).astype(BF16), TN)
            qe = (q[half:] * jnp.exp(c[half:] - edge)).astype(BF16)
            self.lout[0:half, cols] = outs[0]
            self.lout[half:toks, cols] = outs[1] + dotg(qe, s0.astype(BF16), NT)

    def ycopy(self, d):
        mine = self.rows(self.stb, self.other(d))
        dev = {"sp": self.at_y(d)}
        return (
            remote(mine, self.ys.at[self.y], self.ys_s.at[d - 1], self.ys_r.at[d - 1], dev),
            remote(self.decb, self.yd.at[self.y], self.yd_s.at[d - 1], self.yd_r.at[d - 1], dev),
        )

    def join_y(self):
        dev = {"sp": self.sp}
        y, ys, yd = self.y, self.ys, self.yd
        for h in range(2):
            ys[y, h] = self.stb[h, pl.ds(pl.multiple_of(y * self.vs, self.vs), self.vs), :]
        yd[y] = self.decb[...]
        for d in range(1, NY):
            src = self.other(-d)
            remote(ys.at[src], ys.at[src], self.ys_s.at[d - 1], self.ys_r.at[d - 1], dev).wait_recv()
            remote(yd.at[src], yd.at[src], self.yd_s.at[d - 1], self.yd_r.at[d - 1], dev).wait_recv()
        state = [jnp.zeros((self.vs, HEAD), F32) for _ in range(2)]
        span = [jnp.ones((1, HEAD), F32) for _ in range(2)]
        for j in range(NY):
            for h in range(2):
                decay = yd[j, h : h + 1, :]
                state[h] = decay * state[h] + ys[j, h].astype(F32)
                span[h] = span[h] * decay
        for h in range(2):
            self.zb[h] = state[h].astype(BF16)
            self.zdb[h : h + 1, :] = span[h]
        for d in range(1, self.nz):

            @pl.when(self.z + d < self.nz)
            def _():
                for c in self.zcopy(d):
                    c.start()

    def zcopy(self, d):
        dev = {"sp": (self.z + d) * NY + self.y}
        return (
            remote(self.zb, self.zs.at[self.z], self.zs_s.at[d - 1], self.zs_r.at[self.z], dev),
            remote(self.zdb, self.zd.at[self.z], self.zd_s.at[d - 1], self.zd_r.at[self.z], dev),
        )

    def join_z(self):
        zs, zd, ys, yd = self.zs, self.zd, self.ys, self.yd
        dev = {"sp": self.sp}

        def earlier(j, carry):
            remote(zs.at[j], zs.at[j], self.zs_s.at[0], self.zs_r.at[j], dev).wait_recv()
            remote(zd.at[j], zd.at[j], self.zd_s.at[0], self.zd_r.at[j], dev).wait_recv()
            return tuple(zd[j, h : h + 1, :] * carry[h] + zs[j, h].astype(F32) for h in range(2))

        zero = jnp.zeros((self.vs, HEAD), F32)
        state = list(lax.fori_loop(0, self.z, earlier, (zero, zero)))
        for j in range(NY):
            for h in range(2):
                self.ib[j, h] = state[h].astype(BF16)
                state[h] = yd[j, h : h + 1, :] * state[h] + ys[j, h].astype(F32)
        for d in range(1, NY):
            self.icopy(d).start()
        for h in range(2):
            spot = pl.ds(pl.multiple_of(self.y * self.vs, self.vs), self.vs)
            self.into[h, spot, :] = self.ib[self.y, h]

    def icopy(self, d):
        spot = self.rows(self.into, self.y)
        return remote(self.ib.at[self.other(d)], spot, self.i_s.at[d - 1], self.i_r.at[d - 1], {"sp": self.at_y(d)})

    def finish(self):
        for d in range(1, NY):
            spot = self.rows(self.into, self.other(-d))
            remote(spot, spot, self.i_s.at[d - 1], self.i_r.at[d - 1], {"sp": self.sp}).wait_recv()

    def drain(self):
        for d in range(1, NY):
            for c in self.ycopy(d):
                c.wait_send()
            self.icopy(d).wait_send()
        for d in range(1, self.nz):

            @pl.when(self.z + d < self.nz)
            def _():
                for c in self.zcopy(d):
                    c.wait_send()


def mixer_kernel(
    nz, nx, hid, wq, wf, wi, wqdt, wkvdt, wkrt, wku, wvu, wqn, wqrt, qg, kvg, kcos, ksin, qcos, qsin,
    gap, dext, gain, worh, woah, out,
    hall, wa, wb, rall, racc, wrt, left, qn, lat, kvw, qw, wor, woa,
    lout, qx, into, key, cum, stb, decb, ys, yd, zb, zdb, zs, zd, ib,
    qblk, msc, acc, obuf, sbuf, orecv, srecv, mixed, pairs, got_pair, sums, got,
    loc, hs, hr, ks, kr, qs, qr, rs, rr, was, waz, way_, wbs, wbz, wby, ls, lz, ly,
    ys_s, ys_r, yd_s, yd_r, zs_s, zs_r, zd_s, zd_r, i_s, i_r,
    o_s, o_r, s_s, s_r, p_s, p_r, f_s, f_r,
):
    tpn, spn = 2 * nx, nz * NY
    tp, sp = lax.axis_index("tp"), lax.axis_index("sp")
    x, core = tp // 2, lax.rem(tp, 2)
    toks, feat = hid.shape
    tt = lat.shape[1]
    line_h, line_k = Line(hall, hs, hr, nx), Line(kvw, ks, kr, nx)
    line_q, line_r = Line(qw, qs, qr, nx), Line(rall, rs, rr, nx)
    plane_a = PlaneYZ(wa, was, waz, way_, nz)
    plane_b = PlaneZY(wb, wbs, wbz, wby, nz)
    plane_l = PlaneZY(lat, ls, lz, ly, nz)
    sems = (ys_s, ys_r, yd_s, yd_r, zs_s, zs_r, zd_s, zd_r, i_s, i_r)
    scan = Scan(nz, left, gap, dext, lout, qx, into, key, cum, stb, decb, ys, yd, zb, zdb, zs, zd, ib, sems)

    barrier = pltpu.get_barrier_semaphore()
    greet = [{"tp": lax.rem(tp + d, tpn)} for d in range(1, tpn)]
    greet += [{"sp": plane_a.slot(0, d)} for d in range(1, NY)]
    near = [d for d in range(1, nz) if FULL_GREET or d <= 2 or d >= nz - 2]
    greet += [{"sp": plane_a.slot(d, 0)} for d in near]
    for dev in greet:
        pl.semaphore_signal(barrier, inc=1, device_id=dev, device_id_type=MESH)

    own = [
        pltpu.make_async_copy(hid, hall.at[tp], loc.at[0]),
        pltpu.make_async_copy(wq, wa.at[sp], loc.at[1]),
        pltpu.make_async_copy(wf, wb.at[sp, :, pl.ds(0, wf.shape[1])], loc.at[2]),
        pltpu.make_async_copy(wi, wb.at[sp, :, pl.ds(wf.shape[1], wi.shape[1])], loc.at[3]),
        pltpu.make_async_copy(wku, kvw.at[tp, :, pl.ds(0, 128)], loc.at[4]),
        pltpu.make_async_copy(wvu, kvw.at[tp, :, pl.ds(128, 128)], loc.at[5]),
    ]
    late = [pltpu.make_async_copy(worh, wor, loc.at[6]), pltpu.make_async_copy(woah, woa, loc.at[7])]
    for c in own + late:
        c.start()
    wrt[0:64, :] = wqdt[...]
    wrt[64:96, :] = wkvdt[...]
    wrt[96:128, :] = wkrt[...]
    for c in own:
        c.wait()
    pl.semaphore_wait(barrier, len(greet))

    line_h.start()
    plane_a.start()
    plane_b.start()
    line_k.start()
    qw[tp, 0:128, :] = jnp.transpose(wqn[...].astype(F32)).astype(BF16)
    qw[tp, 128:192, :] = wqrt[...]
    qblk[...] = jnp.zeros(qblk.shape, BF16)
    plane_a.begin()

    def wstep(t):
        plane_b.step(t)
        plane_a.step(t)

    def lora():
        line_h.finish()
        acc = None
        for i in range(tpn):
            part = dotg(hall[i], wrt[:, i * feat : (i + 1) * feat], NT)
            acc = part if acc is None else acc + part
        rall[tp] = acc.astype(BF16)
        line_r.start()
        racc[...] = acc
        mine = racc[pl.ds(pl.multiple_of(tp * tt, tt), tt), :]
        lane = lanes_of((tt, 128))
        other = jnp.where(
            lax.rem(lane, 32) < 16, pltpu.roll(mine, 128 - 16, 1), pltpu.roll(mine, 16, 1)
        )
        turned = mine * kcos[...] + other * ksin[...]
        lat[sp, :, 256:384] = jnp.where(lane < 32, pltpu.roll(turned, 32, 1), 0.0).astype(BF16)

    def latents():
        line_r.finish()
        first = pl.multiple_of(tp * tt, tt)
        lane = lanes_of((tt, 128))
        tiles = []
        total = jnp.zeros((tt, 128), F32)
        width = 32 * tpn
        for j in range(2):
            tile = jnp.zeros((tt, 128), F32)
            for k in range(4):
                if 4 * j + k >= tpn:
                    continue
                piece = rall[4 * j + k, pl.ds(first, tt), :].astype(F32)
                moved = pltpu.roll(piece, (32 * k - 64) % 128, 1) if k != 2 else piece
                tile = jnp.where((lane >= 32 * k) & (lane < 32 * (k + 1)), moved, tile)
            tiles.append(tile)
            total = total + tile * tile
        scale = lax.rsqrt(jnp.sum(total, axis=1, keepdims=True) / width + NORM_EPS)
        for j in range(2):
            cols = slice(128 * j, 128 * (j + 1))
            lat[sp, :, cols] = (tiles[j] * scale * kvg[:, cols]).astype(BF16)

    def queries():
        lane = lanes_of((toks, 128))
        total = jnp.zeros((toks, 128), F32)
        for i in range(tpn):
            piece = rall[i].astype(F32)
            total = total + jnp.where(lane < 64, piece * piece, 0.0)
        width = 64 * tpn
        scale = lax.rsqrt(jnp.sum(total, axis=1, keepdims=True) / width + NORM_EPS)
        for j in range(width // 128):
            one, two = rall[2 * j].astype(F32), rall[2 * j + 1].astype(F32)
            tile = jnp.where(lane < 64, one, pltpu.roll(two, 64, 1))
            cols = slice(128 * j, 128 * (j + 1))
            qn[:, cols] = (tile * scale * qg[:, cols]).astype(BF16)

    def project(w, cols, at):
        per = spn // tpn
        acc = None
        for i in range(tpn):
            block = w[i * per : (i + 1) * per, :, cols].reshape(feat, 256)
            part = dot(hall[i], block)
            acc = part if acc is None else acc + part
        left[:, at : at + 256] = acc.astype(BF16)

    jobs = {
        1: [line_h.forward],
        2: [lora, line_k.forward],
        3: [line_r.forward, latents, plane_l.start, line_q.start],
        4: [queries],
    }
    lsteps = list(range(1, plane_l.steps + 1))
    for t in range(1, max(plane_a.steps, 4) + 1):
        if t <= plane_a.steps:
            wstep(t)
        for job in jobs.get(t, []):
            job()
    if lsteps:
        plane_l.step(lsteps.pop(0))
    plane_b.finish()
    tail = [
        lambda: (project(wb, slice(0, 256), 256), project(wb, slice(256, 512), 512)),
        lambda: project(wa, slice(0, 256), 0),
        scan.prepare,
        scan.local,
        line_q.forward,
    ]
    while lsteps or tail:
        if tail:
            tail.pop(0)()
        if lsteps:
            plane_l.step(lsteps.pop(0))
    scan.join_y()
    line_k.finish()
    line_q.finish()
    plane_l.finish()

    per = CHUNK // tt
    base2 = math.log2(math.e) / math.sqrt(NOPE + ROPE)
    whole = sp // per

    def sent(p):
        dev = {"tp": p}
        return (
            remote(obuf.at[p], orecv.at[tp], o_s.at[p], o_r.at[tp], dev),
            remote(sbuf.at[p], srecv.at[tp], s_s.at[p], s_r.at[tp], dev),
        )

    def pair(i, _):
        p = lax.rem(tp + 1 + i, tpn)
        q = dotg(qw[p], qn[...], NT)
        for h in range(2):
            c = slice(h * toks, (h + 1) * toks)
            qblk[64 * h : 64 * (h + 1), c] = q[64 * h : 64 * (h + 1)].astype(BF16)
            a, b = q[128 + 32 * h : 144 + 32 * h], q[144 + 32 * h : 160 + 32 * h]
            qblk[128:144, c] = (a * qcos[...] - b * qsin[...]).astype(BF16)
            qblk[144:160, c] = (a * qsin[...] + b * qcos[...]).astype(BF16)
        msc[...] = jnp.full(msc.shape, NEG_BIG, F32)
        acc[...] = jnp.zeros(acc.shape, F32)

        def chunk(j, masked):
            part = lat[pl.ds(j * per, per)].reshape(CHUNK, 384)
            kv = dot(part[:, : kvw.shape[1]], kvw[p])
            keys = jnp.concatenate([kv[:, :128].astype(BF16), part[:, 256:]], axis=1)
            vals = jnp.transpose(kv[:, 128:]).astype(BF16)
            vals = jnp.concatenate([vals, jnp.ones((16, CHUNK), BF16)], axis=0)
            for h in range(2):
                c = slice(h * toks, (h + 1) * toks)
                s = dot(keys, qblk[:, c])
                if masked:
                    at = lax.broadcasted_iota(jnp.int32, (CHUNK, toks), 0)
                    kpos = (j * per + at // tt) * toks + tp * tt + lax.rem(at, tt)
                    ok = kpos <= sp * toks + lanes_of((CHUNK, toks))
                    s = jnp.where(ok, s, NEG_BIG)
                old = msc[0:1, c]
                new = jnp.maximum(old, jnp.max(s, axis=0, keepdims=True))
                w = jnp.exp2((s - new) * base2)
                if masked:
                    w = jnp.where(ok, w, 0.0)
                fade = jnp.exp2((old - new) * base2)
                acc[:, c] = acc[:, c] * fade + dot(vals, w.astype(BF16))
                msc[0:1, c] = new

        @pl.loop(0, whole)
        def _(j):
            chunk(j, False)

        chunk(whole, True)
        for h in range(2):
            c = slice(h * toks, (h + 1) * toks)
            total = acc[128:129, c]
            some = total > 0.0
            safe = jnp.where(some, total, 1.0)
            obuf[p, 64 * h : 64 * (h + 1), :] = (acc[64 * h : 64 * (h + 1), c] / safe).astype(BF16)
            sbuf[p, h : h + 1, :] = jnp.where(some, msc[0:1, c] * base2 + jnp.log2(safe), NEG_BIG)

        @pl.when(i < tpn - 1)
        def _():
            for c in sent(p):
                c.start()

        return 0

    lax.fori_loop(0, tpn - 2, pair, 0)
    scan.join_z()
    lax.fori_loop(tpn - 2, tpn, pair, 0)
    orecv[tp] = obuf[tp]
    srecv[tp] = sbuf[tp]

    scan.finish()
    cols = []
    for h in range(2):
        c = slice(HEAD * h, HEAD * (h + 1))
        raw = lout[:, c] + dotg(qx[:, c], into[h], NT)
        norm = lax.rsqrt(jnp.mean(raw * raw, axis=1, keepdims=True) + NORM_EPS)
        cols.append((raw * norm * gain[...]).astype(BF16))
    rec = jnp.concatenate(cols, axis=1)
    for c in late:
        c.wait()
    width = wor.shape[1]
    step = got.shape[3]
    for n in range(0, width, step):
        mixed[:, n : n + step] = dot(rec, wor[:, n : n + step])

    for d in range(1, tpn):
        src = lax.rem(tp + d, tpn)
        dev = {"tp": tp}
        remote(orecv.at[src], orecv.at[src], o_s.at[src], o_r.at[src], dev).wait_recv()
        remote(srecv.at[src], srecv.at[src], s_s.at[src], s_r.at[src], dev).wait_recv()
    halves = []
    for h in range(2):
        lse = [srecv[i, h : h + 1, :] for i in range(tpn)]
        top = functools.reduce(jnp.maximum, lse)
        total = jnp.zeros((1, toks), F32)
        merged = jnp.zeros((64, toks), F32)
        for i in range(tpn):
            weight = jnp.exp2(lse[i] - top)
            total = total + weight
            merged = merged + weight * orecv[i, 64 * h : 64 * (h + 1), :].astype(F32)
        halves.append((merged / total).astype(BF16))
    att = jnp.concatenate(halves, axis=0)

    sib = x * 2 + 1 - core

    def to_sib(k):
        return remote(pairs.at[k], got_pair.at[k], p_s.at[k], p_r.at[k], {"tp": sib})

    for k in range(width // step):
        n = slice(k * step, (k + 1) * step)
        mixed[:, n] += dotg(att, woa[:, n], TN)
        for i in range(nx):
            first = pl.multiple_of((2 * i + 1 - core) * tt, tt)
            pairs[k, i] = mixed[pl.ds(first, tt), n].astype(BF16)
        to_sib(k).start()

    def mine(i, k):
        first = pl.multiple_of((2 * i + core) * tt, tt)
        return mixed[pl.ds(first, tt), k * step : (k + 1) * step] + got_pair[k, i].astype(F32)

    def final(d, k):
        to = lax.rem(x + d, nx) * 2 + core
        return remote(sums.at[k, d - 1], got.at[k, d - 1], f_s.at[k, d - 1], f_r.at[k, d - 1], {"tp": to})

    for k in range(width // step):
        to_sib(k).wait_recv()
        for d in range(1, nx):
            sums[k, d - 1] = mine(lax.rem(x + d, nx), k).astype(BF16)
            final(d, k).start()
    for k in range(width // step):
        total = mine(x, k)
        for d in range(1, nx):
            final(d, k).wait_recv()
            total = total + got[k, d - 1].astype(F32)
        out[:, k * step : (k + 1) * step] = total.astype(BF16)
    for k in range(width // step):
        to_sib(k).wait_send()
        for d in range(1, nx):
            final(d, k).wait_send()
    for d in range(1, tpn):
        for c in sent(lax.rem(tp + d, tpn)):
            c.wait_send()
    for part in (line_h, line_k, line_q, line_r, plane_a, plane_b, plane_l, scan):
        part.drain()


def shards(
    nz, nx,
    hidden_in, w_query_rec, w_forget, w_input, forget_gap, decay_extra, rec_gain,
    w_q_down, w_kv_down, w_key_rope, q_gain, kv_gain, w_q_nope, w_q_rope, w_k_up, w_v_up,
    w_out_rec, w_out_att,
):
    tpn, spn = 2 * nx, nz * NY
    toks, feat = hidden_in.shape
    tt = toks // tpn
    rw = w_query_rec.shape[0]
    qrank = w_q_down.shape[1] * tpn
    kvrank = w_k_up.shape[0]
    width = w_out_rec.shape[1]
    sp, tp = lax.axis_index("sp"), lax.axis_index("tp")

    frequency = 1.0 / ROPE_BASE ** (jnp.arange(0, ROPE, 2, dtype=F32) / ROPE)
    position = (sp * toks + jnp.arange(toks)).astype(F32)
    angle = frequency[:, None] * position[None, :]
    qcos, qsin = jnp.cos(angle), jnp.sin(angle)
    keyed = (sp * toks + tp * tt + jnp.arange(tt)).astype(F32)
    angle = keyed[:, None] * jnp.tile(frequency, 8)[None, :]
    sign = jnp.where(jnp.arange(128) % 32 < 16, -1.0, 1.0).astype(F32)
    kcos, ksin = jnp.cos(angle), jnp.sin(angle) * sign[None, :]
    kvg = jnp.pad(kv_gain, (0, 256 - kv_gain.shape[0]))

    vs = HEAD // NY
    step = width // SPLIT
    line = [DMA(()), DMA((2 * nx - 1,))]
    far = max(nx - 1, 1)
    scratch = [
        VM((tpn, toks, feat), BF16),
        VM((spn, rw, 256), BF16),
        VM((spn, rw, 512), BF16),
        VM((tpn, toks, 128), BF16),
        VM((toks, 128), F32),
        VM((128, tpn * feat), BF16),
        VM((toks, 768), BF16),
        VM((toks, qrank), BF16),
        VM((spn, tt, 384), BF16),
        VM((tpn, kvrank, 256), BF16),
        VM((tpn, 192, qrank), BF16),
        VM(w_out_rec.shape, BF16),
        VM(w_out_att.shape, BF16),
        VM((toks, 256), F32),
        VM((toks, 256), BF16),
        VM((2, HEAD, HEAD), BF16),
        VM((toks, 256), F32),
        VM((toks, 256), F32),
        VM((2, HEAD, HEAD), BF16),
        VM((8, HEAD), F32),
        VM((NY, 2, vs, HEAD), BF16),
        VM((NY, 8, HEAD), F32),
        VM((2, vs, HEAD), BF16),
        VM((8, HEAD), F32),
        VM((nz, 2, vs, HEAD), BF16),
        VM((nz, 8, HEAD), F32),
        VM((NY, 2, vs, HEAD), BF16),
        VM((256, 2 * toks), BF16),
        VM((8, 2 * toks), F32),
        VM((144, 2 * toks), F32),
        VM((tpn, 128, toks), BF16),
        VM((tpn, 8, toks), F32),
        VM((tpn, 128, toks), BF16),
        VM((tpn, 8, toks), F32),
        VM((toks, width), F32),
        VM((SPLIT, nx, tt, step), BF16),
        VM((SPLIT, nx, tt, step), BF16),
        VM((SPLIT, far, tt, step), BF16),
        VM((SPLIT, far, tt, step), BF16),
        DMA((8,)),
        *line, *line, *line, *line,
        DMA(()), DMA((nz - 1, NY)), DMA((NY - 1,)),
        DMA(()), DMA((nz - 1,)), DMA(()),
        DMA(()), DMA((nz - 1,)), DMA(()),
        *([DMA((NY - 1,))] * 4),
        DMA((nz - 1,)), DMA((nz,)), DMA((nz - 1,)), DMA((nz,)),
        *([DMA((NY - 1,))] * 2),
        *([DMA((tpn,))] * 4),
        *([DMA((SPLIT,))] * 2),
        *([DMA((SPLIT, far))] * 2),
    ]
    args = (
        hidden_in, w_query_rec, w_forget, w_input, w_q_down.T, w_kv_down.T, w_key_rope.T,
        w_k_up, w_v_up, w_q_nope, w_q_rope.T, q_gain[None], kvg[None], kcos, ksin, qcos, qsin,
        forget_gap[None], decay_extra.T, rec_gain[None], w_out_rec, w_out_att,
    )
    whole, anywhere = pl.BlockSpec(memory_space=VM), pl.BlockSpec(memory_space=pl.ANY)
    return pl.pallas_call(
        functools.partial(mixer_kernel, nz, nx),
        out_shape=jax.ShapeDtypeStruct((tt, width), BF16),
        in_specs=[whole] * (len(args) - 2) + [anywhere] * 2,
        out_specs=whole,
        scratch_shapes=scratch,
        compiler_params=pltpu.CompilerParams(
            collective_id=0, has_side_effects=True, vmem_limit_bytes=60 * 2**20
        ),
        name="mixer",
    )(*args)


def solution(mesh):
    placed = (
        P("sp", "tp"),
        P("sp", "tp"),
        P("sp", "tp"),
        P("sp", "tp"),
        P("tp"),
        P("sp", "tp"),
        P(),
        P(None, "tp"),
        P(None, "tp"),
        P(),
        P(),
        P(),
        P(None, "tp"),
        P(None, "tp"),
        P(None, "tp"),
        P(None, "tp"),
        P("tp", None),
        P("tp", None),
    )
    nz, nx = mesh.shape["sp"] // NY, mesh.shape["tp"] // 2
    return jax.shard_map(
        functools.partial(shards, nz, nx),
        mesh=mesh,
        in_specs=placed,
        out_specs=P(("sp", "tp"), None),
        check_vma=False,
    )
```

```python
import functools
import math

import jax
import jax.numpy as jnp
from jax import lax
from jax.experimental import pallas as pl
from jax.experimental.pallas import tpu as pltpu
from jax.sharding import PartitionSpec as P

HEAD = 128
NOPE = 64
ROPE = 32
NORM_EPS = 1e-06
ROPE_BASE = 10000.0
NEG_BIG = -1e30
NY = 4
CHUNK = 512
SPLIT = 4
FULL_GREET = False
MESH = pl.DeviceIdType.MESH
F32 = jnp.float32
BF16 = jnp.bfloat16
NT = (((1,), (1,)), ((), ()))
TN = (((0,), (0,)), ((), ()))
VM = pltpu.VMEM
DMA = pltpu.SemaphoreType.DMA


def dot(a, b):
    return jnp.dot(a, b, preferred_element_type=F32)


def dotg(a, b, dims):
    return lax.dot_general(a, b, dims, preferred_element_type=F32)


def remote(src, dst, ssem, rsem, dev):
    return pltpu.make_async_remote_copy(
        src_ref=src, dst_ref=dst, send_sem=ssem, recv_sem=rsem, device_id=dev, device_id_type=MESH
    )


def take_bytes(ref, count, sem):
    part = ref.at[pl.ds(0, count)]
    pltpu.make_async_copy(part, part, sem).wait()


def lanes_of(shape):
    return lax.broadcasted_iota(jnp.int32, shape, len(shape) - 1)


class Line:
    def __init__(self, ref, ssem, rsem, nx):
        self.ref, self.ssem, self.rsem, self.nx = ref, ssem, rsem, nx
        tp = lax.axis_index("tp")
        self.tp, self.core, self.x = tp, lax.rem(tp, 2), tp // 2
        self.sib = self.x * 2 + 1 - self.core

    def at_x(self, dx):
        return lax.rem(self.x + dx + self.nx, self.nx) * 2 + self.core

    def copy(self, slot, to, k):
        piece = self.ref.at[slot]
        return remote(piece, piece, self.ssem, self.rsem.at[k], {"tp": to})

    def start(self):
        for d in range(1, self.nx):
            self.copy(self.tp, self.at_x(d), d - 1).start()
        self.copy(self.tp, self.sib, self.nx - 1).start()

    def forward(self):
        for d in range(1, self.nx):
            slot = self.at_x(-d)
            self.copy(slot, self.tp, d - 1).wait_recv()
            self.copy(slot, self.sib, self.nx - 1 + d).start()

    def finish(self):
        for d in range(self.nx):
            x = lax.rem(self.x - d + self.nx, self.nx)
            self.copy(x * 2 + 1 - self.core, self.tp, self.nx - 1 + d).wait_recv()

    def drain(self):
        take_bytes(self.ref, 2 * self.nx - 1, self.ssem)


class Plane:
    def __init__(self, ref, ssem, zsem, ysem, nz):
        self.ref, self.ssem, self.zsem, self.ysem, self.nz = ref, ssem, zsem, ysem, nz
        self.sp = lax.axis_index("sp")
        self.z, self.y = self.sp // NY, lax.rem(self.sp, NY)
        self.limit = {1: nz // 2, -1: nz // 2 - 1}
        self.steps = (nz // 2 + 1) // 2

    def slot(self, dz, dy):
        z = lax.rem(self.z + dz + self.nz, self.nz)
        return z * NY + lax.rem(self.y + dy + NY, NY)

    def copy(self, slot, to, sem):
        piece = self.ref.at[slot]
        return remote(piece, piece, self.ssem, sem, {"sp": to})

    def next_of(self, way, d):
        return [c for c in (d + 2, d + 1) if d % 2 == 0 and c <= self.limit[way]]

    def key(self, way, d):
        return d - 1 if way == 1 else self.limit[1] + d - 1

    def arrivals(self, t):
        return [(w, d) for d in (2 * t - 1, 2 * t) for w in (1, -1) if d <= self.limit[w]]

    def drain(self):
        take_bytes(self.ref, self.nz * NY - 1, self.ssem)


class PlaneZY(Plane):
    def hand_on(self, way, d):
        for c in self.next_of(way, d):
            self.copy(self.slot(-way * d, 0), self.slot(way * (c - d), 0), self.zsem.at[self.key(way, c)]).start()

    def spread(self, slot, t):
        for d in range(1, NY):
            self.copy(slot, self.slot(0, d), self.ysem.at[t]).start()

    def start(self):
        self.hand_on(1, 0)
        self.hand_on(-1, 0)
        self.spread(self.sp, 0)

    def step(self, t):
        for way, d in self.arrivals(t):
            slot = self.slot(-way * d, 0)
            self.copy(slot, self.sp, self.zsem.at[self.key(way, d)]).wait_recv()
            self.hand_on(way, d)
            self.spread(slot, t)

    def finish(self, first, last):
        for t in range(first, last + 1):
            count = len(self.arrivals(t)) if t else 1
            take_bytes(self.ref, count * (NY - 1), self.ysem.at[t])


class PlaneYZ(Plane):
    def hand_on(self, way, d, j):
        for c in self.next_of(way, d):
            sem = self.zsem.at[self.key(way, c), j]
            self.copy(self.slot(-way * d, -j), self.slot(way * (c - d), 0), sem).start()

    def start(self):
        for d in range(1, NY):
            self.copy(self.sp, self.slot(0, d), self.ysem.at[d - 1]).start()
        self.hand_on(1, 0, 0)
        self.hand_on(-1, 0, 0)

    def begin(self):
        for j in range(1, NY):
            self.copy(self.slot(0, -j), self.sp, self.ysem.at[j - 1]).wait_recv()
            self.hand_on(1, 0, j)
            self.hand_on(-1, 0, j)

    def step(self, t):
        for way, d in self.arrivals(t):
            for j in range(NY):
                slot = self.slot(-way * d, -j)
                self.copy(slot, self.sp, self.zsem.at[self.key(way, d), j]).wait_recv()
                self.hand_on(way, d, j)


class Scan:
    def __init__(self, nz, left, gap, dext, lout, qx, into, key, cum, stb, decb, ys, yd, zb, zdb, zs, zd, ib, sems):
        self.nz = nz
        self.left, self.gap, self.dext, self.lout, self.qx, self.into = left, gap, dext, lout, qx, into
        self.key, self.cum = key, cum
        self.stb, self.decb, self.ys, self.yd = stb, decb, ys, yd
        self.zb, self.zdb, self.zs, self.zd, self.ib = zb, zdb, zs, zd, ib
        self.ys_s, self.ys_r, self.yd_s, self.yd_r, self.zs_s, self.zs_r, self.zd_s, self.zd_r, self.i_s, self.i_r = sems
        self.sp = lax.axis_index("sp")
        self.z, self.y = self.sp // NY, lax.rem(self.sp, NY)
        self.vs = HEAD // NY

    def at_y(self, d):
        return self.z * NY + self.other(d)

    def other(self, d):
        return lax.rem(self.y + d + NY, NY)

    def rows(self, ref, j):
        return ref.at[:, pl.ds(pl.multiple_of(j * self.vs, self.vs), self.vs), :]

    def prepare(self):
        toks = self.left.shape[0]
        pre = self.left[:, 256:512].astype(F32)
        key = self.gap[...] * (1.0 / (1.0 + jnp.exp(pre)))
        series = jnp.full(key.shape, 1.0 / 11.0, F32)
        for n in range(10, 0, -1):
            series = series * key + 1.0 / n
        extra = [jnp.transpose(jnp.broadcast_to(self.dext[h : h + 1, :], (HEAD, toks))) for h in range(2)]
        logf = jnp.concatenate(extra, axis=1) - series * key
        rows = lax.broadcasted_iota(jnp.int32, (toks, toks), 0)
        lower = jnp.where(rows >= lanes_of((toks, toks)), 1.0, 0.0).astype(F32)
        cum = jnp.dot(lower, logf, preferred_element_type=F32, precision=lax.Precision.HIGHEST)
        self.key[...] = key
        self.cum[...] = cum

    def states(self):
        toks = self.left.shape[0]
        for h in range(2):
            cols = slice(HEAD * h, HEAD * (h + 1))
            c, k = self.cum[:, cols], self.key[:, cols]
            v = self.left[:, 512 + HEAD * h : 512 + HEAD * (h + 1)]
            last = c[toks - 1 : toks]
            self.stb[h] = dotg(v, (k * jnp.exp(last - c)).astype(BF16), TN).astype(BF16)
            self.decb[h : h + 1, :] = jnp.exp(last)
        for d in range(1, NY):
            for c in self.ycopy(d):
                c.start()

    def inside(self):
        toks = self.left.shape[0]
        half = toks // 2
        tri = lax.broadcasted_iota(jnp.int32, (half, half), 0) >= lanes_of((half, half))
        self.qx[...] = (self.left[:, 0:256].astype(F32) * jnp.exp(self.cum[...])).astype(BF16)
        for h in range(2):
            cols = slice(HEAD * h, HEAD * (h + 1))
            c, k = self.cum[:, cols], self.key[:, cols]
            q = self.left[:, cols].astype(F32)
            v = self.left[:, 512 + HEAD * h : 512 + HEAD * (h + 1)]
            edge = c[half - 1 : half]
            outs = []
            for b in range(2):
                r = slice(half * b, half * (b + 1))
                mid = c[half * b + half // 2 - 1 : half * b + half // 2]
                qd = (q[r] * jnp.exp(c[r] - mid)).astype(BF16)
                kd = (k[r] * jnp.exp(mid - c[r])).astype(BF16)
                a = jnp.where(tri, dotg(qd, kd, NT), 0.0).astype(BF16)
                outs.append(dot(a, v[r]))
            s0 = dotg(v[:half], (k[:half] * jnp.exp(edge - c[:half])).astype(BF16), TN)
            qe = (q[half:] * jnp.exp(c[half:] - edge)).astype(BF16)
            self.lout[0:half, cols] = outs[0]
            self.lout[half:toks, cols] = outs[1] + dotg(qe, s0.astype(BF16), NT)

    def ycopy(self, d):
        mine = self.rows(self.stb, self.other(d))
        dev = {"sp": self.at_y(d)}
        return (
            remote(mine, self.ys.at[self.y], self.ys_s.at[d - 1], self.ys_r.at[d - 1], dev),
            remote(self.decb, self.yd.at[self.y], self.yd_s.at[d - 1], self.yd_r.at[d - 1], dev),
        )

    def join_y(self):
        dev = {"sp": self.sp}
        y, ys, yd = self.y, self.ys, self.yd
        for h in range(2):
            ys[y, h] = self.stb[h, pl.ds(pl.multiple_of(y * self.vs, self.vs), self.vs), :]
        yd[y] = self.decb[...]
        for d in range(1, NY):
            src = self.other(-d)
            remote(ys.at[src], ys.at[src], self.ys_s.at[d - 1], self.ys_r.at[d - 1], dev).wait_recv()
            remote(yd.at[src], yd.at[src], self.yd_s.at[d - 1], self.yd_r.at[d - 1], dev).wait_recv()
        state = [jnp.zeros((self.vs, HEAD), F32) for _ in range(2)]
        span = [jnp.ones((1, HEAD), F32) for _ in range(2)]
        for j in range(NY):
            for h in range(2):
                decay = yd[j, h : h + 1, :]
                state[h] = decay * state[h] + ys[j, h].astype(F32)
                span[h] = span[h] * decay
        for h in range(2):
            self.zb[h] = state[h].astype(BF16)
            self.zdb[h : h + 1, :] = span[h]
        for d in range(self.nz - 1, 0, -1):

            @pl.when(self.z + d < self.nz)
            def _():
                for c in self.zcopy(d):
                    c.start()

    def zcopy(self, d):
        dev = {"sp": (self.z + d) * NY + self.y}
        return (
            remote(self.zb, self.zs.at[self.z], self.zs_s.at[d - 1], self.zs_r.at[self.z], dev),
            remote(self.zdb, self.zd.at[self.z], self.zd_s.at[d - 1], self.zd_r.at[self.z], dev),
        )

    def join_z(self):
        zs, zd, ys, yd = self.zs, self.zd, self.ys, self.yd
        dev = {"sp": self.sp}

        def earlier(j, carry):
            remote(zs.at[j], zs.at[j], self.zs_s.at[0], self.zs_r.at[j], dev).wait_recv()
            remote(zd.at[j], zd.at[j], self.zd_s.at[0], self.zd_r.at[j], dev).wait_recv()
            return tuple(zd[j, h : h + 1, :] * carry[h] + zs[j, h].astype(F32) for h in range(2))

        zero = jnp.zeros((self.vs, HEAD), F32)
        state = list(lax.fori_loop(0, self.z, earlier, (zero, zero)))
        for j in range(NY):
            for h in range(2):
                self.ib[j, h] = state[h].astype(BF16)
                state[h] = yd[j, h : h + 1, :] * state[h] + ys[j, h].astype(F32)
        for d in range(1, NY):
            self.icopy(d).start()
        for h in range(2):
            spot = pl.ds(pl.multiple_of(self.y * self.vs, self.vs), self.vs)
            self.into[h, spot, :] = self.ib[self.y, h]

    def icopy(self, d):
        spot = self.rows(self.into, self.y)
        return remote(self.ib.at[self.other(d)], spot, self.i_s.at[d - 1], self.i_r.at[d - 1], {"sp": self.at_y(d)})

    def finish(self):
        for d in range(1, NY):
            spot = self.rows(self.into, self.other(-d))
            remote(spot, spot, self.i_s.at[d - 1], self.i_r.at[d - 1], {"sp": self.sp}).wait_recv()

    def drain(self):
        for d in range(1, NY):
            for c in self.ycopy(d):
                c.wait_send()
            self.icopy(d).wait_send()
        for d in range(1, self.nz):

            @pl.when(self.z + d < self.nz)
            def _():
                for c in self.zcopy(d):
                    c.wait_send()


def mixer_kernel(
    nz, nx, hid, wq, wf, wi, wqdt, wkvdt, wkrt, wku, wvu, wqn, wqrt, qg, kvg, kcos, ksin, qcos, qsin,
    gap, dext, gain, worh, woah, out,
    hall, wa, wb, wc, rall, racc, wrt, left, qn, lat, kvw, qw, wor, woa,
    lout, qx, into, key, cum, stb, decb, ys, yd, zb, zdb, zs, zd, ib,
    krope, qblk, msc, acc, obuf, sbuf, orecv, srecv, mixed, pairs, got_pair, sums, got,
    loc, hs, hr, ks, kr, qs, qr, rs, rr, was, waz, way_, wbs, wbz, wby, wcs, wcz, wcy, ls, lz, ly,
    ys_s, ys_r, yd_s, yd_r, zs_s, zs_r, zd_s, zd_r, i_s, i_r,
    o_s, o_r, s_s, s_r, p_s, p_r, f_s, f_r,
):
    tpn, spn = 2 * nx, nz * NY
    tp, sp = lax.axis_index("tp"), lax.axis_index("sp")
    x, core = tp // 2, lax.rem(tp, 2)
    toks, feat = hid.shape
    tt = toks // tpn
    line_h, line_k = Line(hall, hs, hr, nx), Line(kvw, ks, kr, nx)
    line_q, line_r = Line(qw, qs, qr, nx), Line(rall, rs, rr, nx)
    plane_a = PlaneYZ(wa, was, waz, way_, nz)
    plane_b = PlaneZY(wb, wbs, wbz, wby, nz)
    plane_c = PlaneYZ(wc, wcs, wcz, wcy, nz)
    plane_l = PlaneZY(lat, ls, lz, ly, nz)
    sems = (ys_s, ys_r, yd_s, yd_r, zs_s, zs_r, zd_s, zd_r, i_s, i_r)
    scan = Scan(nz, left, gap, dext, lout, qx, into, key, cum, stb, decb, ys, yd, zb, zdb, zs, zd, ib, sems)

    barrier = pltpu.get_barrier_semaphore()
    greet = [{"tp": lax.rem(tp + d, tpn)} for d in range(1, tpn)]
    greet += [{"sp": plane_a.slot(0, d)} for d in range(1, NY)]
    near = [d for d in range(1, nz) if FULL_GREET or d <= 2 or d >= nz - 2]
    greet += [{"sp": plane_a.slot(d, 0)} for d in near]
    for dev in greet:
        pl.semaphore_signal(barrier, inc=1, device_id=dev, device_id_type=MESH)

    own = [
        pltpu.make_async_copy(hid, hall.at[tp], loc.at[0]),
        pltpu.make_async_copy(wf.at[:, pl.ds(0, 128)], wa.at[sp], loc.at[1]),
        pltpu.make_async_copy(wf.at[:, pl.ds(128, 128)], wb.at[sp, :, pl.ds(0, 128)], loc.at[2]),
        pltpu.make_async_copy(wi, wb.at[sp, :, pl.ds(128, 256)], loc.at[3]),
        pltpu.make_async_copy(wq, wc.at[sp], loc.at[8]),
        pltpu.make_async_copy(wku, kvw.at[tp, :, pl.ds(0, 128)], loc.at[4]),
        pltpu.make_async_copy(wvu, kvw.at[tp, :, pl.ds(128, 128)], loc.at[5]),
    ]
    late = [pltpu.make_async_copy(worh, wor, loc.at[6]), pltpu.make_async_copy(woah, woa, loc.at[7])]
    for c in own + late:
        c.start()
    wrt[0:64, :] = wqdt[...]
    wrt[64:96, :] = wkvdt[...]
    wrt[96:128, :] = wkrt[...]
    for c in own:
        c.wait()
    pl.semaphore_wait(barrier, len(greet))

    line_h.start()
    plane_a.start()
    plane_b.start()
    line_k.start()
    qw[tp, 0:128, :] = jnp.transpose(wqn[...].astype(F32)).astype(BF16)
    qw[tp, 128:192, :] = wqrt[...]
    qblk[...] = jnp.zeros(qblk.shape, BF16)
    plane_a.begin()

    def wstep(t):
        plane_b.step(t)
        plane_a.step(t)

    def lora():
        line_h.finish()
        acc = None
        for i in range(tpn):
            part = dotg(hall[i], wrt[:, i * feat : (i + 1) * feat], NT)
            acc = part if acc is None else acc + part
        rall[tp] = acc.astype(BF16)
        line_r.start()
        line_q.start()
        racc[...] = acc
        mine = racc[pl.ds(pl.multiple_of(tp * tt, tt), tt), :]
        lane = lanes_of((tt, 128))
        other = jnp.where(
            lax.rem(lane, 32) < 16, pltpu.roll(mine, 128 - 16, 1), pltpu.roll(mine, 16, 1)
        )
        turned = mine * kcos[...] + other * ksin[...]
        quart = tt // 4
        lane = lanes_of((quart, 128))
        packed = jnp.zeros((quart, 128), F32)
        for g in range(4):
            rows = turned[g * quart : (g + 1) * quart]
            moved = pltpu.roll(rows, 32 * (g + 1), 1) if g < 3 else rows
            packed = jnp.where((lane >= 32 * g) & (lane < 32 * (g + 1)), moved, packed)
        lat[sp, 2 * tt : 2 * tt + quart, :] = packed.astype(BF16)

    def latents():
        line_r.finish()
        first = pl.multiple_of(tp * tt, tt)
        lane = lanes_of((tt, 128))
        tiles = []
        total = jnp.zeros((tt, 128), F32)
        width = 32 * tpn
        for j in range(2):
            tile = jnp.zeros((tt, 128), F32)
            for k in range(4):
                if 4 * j + k >= tpn:
                    continue
                piece = rall[4 * j + k, pl.ds(first, tt), :].astype(F32)
                moved = pltpu.roll(piece, (32 * k - 64) % 128, 1) if k != 2 else piece
                tile = jnp.where((lane >= 32 * k) & (lane < 32 * (k + 1)), moved, tile)
            tiles.append(tile)
            total = total + tile * tile
        scale = lax.rsqrt(jnp.sum(total, axis=1, keepdims=True) / width + NORM_EPS)
        for j in range(2):
            cols = slice(128 * j, 128 * (j + 1))
            lat[sp, j * tt : (j + 1) * tt, :] = (tiles[j] * scale * kvg[:, cols]).astype(BF16)

    def queries():
        lane = lanes_of((toks, 128))
        total = jnp.zeros((toks, 128), F32)
        for i in range(tpn):
            piece = rall[i].astype(F32)
            total = total + jnp.where(lane < 64, piece * piece, 0.0)
        width = 64 * tpn
        scale = lax.rsqrt(jnp.sum(total, axis=1, keepdims=True) / width + NORM_EPS)
        for j in range(width // 128):
            one, two = rall[2 * j].astype(F32), rall[2 * j + 1].astype(F32)
            tile = jnp.where(lane < 64, one, pltpu.roll(two, 64, 1))
            cols = slice(128 * j, 128 * (j + 1))
            qn[:, cols] = (tile * scale * qg[:, cols]).astype(BF16)

    def project(blocks, at):
        spans = spn // tpn
        acc = None
        for i in range(tpn):
            block = [w[i * spans : (i + 1) * spans, :, n : n + m].reshape(feat, m) for w, n, m in blocks]
            block = block[0] if len(block) == 1 else jnp.concatenate(block, axis=1)
            part = dot(hall[i], block)
            acc = part if acc is None else acc + part
        left[:, at : at + 256] = acc.astype(BF16)

    jobs = {
        1: [line_h.forward],
        2: [lora],
        3: [line_k.forward, line_r.forward],
        4: [latents, plane_l.start, queries],
    }
    for t in range(1, max(plane_a.steps, 4) + 1):
        if t <= plane_a.steps:
            wstep(t)
        for job in jobs.get(t, []):
            job()
    plane_b.finish(0, plane_b.steps)
    project([(wa, 0, 128), (wb, 0, 128)], 256)
    project([(wb, 128, 256)], 512)
    scan.prepare()
    scan.states()
    steps = plane_l.steps

    def lstep(t):
        if t <= steps:
            plane_l.step(t)

    def cstep(t):
        if t <= steps:
            plane_c.step(t)

    lstep(1)
    line_q.forward()
    lstep(2)
    plane_c.start()
    scan.join_y()
    line_k.finish()
    line_q.finish()

    per = CHUNK // tt
    deep = per // NY
    chunks = spn // per
    base2 = math.log2(math.e) / math.sqrt(NOPE + ROPE)
    own_chunk = sp // per
    z = sp // NY

    def sent(p):
        dev = {"tp": p}
        return (
            remote(obuf.at[p], orecv.at[tp], o_s.at[p], o_r.at[tp], dev),
            remote(sbuf.at[p], srecv.at[tp], s_s.at[p], s_r.at[tp], dev),
        )

    def turn(p, _):
        q = dotg(qw[p], qn[...], NT)
        for h in range(2):
            c = slice(h * toks, (h + 1) * toks)
            qblk[p, 64 * h : 64 * (h + 1), c] = q[64 * h : 64 * (h + 1)].astype(BF16)
            a, b = q[128 + 32 * h : 144 + 32 * h], q[144 + 32 * h : 160 + 32 * h]
            qblk[p, 128:144, c] = (a * qcos[...] - b * qsin[...]).astype(BF16)
            qblk[p, 144:160, c] = (a * qsin[...] + b * qcos[...]).astype(BF16)
        return 0

    quart = tt // 4

    def unpack(j):
        rows = lat[pl.ds(j * per, per), 2 * tt : 2 * tt + quart, :].astype(F32)
        lane = lanes_of(rows.shape)
        parts = [
            jnp.where(lane < 32, pltpu.roll(rows, 128 - 32 * g, 2) if g else rows, 0.0)
            for g in range(4)
        ]
        whole = jnp.stack(parts, axis=1).reshape(CHUNK, 128)
        krope[pl.ds(pl.multiple_of(j * CHUNK, CHUNK), CHUNK), :] = whole.astype(BF16)

    def chunk(p, j, opening):
        tiles = kvw.shape[1] // 128
        part = [lat[pl.ds(j * per, per), i * tt : (i + 1) * tt, :].reshape(CHUNK, 128) for i in range(tiles)]
        part = part[0] if tiles == 1 else jnp.concatenate(part, axis=1)
        kv = dot(part, kvw[p])
        turned = krope[pl.ds(pl.multiple_of(j * CHUNK, CHUNK), CHUNK), :]
        keys = jnp.concatenate([kv[:, :128].astype(BF16), turned], axis=1)
        vals = jnp.transpose(kv[:, 128:]).astype(BF16)
        vals = jnp.concatenate([vals, jnp.ones((16, CHUNK), BF16)], axis=0)
        for h in range(2):
            c = slice(h * toks, (h + 1) * toks)
            s = dot(keys, qblk[p, :, c])
            if opening:
                at = lax.broadcasted_iota(jnp.int32, (CHUNK, toks), 0)
                kpos = (j * per + at // tt) * toks + tp * tt + lax.rem(at, tt)
                ok = kpos <= sp * toks + lanes_of((CHUNK, toks))
                s = jnp.where(ok, s, NEG_BIG)
                new = jnp.max(s, axis=0, keepdims=True)
                w = jnp.where(ok, jnp.exp2((s - new) * base2), 0.0)
                acc[p, :, c] = dot(vals, w.astype(BF16))
            else:
                old = msc[p, 0:1, c]
                new = jnp.maximum(old, jnp.max(s, axis=0, keepdims=True))
                w = jnp.exp2((s - new) * base2)
                fade = jnp.exp2((old - new) * base2)
                acc[p, :, c] = acc[p, :, c] * fade + dot(vals, w.astype(BF16))
            msc[p, 0:1, c] = new

    def reach(j):
        far = None
        for i in range(deep):
            d = z - (j * deep + i)
            d = jnp.where(d <= nz // 2, d, nz - d)
            far = d if far is None else jnp.maximum(far, d)
        return far

    def each(lo, hi, todo):
        @pl.loop(0, chunks)
        def _(j):
            far = reach(j)

            @pl.when((j < own_chunk) & (far > lo) & (far <= hi))
            def _():
                todo(j)

    def opened(p, _):
        chunk(p, own_chunk, True)
        return 0

    def close(i, _):
        p = lax.rem(tp + 1 + i, tpn)
        each(middle, nz, lambda j: chunk(p, j, False))
        for h in range(2):
            c = slice(h * toks, (h + 1) * toks)
            total = acc[p, 128:129, c]
            some = total > 0.0
            safe = jnp.where(some, total, 1.0)
            obuf[p, 64 * h : 64 * (h + 1), :] = (acc[p, 64 * h : 64 * (h + 1), c] / safe).astype(BF16)
            sbuf[p, h : h + 1, :] = jnp.where(some, msc[p, 0:1, c] * base2 + jnp.log2(safe), NEG_BIG)

        @pl.when(i < tpn - 1)
        def _():
            for c in sent(p):
                c.start()

        return 0

    def early(j):
        unpack(j)

        @pl.loop(0, tpn)
        def _(p):
            chunk(p, j, False)

    lax.fori_loop(0, tpn, turn, 0)
    half = tpn // 2
    first, second = min(2, steps), min(3, steps)
    middle = 2 * second if second > first else 0
    plane_l.finish(0, first)
    unpack(own_chunk)
    lax.fori_loop(0, half, opened, 0)
    lstep(3)
    plane_c.begin()
    lax.fori_loop(half, tpn, opened, 0)
    lstep(4)
    cstep(1)
    plane_l.finish(first + 1, second)
    if middle:
        each(0, middle, early)
    cstep(2)
    plane_l.finish(second + 1, steps)
    each(middle, nz, unpack)
    lax.fori_loop(0, half - 1, close, 0)
    cstep(3)
    lax.fori_loop(half - 1, half + 1, close, 0)
    cstep(4)
    scan.join_z()
    lax.fori_loop(half + 1, tpn, close, 0)
    orecv[tp] = obuf[tp]
    srecv[tp] = sbuf[tp]
    project([(wc, 0, 256)], 0)
    scan.inside()

    scan.finish()
    cols = []
    for h in range(2):
        c = slice(HEAD * h, HEAD * (h + 1))
        raw = lout[:, c] + dotg(qx[:, c], into[h], NT)
        norm = lax.rsqrt(jnp.mean(raw * raw, axis=1, keepdims=True) + NORM_EPS)
        cols.append((raw * norm * gain[...]).astype(BF16))
    rec = jnp.concatenate(cols, axis=1)
    for c in late:
        c.wait()
    width = wor.shape[1]
    step = got.shape[3]
    for n in range(0, width, step):
        mixed[:, n : n + step] = dot(rec, wor[:, n : n + step])

    for d in range(1, tpn):
        src = lax.rem(tp + d, tpn)
        dev = {"tp": tp}
        remote(orecv.at[src], orecv.at[src], o_s.at[src], o_r.at[src], dev).wait_recv()
        remote(srecv.at[src], srecv.at[src], s_s.at[src], s_r.at[src], dev).wait_recv()
    halves = []
    for h in range(2):
        lse = [srecv[i, h : h + 1, :] for i in range(tpn)]
        top = functools.reduce(jnp.maximum, lse)
        total = jnp.zeros((1, toks), F32)
        merged = jnp.zeros((64, toks), F32)
        for i in range(tpn):
            weight = jnp.exp2(lse[i] - top)
            total = total + weight
            merged = merged + weight * orecv[i, 64 * h : 64 * (h + 1), :].astype(F32)
        halves.append((merged / total).astype(BF16))
    att = jnp.concatenate(halves, axis=0)

    sib = x * 2 + 1 - core

    def to_sib(k):
        return remote(pairs.at[k], got_pair.at[k], p_s.at[k], p_r.at[k], {"tp": sib})

    for k in range(width // step):
        n = slice(k * step, (k + 1) * step)
        mixed[:, n] += dotg(att, woa[:, n], TN)
        for i in range(nx):
            first = pl.multiple_of((2 * i + 1 - core) * tt, tt)
            pairs[k, i] = mixed[pl.ds(first, tt), n].astype(BF16)
        to_sib(k).start()

    def mine(i, k):
        first = pl.multiple_of((2 * i + core) * tt, tt)
        return mixed[pl.ds(first, tt), k * step : (k + 1) * step] + got_pair[k, i].astype(F32)

    def final(d, k):
        to = lax.rem(x + d, nx) * 2 + core
        return remote(sums.at[k, d - 1], got.at[k, d - 1], f_s.at[k, d - 1], f_r.at[k, d - 1], {"tp": to})

    for k in range(width // step):
        to_sib(k).wait_recv()
        for d in range(1, nx):
            sums[k, d - 1] = mine(lax.rem(x + d, nx), k).astype(BF16)
            final(d, k).start()
    for k in range(width // step):
        total = mine(x, k)
        for d in range(1, nx):
            final(d, k).wait_recv()
            total = total + got[k, d - 1].astype(F32)
        out[:, k * step : (k + 1) * step] = total.astype(BF16)
    for k in range(width // step):
        to_sib(k).wait_send()
        for d in range(1, nx):
            final(d, k).wait_send()
    for d in range(1, tpn):
        for c in sent(lax.rem(tp + d, tpn)):
            c.wait_send()
    for part in (line_h, line_k, line_q, line_r, plane_a, plane_b, plane_c, plane_l, scan):
        part.drain()


def shards(
    nz, nx,
    hidden_in, w_query_rec, w_forget, w_input, forget_gap, decay_extra, rec_gain,
    w_q_down, w_kv_down, w_key_rope, q_gain, kv_gain, w_q_nope, w_q_rope, w_k_up, w_v_up,
    w_out_rec, w_out_att,
):
    tpn, spn = 2 * nx, nz * NY
    toks, feat = hidden_in.shape
    tt = toks // tpn
    rw = w_query_rec.shape[0]
    qrank = w_q_down.shape[1] * tpn
    kvrank = w_k_up.shape[0]
    width = w_out_rec.shape[1]
    sp, tp = lax.axis_index("sp"), lax.axis_index("tp")

    frequency = 1.0 / ROPE_BASE ** (jnp.arange(0, ROPE, 2, dtype=F32) / ROPE)
    position = (sp * toks + jnp.arange(toks)).astype(F32)
    angle = frequency[:, None] * position[None, :]
    qcos, qsin = jnp.cos(angle), jnp.sin(angle)
    keyed = (sp * toks + tp * tt + jnp.arange(tt)).astype(F32)
    angle = keyed[:, None] * jnp.tile(frequency, 8)[None, :]
    sign = jnp.where(jnp.arange(128) % 32 < 16, -1.0, 1.0).astype(F32)
    kcos, ksin = jnp.cos(angle), jnp.sin(angle) * sign[None, :]
    kvg = jnp.pad(kv_gain, (0, 256 - kv_gain.shape[0]))

    vs = HEAD // NY
    step = width // SPLIT
    line = [DMA(()), DMA((2 * nx - 1,))]
    far = max(nx - 1, 1)
    scratch = [
        VM((tpn, toks, feat), BF16),
        VM((spn, rw, 128), BF16),
        VM((spn, rw, 384), BF16),
        VM((spn, rw, 256), BF16),
        VM((tpn, toks, 128), BF16),
        VM((toks, 128), F32),
        VM((128, tpn * feat), BF16),
        VM((toks, 768), BF16),
        VM((toks, qrank), BF16),
        VM((spn, 2 * tt + tt // 4, 128), BF16),
        VM((tpn, kvrank, 256), BF16),
        VM((tpn, 192, qrank), BF16),
        VM(w_out_rec.shape, BF16),
        VM(w_out_att.shape, BF16),
        VM((toks, 256), F32),
        VM((toks, 256), BF16),
        VM((2, HEAD, HEAD), BF16),
        VM((toks, 256), F32),
        VM((toks, 256), F32),
        VM((2, HEAD, HEAD), BF16),
        VM((8, HEAD), F32),
        VM((NY, 2, vs, HEAD), BF16),
        VM((NY, 8, HEAD), F32),
        VM((2, vs, HEAD), BF16),
        VM((8, HEAD), F32),
        VM((nz, 2, vs, HEAD), BF16),
        VM((nz, 8, HEAD), F32),
        VM((NY, 2, vs, HEAD), BF16),
        VM((spn * tt, 128), BF16),
        VM((tpn, 256, 2 * toks), BF16),
        VM((tpn, 8, 2 * toks), F32),
        VM((tpn, 144, 2 * toks), F32),
        VM((tpn, 128, toks), BF16),
        VM((tpn, 8, toks), F32),
        VM((tpn, 128, toks), BF16),
        VM((tpn, 8, toks), F32),
        VM((toks, width), F32),
        VM((SPLIT, nx, tt, step), BF16),
        VM((SPLIT, nx, tt, step), BF16),
        VM((SPLIT, far, tt, step), BF16),
        VM((SPLIT, far, tt, step), BF16),
        DMA((9,)),
        *line, *line, *line, *line,
        DMA(()), DMA((nz - 1, NY)), DMA((NY - 1,)),
        DMA(()), DMA((nz - 1,)), DMA((nz // 4 + 1,)),
        DMA(()), DMA((nz - 1, NY)), DMA((NY - 1,)),
        DMA(()), DMA((nz - 1,)), DMA((nz // 4 + 1,)),
        *([DMA((NY - 1,))] * 4),
        DMA((nz - 1,)), DMA((nz,)), DMA((nz - 1,)), DMA((nz,)),
        *([DMA((NY - 1,))] * 2),
        *([DMA((tpn,))] * 4),
        *([DMA((SPLIT,))] * 2),
        *([DMA((SPLIT, far))] * 2),
    ]
    args = (
        hidden_in, w_query_rec, w_forget, w_input, w_q_down.T, w_kv_down.T, w_key_rope.T,
        w_k_up, w_v_up, w_q_nope, w_q_rope.T, q_gain[None], kvg[None], kcos, ksin, qcos, qsin,
        forget_gap[None], decay_extra.T, rec_gain[None], w_out_rec, w_out_att,
    )
    whole, anywhere = pl.BlockSpec(memory_space=VM), pl.BlockSpec(memory_space=pl.ANY)
    return pl.pallas_call(
        functools.partial(mixer_kernel, nz, nx),
        out_shape=jax.ShapeDtypeStruct((tt, width), BF16),
        in_specs=[whole] * (len(args) - 2) + [anywhere] * 2,
        out_specs=whole,
        scratch_shapes=scratch,
        compiler_params=pltpu.CompilerParams(
            collective_id=0, has_side_effects=True, vmem_limit_bytes=60 * 2**20
        ),
        name="mixer",
    )(*args)


def solution(mesh):
    placed = (
        P("sp", "tp"),
        P("sp", "tp"),
        P("sp", "tp"),
        P("sp", "tp"),
        P("tp"),
        P("sp", "tp"),
        P(),
        P(None, "tp"),
        P(None, "tp"),
        P(),
        P(),
        P(),
        P(None, "tp"),
        P(None, "tp"),
        P(None, "tp"),
        P(None, "tp"),
        P("tp", None),
        P("tp", None),
    )
    nz, nx = mesh.shape["sp"] // NY, mesh.shape["tp"] // 2
    return jax.shard_map(
        functools.partial(shards, nz, nx),
        mesh=mesh,
        in_specs=placed,
        out_specs=P(("sp", "tp"), None),
        check_vma=False,
    )
```

```python
import functools
import math

import jax
import jax.numpy as jnp
from jax import lax
from jax.experimental import pallas as pl
from jax.experimental.pallas import tpu as pltpu
from jax.sharding import PartitionSpec as P

HEAD = 128
NOPE = 64
ROPE = 32
NORM_EPS = 1e-06
ROPE_BASE = 10000.0
NEG_BIG = -1e30
NY = 4
CHUNK = 512
SPLIT = 4
FULL_GREET = False
MESH = pl.DeviceIdType.MESH
F32 = jnp.float32
BF16 = jnp.bfloat16
NT = (((1,), (1,)), ((), ()))
TN = (((0,), (0,)), ((), ()))
VM = pltpu.VMEM
DMA = pltpu.SemaphoreType.DMA


def dot(a, b):
    return jnp.dot(a, b, preferred_element_type=F32)


def dotg(a, b, dims):
    return lax.dot_general(a, b, dims, preferred_element_type=F32)


def remote(src, dst, ssem, rsem, dev):
    return pltpu.make_async_remote_copy(
        src_ref=src, dst_ref=dst, send_sem=ssem, recv_sem=rsem, device_id=dev, device_id_type=MESH
    )


def take_bytes(ref, count, sem):
    part = ref.at[pl.ds(0, count)]
    pltpu.make_async_copy(part, part, sem).wait()


def lanes_of(shape):
    return lax.broadcasted_iota(jnp.int32, shape, len(shape) - 1)


class Line:
    def __init__(self, ref, ssem, rsem, nx):
        self.ref, self.ssem, self.rsem, self.nx = ref, ssem, rsem, nx
        tp = lax.axis_index("tp")
        self.tp, self.core, self.x = tp, lax.rem(tp, 2), tp // 2
        self.sib = self.x * 2 + 1 - self.core

    def near(self):
        return [1, -1] if self.nx > 2 else [1]

    def at_x(self, dx):
        return lax.rem(self.x + dx + self.nx, self.nx) * 2 + self.core

    def copy(self, slot, to, k):
        piece = self.ref.at[slot]
        return remote(piece, piece, self.ssem, self.rsem.at[k], {"tp": to})

    def relay(self, slot, to, k):
        rows = self.ref.shape[1] // 2
        piece = self.ref.at[slot, pl.ds(k * rows, rows)]
        return remote(piece, piece, self.ssem, self.rsem.at[2 + k], {"tp": to})

    def over(self, dx):
        self.copy(self.at_x(-dx), self.sib, self.nx + dx % self.nx).start()

    def start(self):
        for k, d in enumerate(self.near()):
            self.copy(self.tp, self.at_x(d), k).start()
        self.over(0)

    def forward(self):
        for k, d in enumerate(self.near()):
            slot = self.at_x(-d)
            self.copy(slot, self.tp, k).wait_recv()
            if self.nx > 2:
                self.relay(slot, self.at_x(d), k).start()
            self.over(d)

    def forward_far(self):
        if self.nx > 2:
            for k in range(2):
                self.relay(self.at_x(2), self.tp, k).wait_recv()
            self.over(2)

    def finish(self):
        for d in range(self.nx):
            x = lax.rem(self.x - d + self.nx, self.nx)
            self.copy(x * 2 + 1 - self.core, self.tp, self.nx + d).wait_recv()

    def drain(self):
        take_bytes(self.ref, 2 * self.nx - 1, self.ssem)


class Plane:
    def __init__(self, ref, ssem, zsem, ysem, nz):
        self.ref, self.ssem, self.zsem, self.ysem, self.nz = ref, ssem, zsem, ysem, nz
        self.sp = lax.axis_index("sp")
        self.z, self.y = self.sp // NY, lax.rem(self.sp, NY)
        self.limit = {1: nz // 2, -1: nz // 2 - 1}
        self.steps = (nz // 2 + 1) // 2

    def slot(self, dz, dy):
        z = lax.rem(self.z + dz + self.nz, self.nz)
        return z * NY + lax.rem(self.y + dy + NY, NY)

    def copy(self, slot, to, sem):
        piece = self.ref.at[slot]
        return remote(piece, piece, self.ssem, sem, {"sp": to})

    def next_of(self, way, d):
        return [c for c in (d + 2, d + 1) if d % 2 == 0 and c <= self.limit[way]]

    def key(self, way, d):
        return d - 1 if way == 1 else self.limit[1] + d - 1

    def arrivals(self, t):
        return [(w, d) for d in (2 * t - 1, 2 * t) for w in (1, -1) if d <= self.limit[w]]

    def drain(self):
        take_bytes(self.ref, self.nz * NY - 1, self.ssem)


class PlaneZY(Plane):
    def hand_on(self, way, d):
        for c in self.next_of(way, d):
            self.copy(self.slot(-way * d, 0), self.slot(way * (c - d), 0), self.zsem.at[self.key(way, c)]).start()

    def spread(self, slot, t, way):
        if NY == 2:
            self.copy(slot, self.slot(0, 1), self.ysem.at[t, 2]).start()
            return
        self.copy(slot, self.slot(0, 1), self.ysem.at[t, 0 if way == 1 else 2]).start()
        self.copy(slot, self.slot(0, -1), self.ysem.at[t, 2 if way == 1 else 1]).start()

    def start(self):
        self.hand_on(1, 0)
        self.hand_on(-1, 0)
        self.spread(self.sp, 0, 1)

    def step(self, t):
        for way, d in self.arrivals(t):
            slot = self.slot(-way * d, 0)
            self.copy(slot, self.sp, self.zsem.at[self.key(way, d)]).wait_recv()
            self.hand_on(way, d)
            self.spread(slot, t, way)

    def relay(self, t):
        if NY == 2 or t > self.steps:
            return
        for way in (1, -1):
            found = [d for w, d in (self.arrivals(t) if t else [(1, 0)]) if w == way]
            if found:
                take_bytes(self.ref, len(found), self.ysem.at[t, 0 if way == 1 else 1])
            for d in found:
                self.copy(self.slot(-way * d, -way), self.slot(0, way), self.ysem.at[t, 2]).start()

    def finish(self, first, last):
        for t in range(first, last + 1):
            count = len(self.arrivals(t)) if t else 1
            take_bytes(self.ref, count * (1 if NY == 2 else 2), self.ysem.at[t, 2])


class PlaneYZ(Plane):
    def hand_on(self, way, d, j):
        for c in self.next_of(way, d):
            sem = self.zsem.at[self.key(way, c), j]
            self.copy(self.slot(-way * d, -j), self.slot(way * (c - d), 0), sem).start()

    def start(self):
        for d in range(1, NY):
            self.copy(self.sp, self.slot(0, d), self.ysem.at[d - 1]).start()
        self.hand_on(1, 0, 0)
        self.hand_on(-1, 0, 0)

    def begin(self):
        for j in range(1, NY):
            self.copy(self.slot(0, -j), self.sp, self.ysem.at[j - 1]).wait_recv()
            self.hand_on(1, 0, j)
            self.hand_on(-1, 0, j)

    def step(self, t):
        for way, d in self.arrivals(t):
            for j in range(NY):
                slot = self.slot(-way * d, -j)
                self.copy(slot, self.sp, self.zsem.at[self.key(way, d), j]).wait_recv()
                self.hand_on(way, d, j)


class Scan:
    def __init__(self, nz, left, gap, dext, lout, qx, into, key, cum, stb, decb, ys, yd, zb, zdb, zs, zd, ib, sems):
        self.nz = nz
        self.left, self.gap, self.dext, self.lout, self.qx, self.into = left, gap, dext, lout, qx, into
        self.key, self.cum = key, cum
        self.stb, self.decb, self.ys, self.yd = stb, decb, ys, yd
        self.zb, self.zdb, self.zs, self.zd, self.ib = zb, zdb, zs, zd, ib
        self.ys_s, self.ys_r, self.yd_s, self.yd_r, self.zs_s, self.zs_r, self.zd_s, self.zd_r, self.i_s, self.i_r = sems
        self.sp = lax.axis_index("sp")
        self.z, self.y = self.sp // NY, lax.rem(self.sp, NY)
        self.vs = HEAD // NY

    def at_y(self, d):
        return self.z * NY + self.other(d)

    def other(self, d):
        return lax.rem(self.y + d + NY, NY)

    def rows(self, ref, j):
        return ref.at[:, pl.ds(pl.multiple_of(j * self.vs, self.vs), self.vs), :]

    def prepare(self):
        toks = self.left.shape[0]
        pre = self.left[:, 256:512].astype(F32)
        key = self.gap[...] * (1.0 / (1.0 + jnp.exp(pre)))
        series = jnp.full(key.shape, 1.0 / 11.0, F32)
        for n in range(10, 0, -1):
            series = series * key + 1.0 / n
        extra = [jnp.transpose(jnp.broadcast_to(self.dext[h : h + 1, :], (HEAD, toks))) for h in range(2)]
        logf = jnp.concatenate(extra, axis=1) - series * key
        rows = lax.broadcasted_iota(jnp.int32, (toks, toks), 0)
        lower = jnp.where(rows >= lanes_of((toks, toks)), 1.0, 0.0).astype(F32)
        cum = jnp.dot(lower, logf, preferred_element_type=F32, precision=lax.Precision.HIGHEST)
        self.key[...] = key
        self.cum[...] = cum

    def states(self):
        toks = self.left.shape[0]
        for h in range(2):
            cols = slice(HEAD * h, HEAD * (h + 1))
            c, k = self.cum[:, cols], self.key[:, cols]
            v = self.left[:, 512 + HEAD * h : 512 + HEAD * (h + 1)]
            last = c[toks - 1 : toks]
            self.stb[h] = dotg(v, (k * jnp.exp(last - c)).astype(BF16), TN).astype(BF16)
            self.decb[h : h + 1, :] = jnp.exp(last)
        for d in range(1, NY):
            for c in self.ycopy(d):
                c.start()

    def inside(self):
        toks = self.left.shape[0]
        half = toks // 2
        tri = lax.broadcasted_iota(jnp.int32, (half, half), 0) >= lanes_of((half, half))
        self.qx[...] = (self.left[:, 0:256].astype(F32) * jnp.exp(self.cum[...])).astype(BF16)
        for h in range(2):
            cols = slice(HEAD * h, HEAD * (h + 1))
            c, k = self.cum[:, cols], self.key[:, cols]
            q = self.left[:, cols].astype(F32)
            v = self.left[:, 512 + HEAD * h : 512 + HEAD * (h + 1)]
            edge = c[half - 1 : half]
            outs = []
            for b in range(2):
                r = slice(half * b, half * (b + 1))
                mid = c[half * b + half // 2 - 1 : half * b + half // 2]
                qd = (q[r] * jnp.exp(c[r] - mid)).astype(BF16)
                kd = (k[r] * jnp.exp(mid - c[r])).astype(BF16)
                a = jnp.where(tri, dotg(qd, kd, NT), 0.0).astype(BF16)
                outs.append(dot(a, v[r]))
            s0 = dotg(v[:half], (k[:half] * jnp.exp(edge - c[:half])).astype(BF16), TN)
            qe = (q[half:] * jnp.exp(c[half:] - edge)).astype(BF16)
            self.lout[0:half, cols] = outs[0]
            self.lout[half:toks, cols] = outs[1] + dotg(qe, s0.astype(BF16), NT)

    def ycopy(self, d):
        mine = self.rows(self.stb, self.other(d))
        dev = {"sp": self.at_y(d)}
        return (
            remote(mine, self.ys.at[self.y], self.ys_s.at[d - 1], self.ys_r.at[d - 1], dev),
            remote(self.decb, self.yd.at[self.y], self.yd_s.at[d - 1], self.yd_r.at[d - 1], dev),
        )

    def join_y(self):
        dev = {"sp": self.sp}
        y, ys, yd = self.y, self.ys, self.yd
        for h in range(2):
            ys[y, h] = self.stb[h, pl.ds(pl.multiple_of(y * self.vs, self.vs), self.vs), :]
        yd[y] = self.decb[...]
        for d in range(1, NY):
            src = self.other(-d)
            remote(ys.at[src], ys.at[src], self.ys_s.at[d - 1], self.ys_r.at[d - 1], dev).wait_recv()
            remote(yd.at[src], yd.at[src], self.yd_s.at[d - 1], self.yd_r.at[d - 1], dev).wait_recv()
        state = [jnp.zeros((self.vs, HEAD), F32) for _ in range(2)]
        span = [jnp.ones((1, HEAD), F32) for _ in range(2)]
        for j in range(NY):
            for h in range(2):
                decay = yd[j, h : h + 1, :]
                state[h] = decay * state[h] + ys[j, h].astype(F32)
                span[h] = span[h] * decay
        for h in range(2):
            self.zb[h] = state[h].astype(BF16)
            self.zdb[h : h + 1, :] = span[h]
        for d in range(self.nz - 1, 0, -1):

            @pl.when(self.z + d < self.nz)
            def _():
                for c in self.zcopy(d):
                    c.start()

    def zcopy(self, d):
        dev = {"sp": (self.z + d) * NY + self.y}
        return (
            remote(self.zb, self.zs.at[self.z], self.zs_s.at[d - 1], self.zs_r.at[self.z], dev),
            remote(self.zdb, self.zd.at[self.z], self.zd_s.at[d - 1], self.zd_r.at[self.z], dev),
        )

    def join_z(self):
        zs, zd, ys, yd = self.zs, self.zd, self.ys, self.yd
        dev = {"sp": self.sp}

        def earlier(j, carry):
            remote(zs.at[j], zs.at[j], self.zs_s.at[0], self.zs_r.at[j], dev).wait_recv()
            remote(zd.at[j], zd.at[j], self.zd_s.at[0], self.zd_r.at[j], dev).wait_recv()
            return tuple(zd[j, h : h + 1, :] * carry[h] + zs[j, h].astype(F32) for h in range(2))

        zero = jnp.zeros((self.vs, HEAD), F32)
        state = list(lax.fori_loop(0, self.z, earlier, (zero, zero)))
        for j in range(NY):
            for h in range(2):
                self.ib[j, h] = state[h].astype(BF16)
                state[h] = yd[j, h : h + 1, :] * state[h] + ys[j, h].astype(F32)
        for d in range(1, NY):
            self.icopy(d).start()
        for h in range(2):
            spot = pl.ds(pl.multiple_of(self.y * self.vs, self.vs), self.vs)
            self.into[h, spot, :] = self.ib[self.y, h]

    def icopy(self, d):
        spot = self.rows(self.into, self.y)
        return remote(self.ib.at[self.other(d)], spot, self.i_s.at[d - 1], self.i_r.at[d - 1], {"sp": self.at_y(d)})

    def finish(self):
        for d in range(1, NY):
            spot = self.rows(self.into, self.other(-d))
            remote(spot, spot, self.i_s.at[d - 1], self.i_r.at[d - 1], {"sp": self.sp}).wait_recv()

    def drain(self):
        for d in range(1, NY):
            for c in self.ycopy(d):
                c.wait_send()
            self.icopy(d).wait_send()
        for d in range(1, self.nz):

            @pl.when(self.z + d < self.nz)
            def _():
                for c in self.zcopy(d):
                    c.wait_send()


def mixer_kernel(
    nz, nx, hid, wq, wf, wi, wqdt, wkvdt, wkrt, wku, wvu, wqn, wqrt, qg, kvg, kcos, ksin, qcos, qsin,
    gap, dext, gain, worh, woah, out,
    hall, wa, wb, wc, rall, racc, wrt, left, qn, lat, kvw, qw, wor, woa,
    lout, qx, into, key, cum, stb, decb, ys, yd, zb, zdb, zs, zd, ib,
    krope, qblk, msc, acc, obuf, sbuf, orecv, srecv, mixed, pairs, got_pair, sums, got,
    loc, hs, hr, ks, kr, qs, qr, rs, rr, was, waz, way_, wbs, wbz, wby, wcs, wcz, wcy, ls, lz, ly,
    ys_s, ys_r, yd_s, yd_r, zs_s, zs_r, zd_s, zd_r, i_s, i_r,
    o_s, o_r, s_s, s_r, p_s, p_r, f_s, f_r,
):
    tpn, spn = 2 * nx, nz * NY
    tp, sp = lax.axis_index("tp"), lax.axis_index("sp")
    x, core = tp // 2, lax.rem(tp, 2)
    toks, feat = hid.shape
    tt = toks // tpn
    line_h, line_k = Line(hall, hs, hr, nx), Line(kvw, ks, kr, nx)
    line_q, line_r = Line(qw, qs, qr, nx), Line(rall, rs, rr, nx)
    plane_a = PlaneYZ(wa, was, waz, way_, nz)
    plane_b = PlaneZY(wb, wbs, wbz, wby, nz)
    plane_c = PlaneYZ(wc, wcs, wcz, wcy, nz)
    plane_l = PlaneZY(lat, ls, lz, ly, nz)
    sems = (ys_s, ys_r, yd_s, yd_r, zs_s, zs_r, zd_s, zd_r, i_s, i_r)
    scan = Scan(nz, left, gap, dext, lout, qx, into, key, cum, stb, decb, ys, yd, zb, zdb, zs, zd, ib, sems)

    barrier = pltpu.get_barrier_semaphore()
    greet = [{"tp": lax.rem(tp + d, tpn)} for d in range(1, tpn)]
    greet += [{"sp": plane_a.slot(0, d)} for d in range(1, NY)]
    near = [d for d in range(1, nz) if FULL_GREET or d <= 2 or d >= nz - 2]
    greet += [{"sp": plane_a.slot(d, 0)} for d in near]
    for dev in greet:
        pl.semaphore_signal(barrier, inc=1, device_id=dev, device_id_type=MESH)

    own = [
        pltpu.make_async_copy(hid, hall.at[tp], loc.at[0]),
        pltpu.make_async_copy(wf.at[:, pl.ds(0, 128)], wa.at[sp], loc.at[1]),
        pltpu.make_async_copy(wf.at[:, pl.ds(128, 128)], wb.at[sp, :, pl.ds(0, 128)], loc.at[2]),
        pltpu.make_async_copy(wi, wb.at[sp, :, pl.ds(128, 256)], loc.at[3]),
        pltpu.make_async_copy(wq, wc.at[sp], loc.at[8]),
        pltpu.make_async_copy(wku, kvw.at[tp, :, pl.ds(0, 128)], loc.at[4]),
        pltpu.make_async_copy(wvu, kvw.at[tp, :, pl.ds(128, 128)], loc.at[5]),
    ]
    late = [pltpu.make_async_copy(worh, wor, loc.at[6]), pltpu.make_async_copy(woah, woa, loc.at[7])]
    for c in own + late:
        c.start()
    wrt[0:64, :] = wqdt[...]
    wrt[64:96, :] = wkvdt[...]
    wrt[96:128, :] = wkrt[...]
    for c in own:
        c.wait()
    pl.semaphore_wait(barrier, len(greet))

    line_h.start()
    plane_a.start()
    plane_b.start()
    line_k.start()
    qw[tp, 0:128, :] = jnp.transpose(wqn[...].astype(F32)).astype(BF16)
    qw[tp, 128:192, :] = wqrt[...]
    qblk[...] = jnp.zeros(qblk.shape, BF16)
    plane_a.begin()

    def wstep(t):
        plane_b.step(t)
        plane_a.step(t)

    def lora():
        line_h.finish()
        acc = None
        for i in range(tpn):
            part = dotg(hall[i], wrt[:, i * feat : (i + 1) * feat], NT)
            acc = part if acc is None else acc + part
        rall[tp] = acc.astype(BF16)
        line_r.start()
        line_q.start()
        racc[...] = acc
        mine = racc[pl.ds(pl.multiple_of(tp * tt, tt), tt), :]
        lane = lanes_of((tt, 128))
        other = jnp.where(
            lax.rem(lane, 32) < 16, pltpu.roll(mine, 128 - 16, 1), pltpu.roll(mine, 16, 1)
        )
        turned = mine * kcos[...] + other * ksin[...]
        quart = tt // 4
        lane = lanes_of((quart, 128))
        packed = jnp.zeros((quart, 128), F32)
        for g in range(4):
            rows = turned[g * quart : (g + 1) * quart]
            moved = pltpu.roll(rows, 32 * (g + 1), 1) if g < 3 else rows
            packed = jnp.where((lane >= 32 * g) & (lane < 32 * (g + 1)), moved, packed)
        lat[sp, 2 * tt : 2 * tt + quart, :] = packed.astype(BF16)

    def latents():
        line_r.finish()
        first = pl.multiple_of(tp * tt, tt)
        lane = lanes_of((tt, 128))
        tiles = []
        total = jnp.zeros((tt, 128), F32)
        width = 32 * tpn
        for j in range(2):
            tile = jnp.zeros((tt, 128), F32)
            for k in range(4):
                if 4 * j + k >= tpn:
                    continue
                piece = rall[4 * j + k, pl.ds(first, tt), :].astype(F32)
                moved = pltpu.roll(piece, (32 * k - 64) % 128, 1) if k != 2 else piece
                tile = jnp.where((lane >= 32 * k) & (lane < 32 * (k + 1)), moved, tile)
            tiles.append(tile)
            total = total + tile * tile
        scale = lax.rsqrt(jnp.sum(total, axis=1, keepdims=True) / width + NORM_EPS)
        for j in range(2):
            cols = slice(128 * j, 128 * (j + 1))
            lat[sp, j * tt : (j + 1) * tt, :] = (tiles[j] * scale * kvg[:, cols]).astype(BF16)

    def queries():
        lane = lanes_of((toks, 128))
        total = jnp.zeros((toks, 128), F32)
        for i in range(tpn):
            piece = rall[i].astype(F32)
            total = total + jnp.where(lane < 64, piece * piece, 0.0)
        width = 64 * tpn
        scale = lax.rsqrt(jnp.sum(total, axis=1, keepdims=True) / width + NORM_EPS)
        for j in range(width // 128):
            one, two = rall[2 * j].astype(F32), rall[2 * j + 1].astype(F32)
            tile = jnp.where(lane < 64, one, pltpu.roll(two, 64, 1))
            cols = slice(128 * j, 128 * (j + 1))
            qn[:, cols] = (tile * scale * qg[:, cols]).astype(BF16)

    def project(blocks, at):
        spans = spn // tpn
        acc = None
        for i in range(tpn):
            block = [w[i * spans : (i + 1) * spans, :, n : n + m].reshape(feat, m) for w, n, m in blocks]
            block = block[0] if len(block) == 1 else jnp.concatenate(block, axis=1)
            part = dot(hall[i], block)
            acc = part if acc is None else acc + part
        left[:, at : at + 256] = acc.astype(BF16)

    jobs = {
        1: [line_h.forward],
        2: [line_h.forward_far, lora],
        3: [line_k.forward, line_r.forward],
        4: [line_k.forward_far, line_r.forward_far, latents, plane_l.start, queries],
    }
    for t in range(1, max(plane_a.steps, 4) + 1):
        if t <= plane_a.steps:
            wstep(t)
        plane_b.relay(t - 1)
        for job in jobs.get(t, []):
            job()
    for t in range(max(plane_a.steps, 4), plane_b.steps + 1):
        plane_b.relay(t)
    plane_b.finish(0, plane_b.steps)
    project([(wa, 0, 128), (wb, 0, 128)], 256)
    project([(wb, 128, 256)], 512)
    scan.prepare()
    scan.states()
    steps = plane_l.steps

    def lstep(t):
        if t <= steps:
            plane_l.step(t)

    def cstep(t):
        if t <= steps:
            plane_c.step(t)

    lstep(1)
    plane_l.relay(0)
    plane_c.start()
    line_q.forward()
    lstep(2)
    plane_l.relay(1)
    plane_c.begin()
    scan.join_y()
    line_q.forward_far()
    lstep(3)
    plane_l.relay(2)
    cstep(1)
    line_k.finish()
    line_q.finish()

    per = CHUNK // tt
    deep = per // NY
    chunks = spn // per
    base2 = math.log2(math.e) / math.sqrt(NOPE + ROPE)
    own_chunk = sp // per
    z = sp // NY

    def sent(p):
        dev = {"tp": p}
        return (
            remote(obuf.at[p], orecv.at[tp], o_s.at[p], o_r.at[tp], dev),
            remote(sbuf.at[p], srecv.at[tp], s_s.at[p], s_r.at[tp], dev),
        )

    def turn(p, _):
        q = dotg(qw[p], qn[...], NT)
        for h in range(2):
            c = slice(h * toks, (h + 1) * toks)
            qblk[p, 64 * h : 64 * (h + 1), c] = q[64 * h : 64 * (h + 1)].astype(BF16)
            a, b = q[128 + 32 * h : 144 + 32 * h], q[144 + 32 * h : 160 + 32 * h]
            qblk[p, 128:144, c] = (a * qcos[...] - b * qsin[...]).astype(BF16)
            qblk[p, 144:160, c] = (a * qsin[...] + b * qcos[...]).astype(BF16)
        return 0

    quart = tt // 4

    def unpack(j):
        rows = lat[pl.ds(j * per, per), 2 * tt : 2 * tt + quart, :].astype(F32)
        lane = lanes_of(rows.shape)
        parts = [
            jnp.where(lane < 32, pltpu.roll(rows, 128 - 32 * g, 2) if g else rows, 0.0)
            for g in range(4)
        ]
        whole = jnp.stack(parts, axis=1).reshape(CHUNK, 128)
        krope[pl.ds(pl.multiple_of(j * CHUNK, CHUNK), CHUNK), :] = whole.astype(BF16)

    def chunk(p, j, opening):
        tiles = kvw.shape[1] // 128
        part = [lat[pl.ds(j * per, per), i * tt : (i + 1) * tt, :].reshape(CHUNK, 128) for i in range(tiles)]
        part = part[0] if tiles == 1 else jnp.concatenate(part, axis=1)
        kv = dot(part, kvw[p])
        turned = krope[pl.ds(pl.multiple_of(j * CHUNK, CHUNK), CHUNK), :]
        keys = jnp.concatenate([kv[:, :128].astype(BF16), turned], axis=1)
        vals = jnp.transpose(kv[:, 128:]).astype(BF16)
        vals = jnp.concatenate([vals, jnp.ones((16, CHUNK), BF16)], axis=0)
        for h in range(2):
            c = slice(h * toks, (h + 1) * toks)
            s = dot(keys, qblk[p, :, c])
            if opening:
                at = lax.broadcasted_iota(jnp.int32, (CHUNK, toks), 0)
                kpos = (j * per + at // tt) * toks + tp * tt + lax.rem(at, tt)
                ok = kpos <= sp * toks + lanes_of((CHUNK, toks))
                s = jnp.where(ok, s, NEG_BIG)
                new = jnp.max(s, axis=0, keepdims=True)
                w = jnp.where(ok, jnp.exp2((s - new) * base2), 0.0)
                acc[p, :, c] = dot(vals, w.astype(BF16))
            else:
                old = msc[p, 0:1, c]
                new = jnp.maximum(old, jnp.max(s, axis=0, keepdims=True))
                w = jnp.exp2((s - new) * base2)
                fade = jnp.exp2((old - new) * base2)
                acc[p, :, c] = acc[p, :, c] * fade + dot(vals, w.astype(BF16))
            msc[p, 0:1, c] = new

    def reach(j):
        far = None
        for i in range(deep):
            d = z - (j * deep + i)
            d = jnp.where(d <= nz // 2, d, nz - d)
            far = d if far is None else jnp.maximum(far, d)
        return far

    def each(lo, hi, todo):
        @pl.loop(0, chunks)
        def _(j):
            far = reach(j)

            @pl.when((j < own_chunk) & (far > lo) & (far <= hi))
            def _():
                todo(j)

    def opened(p, _):
        chunk(p, own_chunk, True)
        return 0

    def close(i, _):
        p = lax.rem(tp + 1 + i, tpn)
        each(middle, nz, lambda j: chunk(p, j, False))
        for h in range(2):
            c = slice(h * toks, (h + 1) * toks)
            total = acc[p, 128:129, c]
            some = total > 0.0
            safe = jnp.where(some, total, 1.0)
            obuf[p, 64 * h : 64 * (h + 1), :] = (acc[p, 64 * h : 64 * (h + 1), c] / safe).astype(BF16)
            sbuf[p, h : h + 1, :] = jnp.where(some, msc[p, 0:1, c] * base2 + jnp.log2(safe), NEG_BIG)

        @pl.when(i < tpn - 1)
        def _():
            for c in sent(p):
                c.start()

        return 0

    def early(j):
        unpack(j)

        @pl.loop(0, tpn)
        def _(p):
            chunk(p, j, False)

    lax.fori_loop(0, tpn, turn, 0)
    half = tpn // 2
    first, second = min(2, steps), min(3, steps)
    middle = 2 * second if second > first else 0
    plane_l.finish(0, first)
    unpack(own_chunk)
    lax.fori_loop(0, half, opened, 0)
    lstep(4)
    plane_l.relay(3)
    cstep(2)
    lax.fori_loop(half, tpn, opened, 0)
    plane_l.relay(4)
    cstep(3)
    plane_l.finish(first + 1, second)
    if middle:
        each(0, middle, early)
    cstep(4)
    plane_l.finish(second + 1, steps)
    each(middle, nz, unpack)
    lax.fori_loop(0, half + 1, close, 0)
    scan.join_z()
    lax.fori_loop(half + 1, tpn, close, 0)
    orecv[tp] = obuf[tp]
    srecv[tp] = sbuf[tp]
    project([(wc, 0, 256)], 0)
    scan.inside()

    scan.finish()
    cols = []
    for h in range(2):
        c = slice(HEAD * h, HEAD * (h + 1))
        raw = lout[:, c] + dotg(qx[:, c], into[h], NT)
        norm = lax.rsqrt(jnp.mean(raw * raw, axis=1, keepdims=True) + NORM_EPS)
        cols.append((raw * norm * gain[...]).astype(BF16))
    rec = jnp.concatenate(cols, axis=1)
    for c in late:
        c.wait()
    width = wor.shape[1]
    step = got.shape[3]
    for n in range(0, width, step):
        mixed[:, n : n + step] = dot(rec, wor[:, n : n + step])

    for d in range(1, tpn):
        src = lax.rem(tp + d, tpn)
        dev = {"tp": tp}
        remote(orecv.at[src], orecv.at[src], o_s.at[src], o_r.at[src], dev).wait_recv()
        remote(srecv.at[src], srecv.at[src], s_s.at[src], s_r.at[src], dev).wait_recv()
    halves = []
    for h in range(2):
        lse = [srecv[i, h : h + 1, :] for i in range(tpn)]
        top = functools.reduce(jnp.maximum, lse)
        total = jnp.zeros((1, toks), F32)
        merged = jnp.zeros((64, toks), F32)
        for i in range(tpn):
            weight = jnp.exp2(lse[i] - top)
            total = total + weight
            merged = merged + weight * orecv[i, 64 * h : 64 * (h + 1), :].astype(F32)
        halves.append((merged / total).astype(BF16))
    att = jnp.concatenate(halves, axis=0)

    sib = x * 2 + 1 - core

    def to_sib(k):
        return remote(pairs.at[k], got_pair.at[k], p_s.at[k], p_r.at[k], {"tp": sib})

    for k in range(width // step):
        n = slice(k * step, (k + 1) * step)
        mixed[:, n] += dotg(att, woa[:, n], TN)
        for i in range(nx):
            first = pl.multiple_of((2 * i + 1 - core) * tt, tt)
            pairs[k, i] = mixed[pl.ds(first, tt), n].astype(BF16)
        to_sib(k).start()

    def mine(i, k):
        first = pl.multiple_of((2 * i + core) * tt, tt)
        return mixed[pl.ds(first, tt), k * step : (k + 1) * step] + got_pair[k, i].astype(F32)

    def final(k, n):
        way = 1 if k % 2 == 0 else -1
        to = lax.rem(x + (-way if n == 1 else way) + nx, nx) * 2 + core
        return remote(sums.at[k, n], got.at[k, n], f_s.at[k, n], f_r.at[k, n], {"tp": to})

    pieces = range(width // step)
    kinds = [0, 1, 2] if nx > 2 else [0]
    for k in pieces:
        way = 1 if k % 2 == 0 else -1
        to_sib(k).wait_recv()
        if nx > 2:
            sums[k, 2] = mine(lax.rem(x + 2, nx), k).astype(BF16)
            final(k, 2).start()
            sums[k, 1] = mine(lax.rem(x - way + nx, nx), k).astype(BF16)
            final(k, 1).start()
    for k in pieces:
        way = 1 if k % 2 == 0 else -1
        passed = mine(lax.rem(x + way + nx, nx), k)
        if nx > 2:
            final(k, 2).wait_recv()
            passed = passed + got[k, 2].astype(F32)
        sums[k, 0] = passed.astype(BF16)
        final(k, 0).start()
    for k in pieces:
        total = mine(x, k)
        for n in kinds[:2]:
            final(k, n).wait_recv()
            total = total + got[k, n].astype(F32)
        out[:, k * step : (k + 1) * step] = total.astype(BF16)
    for k in pieces:
        to_sib(k).wait_send()
        for n in kinds:
            final(k, n).wait_send()
    for d in range(1, tpn):
        for c in sent(lax.rem(tp + d, tpn)):
            c.wait_send()
    for part in (line_h, line_k, line_q, line_r, plane_a, plane_b, plane_c, plane_l, scan):
        part.drain()


def shards(
    nz, nx,
    hidden_in, w_query_rec, w_forget, w_input, forget_gap, decay_extra, rec_gain,
    w_q_down, w_kv_down, w_key_rope, q_gain, kv_gain, w_q_nope, w_q_rope, w_k_up, w_v_up,
    w_out_rec, w_out_att,
):
    tpn, spn = 2 * nx, nz * NY
    toks, feat = hidden_in.shape
    tt = toks // tpn
    rw = w_query_rec.shape[0]
    qrank = w_q_down.shape[1] * tpn
    kvrank = w_k_up.shape[0]
    width = w_out_rec.shape[1]
    sp, tp = lax.axis_index("sp"), lax.axis_index("tp")

    frequency = 1.0 / ROPE_BASE ** (jnp.arange(0, ROPE, 2, dtype=F32) / ROPE)
    position = (sp * toks + jnp.arange(toks)).astype(F32)
    angle = frequency[:, None] * position[None, :]
    qcos, qsin = jnp.cos(angle), jnp.sin(angle)
    keyed = (sp * toks + tp * tt + jnp.arange(tt)).astype(F32)
    angle = keyed[:, None] * jnp.tile(frequency, 8)[None, :]
    sign = jnp.where(jnp.arange(128) % 32 < 16, -1.0, 1.0).astype(F32)
    kcos, ksin = jnp.cos(angle), jnp.sin(angle) * sign[None, :]
    kvg = jnp.pad(kv_gain, (0, 256 - kv_gain.shape[0]))

    vs = HEAD // NY
    step = width // SPLIT
    line = [DMA(()), DMA((2 * nx,))]
    far = 3
    scratch = [
        VM((tpn, toks, feat), BF16),
        VM((spn, rw, 128), BF16),
        VM((spn, rw, 384), BF16),
        VM((spn, rw, 256), BF16),
        VM((tpn, toks, 128), BF16),
        VM((toks, 128), F32),
        VM((128, tpn * feat), BF16),
        VM((toks, 768), BF16),
        VM((toks, qrank), BF16),
        VM((spn, 2 * tt + tt // 4, 128), BF16),
        VM((tpn, kvrank, 256), BF16),
        VM((tpn, 192, qrank), BF16),
        VM(w_out_rec.shape, BF16),
        VM(w_out_att.shape, BF16),
        VM((toks, 256), F32),
        VM((toks, 256), BF16),
        VM((2, HEAD, HEAD), BF16),
        VM((toks, 256), F32),
        VM((toks, 256), F32),
        VM((2, HEAD, HEAD), BF16),
        VM((8, HEAD), F32),
        VM((NY, 2, vs, HEAD), BF16),
        VM((NY, 8, HEAD), F32),
        VM((2, vs, HEAD), BF16),
        VM((8, HEAD), F32),
        VM((nz, 2, vs, HEAD), BF16),
        VM((nz, 8, HEAD), F32),
        VM((NY, 2, vs, HEAD), BF16),
        VM((spn * tt, 128), BF16),
        VM((tpn, 256, 2 * toks), BF16),
        VM((tpn, 8, 2 * toks), F32),
        VM((tpn, 144, 2 * toks), F32),
        VM((tpn, 128, toks), BF16),
        VM((tpn, 8, toks), F32),
        VM((tpn, 128, toks), BF16),
        VM((tpn, 8, toks), F32),
        VM((toks, width), F32),
        VM((SPLIT, nx, tt, step), BF16),
        VM((SPLIT, nx, tt, step), BF16),
        VM((SPLIT, far, tt, step), BF16),
        VM((SPLIT, far, tt, step), BF16),
        DMA((9,)),
        *line, *line, *line, *line,
        DMA(()), DMA((nz - 1, NY)), DMA((NY - 1,)),
        DMA(()), DMA((nz - 1,)), DMA((nz // 4 + 1, 3)),
        DMA(()), DMA((nz - 1, NY)), DMA((NY - 1,)),
        DMA(()), DMA((nz - 1,)), DMA((nz // 4 + 1, 3)),
        *([DMA((NY - 1,))] * 4),
        DMA((nz - 1,)), DMA((nz,)), DMA((nz - 1,)), DMA((nz,)),
        *([DMA((NY - 1,))] * 2),
        *([DMA((tpn,))] * 4),
        *([DMA((SPLIT,))] * 2),
        *([DMA((SPLIT, far))] * 2),
    ]
    args = (
        hidden_in, w_query_rec, w_forget, w_input, w_q_down.T, w_kv_down.T, w_key_rope.T,
        w_k_up, w_v_up, w_q_nope, w_q_rope.T, q_gain[None], kvg[None], kcos, ksin, qcos, qsin,
        forget_gap[None], decay_extra.T, rec_gain[None], w_out_rec, w_out_att,
    )
    whole, anywhere = pl.BlockSpec(memory_space=VM), pl.BlockSpec(memory_space=pl.ANY)
    return pl.pallas_call(
        functools.partial(mixer_kernel, nz, nx),
        out_shape=jax.ShapeDtypeStruct((tt, width), BF16),
        in_specs=[whole] * (len(args) - 2) + [anywhere] * 2,
        out_specs=whole,
        scratch_shapes=scratch,
        compiler_params=pltpu.CompilerParams(
            collective_id=0, has_side_effects=True, vmem_limit_bytes=60 * 2**20
        ),
        name="mixer",
    )(*args)


def solution(mesh):
    placed = (
        P("sp", "tp"),
        P("sp", "tp"),
        P("sp", "tp"),
        P("sp", "tp"),
        P("tp"),
        P("sp", "tp"),
        P(),
        P(None, "tp"),
        P(None, "tp"),
        P(),
        P(),
        P(),
        P(None, "tp"),
        P(None, "tp"),
        P(None, "tp"),
        P(None, "tp"),
        P("tp", None),
        P("tp", None),
    )
    nz, nx = mesh.shape["sp"] // NY, mesh.shape["tp"] // 2
    return jax.shard_map(
        functools.partial(shards, nz, nx),
        mesh=mesh,
        in_specs=placed,
        out_specs=P(("sp", "tp"), None),
        check_vma=False,
    )
```

```python
import functools
import math

import jax
import jax.numpy as jnp
from jax import lax
from jax.experimental import pallas as pl
from jax.experimental.pallas import tpu as pltpu
from jax.sharding import PartitionSpec as P

HEAD = 128
NOPE = 64
ROPE = 32
NORM_EPS = 1e-06
ROPE_BASE = 10000.0
NEG_BIG = -1e30
NY = 4
CHUNK = 512
SPLIT = 4
MESH = pl.DeviceIdType.MESH
F32 = jnp.float32
BF16 = jnp.bfloat16
NT = (((1,), (1,)), ((), ()))
TN = (((0,), (0,)), ((), ()))
VM = pltpu.VMEM
DMA = pltpu.SemaphoreType.DMA


def dot(a, b):
    return jnp.dot(a, b, preferred_element_type=F32)


def dotg(a, b, dims):
    return lax.dot_general(a, b, dims, preferred_element_type=F32)


def remote(src, dst, ssem, rsem, dev):
    return pltpu.make_async_remote_copy(
        src_ref=src, dst_ref=dst, send_sem=ssem, recv_sem=rsem, device_id=dev, device_id_type=MESH
    )


def take_bytes(ref, count, sem):
    part = ref.at[pl.ds(0, count)]
    pltpu.make_async_copy(part, part, sem).wait()


def lanes_of(shape):
    return lax.broadcasted_iota(jnp.int32, shape, len(shape) - 1)


class Line:
    def __init__(self, ref, ssem, rsem, nx):
        self.ref, self.ssem, self.rsem, self.nx = ref, ssem, rsem, nx
        tp = lax.axis_index("tp")
        self.tp, self.core, self.x = tp, lax.rem(tp, 2), tp // 2
        self.sib = self.x * 2 + 1 - self.core

    def at_x(self, dx):
        return lax.rem(self.x + dx + self.nx, self.nx) * 2 + self.core

    def copy(self, slot, to, k):
        piece = self.ref.at[slot]
        return remote(piece, piece, self.ssem, self.rsem.at[k], {"tp": to})

    def start(self):
        for d in range(1, self.nx):
            self.copy(self.tp, self.at_x(d), d - 1).start()
        self.copy(self.tp, self.sib, self.nx - 1).start()

    def forward(self):
        for d in range(1, self.nx):
            slot = self.at_x(-d)
            self.copy(slot, self.tp, d - 1).wait_recv()
            self.copy(slot, self.sib, self.nx - 1 + d).start()

    def finish(self):
        for d in range(self.nx):
            x = lax.rem(self.x - d + self.nx, self.nx)
            self.copy(x * 2 + 1 - self.core, self.tp, self.nx - 1 + d).wait_recv()

    def drain(self):
        take_bytes(self.ref, 2 * self.nx - 1, self.ssem)


class Plane:
    jump = 2

    def __init__(self, ref, ssem, zsem, ysem, nz):
        self.ref, self.ssem, self.zsem, self.ysem, self.nz = ref, ssem, zsem, ysem, nz
        self.sp = lax.axis_index("sp")
        self.z, self.y = self.sp // NY, lax.rem(self.sp, NY)
        self.limit = {1: nz // 2, -1: nz // 2 - 1}
        self.steps = -(-(nz // 2) // self.jump)

    def slot(self, dz, dy):
        z = lax.rem(self.z + dz + self.nz, self.nz)
        return z * NY + lax.rem(self.y + dy + NY, NY)

    def copy(self, slot, to, sem):
        piece = self.ref.at[slot]
        return remote(piece, piece, self.ssem, sem, {"sp": to})

    def next_of(self, way, d):
        ahead = [d + self.jump] + [d + i for i in range(1, self.jump)]
        return [c for c in ahead if d % self.jump == 0 and c <= self.limit[way]]

    def key(self, way, d):
        return d - 1 if way == 1 else self.limit[1] + d - 1

    def arrivals(self, t):
        top = self.jump * t
        order = [top - 1, top] if self.jump == 2 else [top - 3, top - 2, top, top - 1]
        return [(w, d) for d in order for w in (1, -1) if d <= self.limit[w]]

    def drain(self):
        take_bytes(self.ref, self.nz * NY - 1, self.ssem)


class PlaneZY(Plane):
    jump = 4

    def hand_on(self, way, d):
        for c in self.next_of(way, d):
            self.copy(self.slot(-way * d, 0), self.slot(way * (c - d), 0), self.zsem.at[self.key(way, c)]).start()

    def spread(self, slot, t):
        for d in range(1, NY):
            self.copy(slot, self.slot(0, d), self.ysem.at[t]).start()

    def start(self):
        self.hand_on(1, 0)
        self.hand_on(-1, 0)
        self.spread(self.sp, 0)

    def step(self, t):
        for way, d in self.arrivals(t):
            slot = self.slot(-way * d, 0)
            self.copy(slot, self.sp, self.zsem.at[self.key(way, d)]).wait_recv()
            self.hand_on(way, d)
            self.spread(slot, t)

    def finish(self, first, last):
        for t in range(first, last + 1):
            count = len(self.arrivals(t)) if t else 1
            take_bytes(self.ref, count * (NY - 1), self.ysem.at[t])


class PlaneYZ(Plane):
    def hand_on(self, way, d, j):
        for c in self.next_of(way, d):
            sem = self.zsem.at[self.key(way, c), j]
            self.copy(self.slot(-way * d, -j), self.slot(way * (c - d), 0), sem).start()

    def start(self):
        for d in range(1, NY):
            self.copy(self.sp, self.slot(0, d), self.ysem.at[d - 1]).start()
        self.hand_on(1, 0, 0)
        self.hand_on(-1, 0, 0)

    def begin(self):
        for j in range(1, NY):
            self.copy(self.slot(0, -j), self.sp, self.ysem.at[j - 1]).wait_recv()
            self.hand_on(1, 0, j)
            self.hand_on(-1, 0, j)

    def step(self, t):
        for way, d in self.arrivals(t):
            for j in range(NY):
                slot = self.slot(-way * d, -j)
                self.copy(slot, self.sp, self.zsem.at[self.key(way, d), j]).wait_recv()
                self.hand_on(way, d, j)


class Scan:
    def __init__(self, nz, left, gap, dext, lout, qx, into, key, cum, stb, decb, ys, yd, zb, zdb, zs, zd, ib, sems):
        self.nz = nz
        self.left, self.gap, self.dext, self.lout, self.qx, self.into = left, gap, dext, lout, qx, into
        self.key, self.cum = key, cum
        self.stb, self.decb, self.ys, self.yd = stb, decb, ys, yd
        self.zb, self.zdb, self.zs, self.zd, self.ib = zb, zdb, zs, zd, ib
        self.ys_s, self.ys_r, self.yd_s, self.yd_r, self.zs_s, self.zs_r, self.zd_s, self.zd_r, self.i_s, self.i_r = sems
        self.sp = lax.axis_index("sp")
        self.z, self.y = self.sp // NY, lax.rem(self.sp, NY)
        self.vs = HEAD // NY

    def at_y(self, d):
        return self.z * NY + self.other(d)

    def other(self, d):
        return lax.rem(self.y + d + NY, NY)

    def rows(self, ref, j):
        return ref.at[:, pl.ds(pl.multiple_of(j * self.vs, self.vs), self.vs), :]

    def prepare(self):
        toks = self.left.shape[0]
        pre = self.left[:, 256:512].astype(F32)
        key = self.gap[...] * (1.0 / (1.0 + jnp.exp(pre)))
        series = jnp.full(key.shape, 1.0 / 11.0, F32)
        for n in range(10, 0, -1):
            series = series * key + 1.0 / n
        extra = [jnp.transpose(jnp.broadcast_to(self.dext[h : h + 1, :], (HEAD, toks))) for h in range(2)]
        logf = jnp.concatenate(extra, axis=1) - series * key
        rows = lax.broadcasted_iota(jnp.int32, (toks, toks), 0)
        lower = jnp.where(rows >= lanes_of((toks, toks)), 1.0, 0.0).astype(F32)
        cum = jnp.dot(lower, logf, preferred_element_type=F32, precision=lax.Precision.HIGHEST)
        self.key[...] = key
        self.cum[...] = cum

    def states(self):
        toks = self.left.shape[0]
        for h in range(2):
            cols = slice(HEAD * h, HEAD * (h + 1))
            c, k = self.cum[:, cols], self.key[:, cols]
            v = self.left[:, 512 + HEAD * h : 512 + HEAD * (h + 1)]
            last = c[toks - 1 : toks]
            self.stb[h] = dotg(v, (k * jnp.exp(last - c)).astype(BF16), TN).astype(BF16)
            self.decb[h : h + 1, :] = jnp.exp(last)
        for d in range(1, NY):
            for c in self.ycopy(d):
                c.start()

    def inside(self):
        toks = self.left.shape[0]
        half = toks // 2
        tri = lax.broadcasted_iota(jnp.int32, (half, half), 0) >= lanes_of((half, half))
        self.qx[...] = (self.left[:, 0:256].astype(F32) * jnp.exp(self.cum[...])).astype(BF16)
        for h in range(2):
            cols = slice(HEAD * h, HEAD * (h + 1))
            c, k = self.cum[:, cols], self.key[:, cols]
            q = self.left[:, cols].astype(F32)
            v = self.left[:, 512 + HEAD * h : 512 + HEAD * (h + 1)]
            edge = c[half - 1 : half]
            outs = []
            for b in range(2):
                r = slice(half * b, half * (b + 1))
                mid = c[half * b + half // 2 - 1 : half * b + half // 2]
                qd = (q[r] * jnp.exp(c[r] - mid)).astype(BF16)
                kd = (k[r] * jnp.exp(mid - c[r])).astype(BF16)
                a = jnp.where(tri, dotg(qd, kd, NT), 0.0).astype(BF16)
                outs.append(dot(a, v[r]))
            s0 = dotg(v[:half], (k[:half] * jnp.exp(edge - c[:half])).astype(BF16), TN)
            qe = (q[half:] * jnp.exp(c[half:] - edge)).astype(BF16)
            self.lout[0:half, cols] = outs[0]
            self.lout[half:toks, cols] = outs[1] + dotg(qe, s0.astype(BF16), NT)

    def ycopy(self, d):
        mine = self.rows(self.stb, self.other(d))
        dev = {"sp": self.at_y(d)}
        return (
            remote(mine, self.ys.at[self.y], self.ys_s.at[d - 1], self.ys_r.at[d - 1], dev),
            remote(self.decb, self.yd.at[self.y], self.yd_s.at[d - 1], self.yd_r.at[d - 1], dev),
        )

    def join_y(self):
        dev = {"sp": self.sp}
        y, ys, yd = self.y, self.ys, self.yd
        for h in range(2):
            ys[y, h] = self.stb[h, pl.ds(pl.multiple_of(y * self.vs, self.vs), self.vs), :]
        yd[y] = self.decb[...]
        for d in range(1, NY):
            src = self.other(-d)
            remote(ys.at[src], ys.at[src], self.ys_s.at[d - 1], self.ys_r.at[d - 1], dev).wait_recv()
            remote(yd.at[src], yd.at[src], self.yd_s.at[d - 1], self.yd_r.at[d - 1], dev).wait_recv()
        state = [jnp.zeros((self.vs, HEAD), F32) for _ in range(2)]
        span = [jnp.ones((1, HEAD), F32) for _ in range(2)]
        for j in range(NY):
            for h in range(2):
                decay = yd[j, h : h + 1, :]
                state[h] = decay * state[h] + ys[j, h].astype(F32)
                span[h] = span[h] * decay
        for h in range(2):
            self.zb[h] = state[h].astype(BF16)
            self.zdb[h : h + 1, :] = span[h]
        for d in range(self.nz - 1, 0, -1):

            @pl.when(self.z + d < self.nz)
            def _():
                for c in self.zcopy(d):
                    c.start()

    def zcopy(self, d):
        dev = {"sp": (self.z + d) * NY + self.y}
        return (
            remote(self.zb, self.zs.at[self.z], self.zs_s.at[d - 1], self.zs_r.at[self.z], dev),
            remote(self.zdb, self.zd.at[self.z], self.zd_s.at[d - 1], self.zd_r.at[self.z], dev),
        )

    def join_z(self):
        zs, zd, ys, yd = self.zs, self.zd, self.ys, self.yd
        dev = {"sp": self.sp}

        def earlier(j, carry):
            remote(zs.at[j], zs.at[j], self.zs_s.at[0], self.zs_r.at[j], dev).wait_recv()
            remote(zd.at[j], zd.at[j], self.zd_s.at[0], self.zd_r.at[j], dev).wait_recv()
            return tuple(zd[j, h : h + 1, :] * carry[h] + zs[j, h].astype(F32) for h in range(2))

        zero = jnp.zeros((self.vs, HEAD), F32)
        state = list(lax.fori_loop(0, self.z, earlier, (zero, zero)))
        for j in range(NY):
            for h in range(2):
                self.ib[j, h] = state[h].astype(BF16)
                state[h] = yd[j, h : h + 1, :] * state[h] + ys[j, h].astype(F32)
        for d in range(1, NY):
            self.icopy(d).start()
        for h in range(2):
            spot = pl.ds(pl.multiple_of(self.y * self.vs, self.vs), self.vs)
            self.into[h, spot, :] = self.ib[self.y, h]

    def icopy(self, d):
        spot = self.rows(self.into, self.y)
        return remote(self.ib.at[self.other(d)], spot, self.i_s.at[d - 1], self.i_r.at[d - 1], {"sp": self.at_y(d)})

    def finish(self):
        for d in range(1, NY):
            spot = self.rows(self.into, self.other(-d))
            remote(spot, spot, self.i_s.at[d - 1], self.i_r.at[d - 1], {"sp": self.sp}).wait_recv()

    def drain(self):
        for d in range(1, NY):
            for c in self.ycopy(d):
                c.wait_send()
            self.icopy(d).wait_send()
        for d in range(1, self.nz):

            @pl.when(self.z + d < self.nz)
            def _():
                for c in self.zcopy(d):
                    c.wait_send()


def mixer_kernel(
    nz, nx, hid, wq, wf, wi, wqdt, wkvdt, wkrt, wku, wvu, wqn, wqrt, qg, kvg, kcos, ksin, qcos, qsin,
    gap, dext, gain, worh, woah, out,
    hall, wa, wb, wc, rall, kvin, racc, wrt, left, qn, lat, kvw, qw, wor, woa,
    lout, qx, into, key, cum, stb, decb, ys, yd, zb, zdb, zs, zd, ib,
    krope, qblk, msc, acc, obuf, sbuf, orecv, srecv, mixed, pairs, got_pair, sums, got,
    loc, hs, hr, ks, kr, qs, qr, rs, rr, was, waz, way_, wbs, wbz, wby, wcs, wcz, wcy, ls, lz, ly,
    ys_s, ys_r, yd_s, yd_r, zs_s, zs_r, zd_s, zd_r, i_s, i_r,
    o_s, o_r, s_s, s_r, kv_s, kv_r, p_s, p_r, f_s, f_r,
):
    tpn, spn = 2 * nx, nz * NY
    tp, sp = lax.axis_index("tp"), lax.axis_index("sp")
    x, core = tp // 2, lax.rem(tp, 2)
    toks, feat = hid.shape
    tt = toks // tpn
    line_h, line_k = Line(hall, hs, hr, nx), Line(kvw, ks, kr, nx)
    line_q, line_r = Line(qw, qs, qr, nx), Line(rall, rs, rr, nx)
    plane_a = PlaneYZ(wa, was, waz, way_, nz)
    plane_b = PlaneZY(wb, wbs, wbz, wby, nz)
    plane_c = PlaneZY(wc, wcs, wcz, wcy, nz)
    plane_l = PlaneZY(lat, ls, lz, ly, nz)
    sems = (ys_s, ys_r, yd_s, yd_r, zs_s, zs_r, zd_s, zd_r, i_s, i_r)
    scan = Scan(nz, left, gap, dext, lout, qx, into, key, cum, stb, decb, ys, yd, zb, zdb, zs, zd, ib, sems)

    barrier = pltpu.get_barrier_semaphore()
    greet = [{"tp": lax.rem(tp + d, tpn)} for d in range(1, tpn)]
    greet += [{"sp": plane_a.slot(0, d)} for d in range(1, NY)]
    near = [d for d in range(1, nz) if d <= 4 or d >= nz - 4]
    greet += [{"sp": plane_a.slot(d, 0)} for d in near]
    for dev in greet:
        pl.semaphore_signal(barrier, inc=1, device_id=dev, device_id_type=MESH)

    own = [
        pltpu.make_async_copy(hid, hall.at[tp], loc.at[0]),
        pltpu.make_async_copy(wf.at[:, pl.ds(0, 128)], wa.at[sp], loc.at[1]),
        pltpu.make_async_copy(wf.at[:, pl.ds(128, 128)], wb.at[sp, :, pl.ds(0, 128)], loc.at[2]),
        pltpu.make_async_copy(wi, wb.at[sp, :, pl.ds(128, 256)], loc.at[3]),
        pltpu.make_async_copy(wq, wc.at[sp], loc.at[8]),
        pltpu.make_async_copy(wku, kvw.at[tp, :, pl.ds(0, 128)], loc.at[4]),
        pltpu.make_async_copy(wvu, kvw.at[tp, :, pl.ds(128, 128)], loc.at[5]),
    ]
    late = [pltpu.make_async_copy(worh, wor, loc.at[6]), pltpu.make_async_copy(woah, woa, loc.at[7])]
    for c in own + late:
        c.start()
    wrt[0:64, :] = wqdt[...]
    wrt[64:96, :] = wkvdt[...]
    wrt[96:128, :] = wkrt[...]
    for c in own:
        c.wait()
    pl.semaphore_wait(barrier, len(greet))

    line_h.start()
    plane_a.start()
    plane_b.start()
    qw[tp, 0:128, :] = jnp.transpose(wqn[...].astype(F32)).astype(BF16)
    qw[tp, 128:192, :] = wqrt[...]
    qblk[...] = jnp.zeros(qblk.shape, BF16)
    plane_a.begin()

    def wstep(t):
        plane_b.step(t)
        plane_a.step(t)

    def kv_copy(to):
        mine = rall.at[tp, pl.ds(pl.multiple_of(to * tt, tt), tt)]
        return remote(mine, kvin.at[tp], kv_s.at[to], kv_r.at[tp], {"tp": to})

    def lora():
        line_h.finish()
        acc = None
        for i in range(tpn):
            part = dotg(hall[i], wrt[:, i * feat : (i + 1) * feat], NT)
            acc = part if acc is None else acc + part
        rall[tp] = acc.astype(BF16)
        for d in range(1, tpn):
            kv_copy(lax.rem(tp + d, tpn)).start()
        line_r.start()
        line_k.start()
        line_q.start()
        kvin[tp] = rall[tp, pl.ds(pl.multiple_of(tp * tt, tt), tt), :]
        racc[...] = acc
        mine = racc[pl.ds(pl.multiple_of(tp * tt, tt), tt), :]
        lane = lanes_of((tt, 128))
        other = jnp.where(
            lax.rem(lane, 32) < 16, pltpu.roll(mine, 128 - 16, 1), pltpu.roll(mine, 16, 1)
        )
        turned = mine * kcos[...] + other * ksin[...]
        quart = tt // 4
        lane = lanes_of((quart, 128))
        packed = jnp.zeros((quart, 128), F32)
        for g in range(4):
            rows = turned[g * quart : (g + 1) * quart]
            moved = pltpu.roll(rows, 32 * (g + 1), 1) if g < 3 else rows
            packed = jnp.where((lane >= 32 * g) & (lane < 32 * (g + 1)), moved, packed)
        lat[sp, 2 * tt : 2 * tt + quart, :] = packed.astype(BF16)

    def latents():
        for d in range(1, tpn):
            src = lax.rem(tp + d, tpn)
            remote(kvin.at[src], kvin.at[src], kv_s.at[src], kv_r.at[src], {"tp": tp}).wait_recv()
        lane = lanes_of((tt, 128))
        tiles = []
        total = jnp.zeros((tt, 128), F32)
        width = 32 * tpn
        for j in range(2):
            tile = jnp.zeros((tt, 128), F32)
            for k in range(4):
                if 4 * j + k >= tpn:
                    continue
                piece = kvin[4 * j + k].astype(F32)
                moved = pltpu.roll(piece, (32 * k - 64) % 128, 1) if k != 2 else piece
                tile = jnp.where((lane >= 32 * k) & (lane < 32 * (k + 1)), moved, tile)
            tiles.append(tile)
            total = total + tile * tile
        scale = lax.rsqrt(jnp.sum(total, axis=1, keepdims=True) / width + NORM_EPS)
        for j in range(2):
            cols = slice(128 * j, 128 * (j + 1))
            lat[sp, j * tt : (j + 1) * tt, :] = (tiles[j] * scale * kvg[:, cols]).astype(BF16)

    def queries():
        line_r.finish()
        lane = lanes_of((toks, 128))
        total = jnp.zeros((toks, 128), F32)
        for i in range(tpn):
            piece = rall[i].astype(F32)
            total = total + jnp.where(lane < 64, piece * piece, 0.0)
        width = 64 * tpn
        scale = lax.rsqrt(jnp.sum(total, axis=1, keepdims=True) / width + NORM_EPS)
        for j in range(width // 128):
            one, two = rall[2 * j].astype(F32), rall[2 * j + 1].astype(F32)
            tile = jnp.where(lane < 64, one, pltpu.roll(two, 64, 1))
            cols = slice(128 * j, 128 * (j + 1))
            qn[:, cols] = (tile * scale * qg[:, cols]).astype(BF16)

    def project(blocks, at):
        spans = spn // tpn
        acc = None
        for i in range(tpn):
            block = [w[i * spans : (i + 1) * spans, :, n : n + m].reshape(feat, m) for w, n, m in blocks]
            block = block[0] if len(block) == 1 else jnp.concatenate(block, axis=1)
            part = dot(hall[i], block)
            acc = part if acc is None else acc + part
        left[:, at : at + 256] = acc.astype(BF16)

    def step(plane, t):
        if t <= plane.steps:
            plane.step(t)

    step(plane_a, 1)
    step(plane_b, 1)
    line_h.forward()
    step(plane_a, 2)
    step(plane_b, 2)
    lora()
    step(plane_a, 3)
    latents()
    plane_l.start()
    step(plane_a, 4)
    plane_c.start()
    line_r.forward()
    plane_b.finish(0, plane_b.steps)
    project([(wa, 0, 128), (wb, 0, 128)], 256)
    project([(wb, 128, 256)], 512)
    scan.prepare()
    scan.states()
    steps = plane_l.steps
    step(plane_l, 1)
    line_k.forward()
    step(plane_c, 1)
    scan.join_y()
    step(plane_l, 2)
    queries()
    line_q.forward()
    step(plane_c, 2)
    line_k.finish()
    line_q.finish()

    per = CHUNK // tt
    deep = per // NY
    chunks = spn // per
    base2 = math.log2(math.e) / math.sqrt(NOPE + ROPE)
    own_chunk = sp // per
    z = sp // NY

    def sent(p):
        dev = {"tp": p}
        return (
            remote(obuf.at[p], orecv.at[tp], o_s.at[p], o_r.at[tp], dev),
            remote(sbuf.at[p], srecv.at[tp], s_s.at[p], s_r.at[tp], dev),
        )

    def turn(p, _):
        q = dotg(qw[p], qn[...], NT)
        for h in range(2):
            c = slice(h * toks, (h + 1) * toks)
            qblk[p, 64 * h : 64 * (h + 1), c] = q[64 * h : 64 * (h + 1)].astype(BF16)
            a, b = q[128 + 32 * h : 144 + 32 * h], q[144 + 32 * h : 160 + 32 * h]
            qblk[p, 128:144, c] = (a * qcos[...] - b * qsin[...]).astype(BF16)
            qblk[p, 144:160, c] = (a * qsin[...] + b * qcos[...]).astype(BF16)
        return 0

    quart = tt // 4

    def unpack(j):
        rows = lat[pl.ds(j * per, per), 2 * tt : 2 * tt + quart, :].astype(F32)
        lane = lanes_of(rows.shape)
        parts = [
            jnp.where(lane < 32, pltpu.roll(rows, 128 - 32 * g, 2) if g else rows, 0.0)
            for g in range(4)
        ]
        whole = jnp.stack(parts, axis=1).reshape(CHUNK, 128)
        krope[pl.ds(pl.multiple_of(j * CHUNK, CHUNK), CHUNK), :] = whole.astype(BF16)

    def chunk(p, j, opening):
        tiles = kvw.shape[1] // 128
        part = [lat[pl.ds(j * per, per), i * tt : (i + 1) * tt, :].reshape(CHUNK, 128) for i in range(tiles)]
        part = part[0] if tiles == 1 else jnp.concatenate(part, axis=1)
        kv = dot(part, kvw[p])
        turned = krope[pl.ds(pl.multiple_of(j * CHUNK, CHUNK), CHUNK), :]
        keys = jnp.concatenate([kv[:, :128].astype(BF16), turned], axis=1)
        vals = jnp.transpose(kv[:, 128:]).astype(BF16)
        vals = jnp.concatenate([vals, jnp.ones((16, CHUNK), BF16)], axis=0)
        for h in range(2):
            c = slice(h * toks, (h + 1) * toks)
            s = dot(keys, qblk[p, :, c])
            if opening:
                at = lax.broadcasted_iota(jnp.int32, (CHUNK, toks), 0)
                kpos = (j * per + at // tt) * toks + tp * tt + lax.rem(at, tt)
                ok = kpos <= sp * toks + lanes_of((CHUNK, toks))
                s = jnp.where(ok, s, NEG_BIG)
                new = jnp.max(s, axis=0, keepdims=True)
                w = jnp.where(ok, jnp.exp2((s - new) * base2), 0.0)
                acc[p, :, c] = dot(vals, w.astype(BF16))
            else:
                old = msc[p, 0:1, c]
                new = jnp.maximum(old, jnp.max(s, axis=0, keepdims=True))
                w = jnp.exp2((s - new) * base2)
                fade = jnp.exp2((old - new) * base2)
                acc[p, :, c] = acc[p, :, c] * fade + dot(vals, w.astype(BF16))
            msc[p, 0:1, c] = new

    def reach(j):
        far = None
        for i in range(deep):
            d = z - (j * deep + i)
            d = jnp.where(d <= nz // 2, d, nz - d)
            far = d if far is None else jnp.maximum(far, d)
        return far

    def each(lo, hi, todo):
        @pl.loop(0, chunks)
        def _(j):
            far = reach(j)

            @pl.when((j < own_chunk) & (far > lo) & (far <= hi))
            def _():
                todo(j)

    def opened(p, _):
        chunk(p, own_chunk, True)
        return 0

    def close(i, _):
        p = lax.rem(tp + 1 + i, tpn)
        each(middle, nz, lambda j: chunk(p, j, False))
        for h in range(2):
            c = slice(h * toks, (h + 1) * toks)
            total = acc[p, 128:129, c]
            some = total > 0.0
            safe = jnp.where(some, total, 1.0)
            obuf[p, 64 * h : 64 * (h + 1), :] = (acc[p, 64 * h : 64 * (h + 1), c] / safe).astype(BF16)
            sbuf[p, h : h + 1, :] = jnp.where(some, msc[p, 0:1, c] * base2 + jnp.log2(safe), NEG_BIG)

        @pl.when(i < tpn - 1)
        def _():
            for c in sent(p):
                c.start()

        return 0

    def early(j):
        unpack(j)

        @pl.loop(0, tpn)
        def _(p):
            chunk(p, j, False)

    lax.fori_loop(0, tpn, turn, 0)
    half = tpn // 2
    middle = plane_l.jump if steps > 1 else 0
    plane_l.finish(0, 1)
    unpack(own_chunk)
    lax.fori_loop(0, tpn, opened, 0)
    if middle:
        each(0, middle, early)
    plane_l.finish(2, steps)
    each(middle, nz, unpack)
    lax.fori_loop(0, half + 1, close, 0)
    scan.join_z()
    lax.fori_loop(half + 1, tpn, close, 0)
    orecv[tp] = obuf[tp]
    srecv[tp] = sbuf[tp]
    plane_c.finish(0, plane_c.steps)
    project([(wc, 0, 256)], 0)
    scan.inside()

    scan.finish()
    cols = []
    for h in range(2):
        c = slice(HEAD * h, HEAD * (h + 1))
        raw = lout[:, c] + dotg(qx[:, c], into[h], NT)
        norm = lax.rsqrt(jnp.mean(raw * raw, axis=1, keepdims=True) + NORM_EPS)
        cols.append((raw * norm * gain[...]).astype(BF16))
    rec = jnp.concatenate(cols, axis=1)
    for c in late:
        c.wait()
    width = wor.shape[1]
    step = got.shape[3]
    for n in range(0, width, step):
        mixed[:, n : n + step] = dot(rec, wor[:, n : n + step])

    for d in range(1, tpn):
        src = lax.rem(tp + d, tpn)
        dev = {"tp": tp}
        remote(orecv.at[src], orecv.at[src], o_s.at[src], o_r.at[src], dev).wait_recv()
        remote(srecv.at[src], srecv.at[src], s_s.at[src], s_r.at[src], dev).wait_recv()
    halves = []
    for h in range(2):
        lse = [srecv[i, h : h + 1, :] for i in range(tpn)]
        top = functools.reduce(jnp.maximum, lse)
        total = jnp.zeros((1, toks), F32)
        merged = jnp.zeros((64, toks), F32)
        for i in range(tpn):
            weight = jnp.exp2(lse[i] - top)
            total = total + weight
            merged = merged + weight * orecv[i, 64 * h : 64 * (h + 1), :].astype(F32)
        halves.append((merged / total).astype(BF16))
    att = jnp.concatenate(halves, axis=0)

    sib = x * 2 + 1 - core

    def to_sib(k):
        return remote(pairs.at[k], got_pair.at[k], p_s.at[k], p_r.at[k], {"tp": sib})

    for k in range(width // step):
        n = slice(k * step, (k + 1) * step)
        mixed[:, n] += dotg(att, woa[:, n], TN)
        for i in range(nx):
            first = pl.multiple_of((2 * i + 1 - core) * tt, tt)
            pairs[k, i] = mixed[pl.ds(first, tt), n].astype(BF16)
        to_sib(k).start()

    def mine(i, k):
        first = pl.multiple_of((2 * i + core) * tt, tt)
        return mixed[pl.ds(first, tt), k * step : (k + 1) * step] + got_pair[k, i].astype(F32)

    def final(d, k):
        to = lax.rem(x + d, nx) * 2 + core
        return remote(sums.at[k, d - 1], got.at[k, d - 1], f_s.at[k, d - 1], f_r.at[k, d - 1], {"tp": to})

    for k in range(width // step):
        to_sib(k).wait_recv()
        for d in range(1, nx):
            sums[k, d - 1] = mine(lax.rem(x + d, nx), k).astype(BF16)
            final(d, k).start()
    for k in range(width // step):
        total = mine(x, k)
        for d in range(1, nx):
            final(d, k).wait_recv()
            total = total + got[k, d - 1].astype(F32)
        out[:, k * step : (k + 1) * step] = total.astype(BF16)
    for k in range(width // step):
        to_sib(k).wait_send()
        for d in range(1, nx):
            final(d, k).wait_send()
    for d in range(1, tpn):
        for c in sent(lax.rem(tp + d, tpn)):
            c.wait_send()
        kv_copy(lax.rem(tp + d, tpn)).wait_send()
    for part in (line_h, line_k, line_q, line_r, plane_a, plane_b, plane_c, plane_l, scan):
        part.drain()


def shards(
    nz, nx,
    hidden_in, w_query_rec, w_forget, w_input, forget_gap, decay_extra, rec_gain,
    w_q_down, w_kv_down, w_key_rope, q_gain, kv_gain, w_q_nope, w_q_rope, w_k_up, w_v_up,
    w_out_rec, w_out_att,
):
    tpn, spn = 2 * nx, nz * NY
    toks, feat = hidden_in.shape
    tt = toks // tpn
    rw = w_query_rec.shape[0]
    qrank = w_q_down.shape[1] * tpn
    kvrank = w_k_up.shape[0]
    width = w_out_rec.shape[1]
    sp, tp = lax.axis_index("sp"), lax.axis_index("tp")

    frequency = 1.0 / ROPE_BASE ** (jnp.arange(0, ROPE, 2, dtype=F32) / ROPE)
    position = (sp * toks + jnp.arange(toks)).astype(F32)
    angle = frequency[:, None] * position[None, :]
    qcos, qsin = jnp.cos(angle), jnp.sin(angle)
    keyed = (sp * toks + tp * tt + jnp.arange(tt)).astype(F32)
    angle = keyed[:, None] * jnp.tile(frequency, 8)[None, :]
    sign = jnp.where(jnp.arange(128) % 32 < 16, -1.0, 1.0).astype(F32)
    kcos, ksin = jnp.cos(angle), jnp.sin(angle) * sign[None, :]
    kvg = jnp.pad(kv_gain, (0, 256 - kv_gain.shape[0]))

    vs = HEAD // NY
    step = width // SPLIT
    line = [DMA(()), DMA((2 * nx - 1,))]
    far = max(nx - 1, 1)
    scratch = [
        VM((tpn, toks, feat), BF16),
        VM((spn, rw, 128), BF16),
        VM((spn, rw, 384), BF16),
        VM((spn, rw, 256), BF16),
        VM((tpn, toks, 128), BF16),
        VM((tpn, tt, 128), BF16),
        VM((toks, 128), F32),
        VM((128, tpn * feat), BF16),
        VM((toks, 768), BF16),
        VM((toks, qrank), BF16),
        VM((spn, 2 * tt + tt // 4, 128), BF16),
        VM((tpn, kvrank, 256), BF16),
        VM((tpn, 192, qrank), BF16),
        VM(w_out_rec.shape, BF16),
        VM(w_out_att.shape, BF16),
        VM((toks, 256), F32),
        VM((toks, 256), BF16),
        VM((2, HEAD, HEAD), BF16),
        VM((toks, 256), F32),
        VM((toks, 256), F32),
        VM((2, HEAD, HEAD), BF16),
        VM((8, HEAD), F32),
        VM((NY, 2, vs, HEAD), BF16),
        VM((NY, 8, HEAD), F32),
        VM((2, vs, HEAD), BF16),
        VM((8, HEAD), F32),
        VM((nz, 2, vs, HEAD), BF16),
        VM((nz, 8, HEAD), F32),
        VM((NY, 2, vs, HEAD), BF16),
        VM((spn * tt, 128), BF16),
        VM((tpn, 256, 2 * toks), BF16),
        VM((tpn, 8, 2 * toks), F32),
        VM((tpn, 144, 2 * toks), F32),
        VM((tpn, 128, toks), BF16),
        VM((tpn, 8, toks), F32),
        VM((tpn, 128, toks), BF16),
        VM((tpn, 8, toks), F32),
        VM((toks, width), F32),
        VM((SPLIT, nx, tt, step), BF16),
        VM((SPLIT, nx, tt, step), BF16),
        VM((SPLIT, far, tt, step), BF16),
        VM((SPLIT, far, tt, step), BF16),
        DMA((9,)),
        *line, *line, *line, *line,
        DMA(()), DMA((nz - 1, NY)), DMA((NY - 1,)),
        DMA(()), DMA((nz - 1,)), DMA((nz // 4 + 1,)),
        DMA(()), DMA((nz - 1,)), DMA((nz // 4 + 1,)),
        DMA(()), DMA((nz - 1,)), DMA((nz // 4 + 1,)),
        *([DMA((NY - 1,))] * 4),
        DMA((nz - 1,)), DMA((nz,)), DMA((nz - 1,)), DMA((nz,)),
        *([DMA((NY - 1,))] * 2),
        *([DMA((tpn,))] * 6),
        *([DMA((SPLIT,))] * 2),
        *([DMA((SPLIT, far))] * 2),
    ]
    args = (
        hidden_in, w_query_rec, w_forget, w_input, w_q_down.T, w_kv_down.T, w_key_rope.T,
        w_k_up, w_v_up, w_q_nope, w_q_rope.T, q_gain[None], kvg[None], kcos, ksin, qcos, qsin,
        forget_gap[None], decay_extra.T, rec_gain[None], w_out_rec, w_out_att,
    )
    whole, anywhere = pl.BlockSpec(memory_space=VM), pl.BlockSpec(memory_space=pl.ANY)
    return pl.pallas_call(
        functools.partial(mixer_kernel, nz, nx),
        out_shape=jax.ShapeDtypeStruct((tt, width), BF16),
        in_specs=[anywhere if i in (0, 1, 2, 3, 7, 8, 20, 21) else whole for i in range(len(args))],
        out_specs=whole,
        scratch_shapes=scratch,
        compiler_params=pltpu.CompilerParams(
            collective_id=0, has_side_effects=True, vmem_limit_bytes=60 * 2**20
        ),
        name="mixer",
    )(*args)


def solution(mesh):
    placed = (
        P("sp", "tp"),
        P("sp", "tp"),
        P("sp", "tp"),
        P("sp", "tp"),
        P("tp"),
        P("sp", "tp"),
        P(),
        P(None, "tp"),
        P(None, "tp"),
        P(),
        P(),
        P(),
        P(None, "tp"),
        P(None, "tp"),
        P(None, "tp"),
        P(None, "tp"),
        P("tp", None),
        P("tp", None),
    )
    nz, nx = mesh.shape["sp"] // NY, mesh.shape["tp"] // 2
    return jax.shard_map(
        functools.partial(shards, nz, nx),
        mesh=mesh,
        in_specs=placed,
        out_specs=P(("sp", "tp"), None),
        check_vma=False,
    )
```

```python
import functools
import math

import jax
import jax.numpy as jnp
from jax import lax
from jax.experimental import pallas as pl
from jax.experimental.pallas import tpu as pltpu
from jax.sharding import PartitionSpec as P

HEAD = 128
NOPE = 64
ROPE = 32
NORM_EPS = 1e-06
ROPE_BASE = 10000.0
NEG_BIG = -1e30
NY = 4
CHUNK = 512
SPLIT = 4
MESH = pl.DeviceIdType.MESH
F32 = jnp.float32
BF16 = jnp.bfloat16
NT = (((1,), (1,)), ((), ()))
TN = (((0,), (0,)), ((), ()))
VM = pltpu.VMEM
DMA = pltpu.SemaphoreType.DMA


def dot(a, b):
    return jnp.dot(a, b, preferred_element_type=F32)


def dotg(a, b, dims):
    return lax.dot_general(a, b, dims, preferred_element_type=F32)


def remote(src, dst, ssem, rsem, dev):
    return pltpu.make_async_remote_copy(
        src_ref=src, dst_ref=dst, send_sem=ssem, recv_sem=rsem, device_id=dev, device_id_type=MESH
    )


def take_bytes(ref, count, sem):
    part = ref.at[pl.ds(0, count)]
    pltpu.make_async_copy(part, part, sem).wait()


def lanes_of(shape):
    return lax.broadcasted_iota(jnp.int32, shape, len(shape) - 1)


class Line:
    def __init__(self, ref, ssem, rsem, nx):
        self.ref, self.ssem, self.rsem, self.nx = ref, ssem, rsem, nx
        tp = lax.axis_index("tp")
        self.tp, self.core, self.x = tp, lax.rem(tp, 2), tp // 2
        self.sib = self.x * 2 + 1 - self.core

    def at_x(self, dx):
        return lax.rem(self.x + dx + self.nx, self.nx) * 2 + self.core

    def copy(self, slot, to, k):
        piece = self.ref.at[slot]
        return remote(piece, piece, self.ssem, self.rsem.at[k], {"tp": to})

    def start(self):
        for d in range(1, self.nx):
            self.copy(self.tp, self.at_x(d), d - 1).start()
        self.copy(self.tp, self.sib, self.nx - 1).start()

    def forward(self):
        for d in range(1, self.nx):
            slot = self.at_x(-d)
            self.copy(slot, self.tp, d - 1).wait_recv()
            self.copy(slot, self.sib, self.nx - 1 + d).start()

    def finish(self):
        for d in range(self.nx):
            x = lax.rem(self.x - d + self.nx, self.nx)
            self.copy(x * 2 + 1 - self.core, self.tp, self.nx - 1 + d).wait_recv()

    def drain(self):
        take_bytes(self.ref, 2 * self.nx - 1, self.ssem)


class Plane:
    def __init__(self, ref, ssem, zsem, ysem, nz):
        self.ref, self.ssem, self.zsem, self.ysem, self.nz = ref, ssem, zsem, ysem, nz
        self.sp = lax.axis_index("sp")
        self.z, self.y = self.sp // NY, lax.rem(self.sp, NY)
        self.limit = {1: nz // 2, -1: nz // 2 - 1}
        self.steps = (nz // 2 + 1) // 2

    def slot(self, dz, dy):
        z = lax.rem(self.z + dz + self.nz, self.nz)
        return z * NY + lax.rem(self.y + dy + NY, NY)

    def copy(self, slot, to, sem):
        piece = self.ref.at[slot]
        return remote(piece, piece, self.ssem, sem, {"sp": to})

    def next_of(self, way, d):
        return [c for c in (d + 2, d + 1) if d % 2 == 0 and c <= self.limit[way]]

    def key(self, way, d):
        return d - 1 if way == 1 else self.limit[1] + d - 1

    def arrivals(self, t):
        return [(w, d) for d in (2 * t - 1, 2 * t) for w in (1, -1) if d <= self.limit[w]]

    def drain(self):
        take_bytes(self.ref, self.nz * NY - 1, self.ssem)


class PlaneZY(Plane):
    def hand_on(self, way, d):
        for c in self.next_of(way, d):
            self.copy(self.slot(-way * d, 0), self.slot(way * (c - d), 0), self.zsem.at[self.key(way, c)]).start()

    def spread(self, slot):
        for d in range(1, NY):
            self.copy(slot, self.slot(0, d), self.ysem).start()

    def start(self):
        self.hand_on(1, 0)
        self.hand_on(-1, 0)
        self.spread(self.sp)

    def step(self, t):
        for way, d in self.arrivals(t):
            slot = self.slot(-way * d, 0)
            self.copy(slot, self.sp, self.zsem.at[self.key(way, d)]).wait_recv()
            self.hand_on(way, d)
            self.spread(slot)

    def finish(self):
        take_bytes(self.ref, self.nz * (NY - 1), self.ysem)


class PlaneYZ(Plane):
    def hand_on(self, way, d, j):
        for c in self.next_of(way, d):
            sem = self.zsem.at[self.key(way, c), j]
            self.copy(self.slot(-way * d, -j), self.slot(way * (c - d), 0), sem).start()

    def start(self):
        for d in range(1, NY):
            self.copy(self.sp, self.slot(0, d), self.ysem.at[d - 1]).start()
        self.hand_on(1, 0, 0)
        self.hand_on(-1, 0, 0)

    def begin(self):
        for j in range(1, NY):
            self.copy(self.slot(0, -j), self.sp, self.ysem.at[j - 1]).wait_recv()
            self.hand_on(1, 0, j)
            self.hand_on(-1, 0, j)

    def step(self, t):
        for way, d in self.arrivals(t):
            for j in range(NY):
                slot = self.slot(-way * d, -j)
                self.copy(slot, self.sp, self.zsem.at[self.key(way, d), j]).wait_recv()
                self.hand_on(way, d, j)


class Scan:
    def __init__(self, nz, left, gap, dext, lout, qx, into, key, cum, stb, decb, ys, yd, zb, zdb, zs, zd, ib, sems):
        self.nz = nz
        self.left, self.gap, self.dext, self.lout, self.qx, self.into = left, gap, dext, lout, qx, into
        self.key, self.cum = key, cum
        self.stb, self.decb, self.ys, self.yd = stb, decb, ys, yd
        self.zb, self.zdb, self.zs, self.zd, self.ib = zb, zdb, zs, zd, ib
        self.ys_s, self.ys_r, self.yd_s, self.yd_r, self.zs_s, self.zs_r, self.zd_s, self.zd_r, self.i_s, self.i_r = sems
        self.sp = lax.axis_index("sp")
        self.z, self.y = self.sp // NY, lax.rem(self.sp, NY)
        self.vs = HEAD // NY

    def at_y(self, d):
        return self.z * NY + self.other(d)

    def other(self, d):
        return lax.rem(self.y + d + NY, NY)

    def rows(self, ref, j):
        return ref.at[:, pl.ds(pl.multiple_of(j * self.vs, self.vs), self.vs), :]

    def prepare(self):
        toks = self.left.shape[0]
        pre = self.left[:, 256:512].astype(F32)
        key = self.gap[...] * (1.0 / (1.0 + jnp.exp(pre)))
        series = jnp.full(key.shape, 1.0 / 11.0, F32)
        for n in range(10, 0, -1):
            series = series * key + 1.0 / n
        extra = [jnp.transpose(jnp.broadcast_to(self.dext[h : h + 1, :], (HEAD, toks))) for h in range(2)]
        logf = jnp.concatenate(extra, axis=1) - series * key
        rows = lax.broadcasted_iota(jnp.int32, (toks, toks), 0)
        lower = jnp.where(rows >= lanes_of((toks, toks)), 1.0, 0.0).astype(F32)
        cum = jnp.dot(lower, logf, preferred_element_type=F32, precision=lax.Precision.HIGHEST)
        self.qx[...] = (self.left[:, 0:256].astype(F32) * jnp.exp(cum)).astype(BF16)
        self.key[...] = key
        self.cum[...] = cum

    def local(self):
        toks = self.left.shape[0]
        half = toks // 2
        tri = lax.broadcasted_iota(jnp.int32, (half, half), 0) >= lanes_of((half, half))
        for h in range(2):
            cols = slice(HEAD * h, HEAD * (h + 1))
            c, k = self.cum[:, cols], self.key[:, cols]
            v = self.left[:, 512 + HEAD * h : 512 + HEAD * (h + 1)]
            last = c[toks - 1 : toks]
            self.stb[h] = dotg(v, (k * jnp.exp(last - c)).astype(BF16), TN).astype(BF16)
            self.decb[h : h + 1, :] = jnp.exp(last)
        for d in range(1, NY):
            for c in self.ycopy(d):
                c.start()
        for h in range(2):
            cols = slice(HEAD * h, HEAD * (h + 1))
            c, k = self.cum[:, cols], self.key[:, cols]
            q = self.left[:, cols].astype(F32)
            v = self.left[:, 512 + HEAD * h : 512 + HEAD * (h + 1)]
            edge = c[half - 1 : half]
            outs = []
            for b in range(2):
                r = slice(half * b, half * (b + 1))
                mid = c[half * b + half // 2 - 1 : half * b + half // 2]
                qd = (q[r] * jnp.exp(c[r] - mid)).astype(BF16)
                kd = (k[r] * jnp.exp(mid - c[r])).astype(BF16)
                a = jnp.where(tri, dotg(qd, kd, NT), 0.0).astype(BF16)
                outs.append(dot(a, v[r]))
            s0 = dotg(v[:half], (k[:half] * jnp.exp(edge - c[:half])).astype(BF16), TN)
            qe = (q[half:] * jnp.exp(c[half:] - edge)).astype(BF16)
            self.lout[0:half, cols] = outs[0]
            self.lout[half:toks, cols] = outs[1] + dotg(qe, s0.astype(BF16), NT)

    def ycopy(self, d):
        mine = self.rows(self.stb, self.other(d))
        dev = {"sp": self.at_y(d)}
        return (
            remote(mine, self.ys.at[self.y], self.ys_s.at[d - 1], self.ys_r.at[d - 1], dev),
            remote(self.decb, self.yd.at[self.y], self.yd_s.at[d - 1], self.yd_r.at[d - 1], dev),
        )

    def join_y(self):
        dev = {"sp": self.sp}
        y, ys, yd = self.y, self.ys, self.yd
        for h in range(2):
            ys[y, h] = self.stb[h, pl.ds(pl.multiple_of(y * self.vs, self.vs), self.vs), :]
        yd[y] = self.decb[...]
        for d in range(1, NY):
            src = self.other(-d)
            remote(ys.at[src], ys.at[src], self.ys_s.at[d - 1], self.ys_r.at[d - 1], dev).wait_recv()
            remote(yd.at[src], yd.at[src], self.yd_s.at[d - 1], self.yd_r.at[d - 1], dev).wait_recv()
        state = [jnp.zeros((self.vs, HEAD), F32) for _ in range(2)]
        span = [jnp.ones((1, HEAD), F32) for _ in range(2)]
        for j in range(NY):
            for h in range(2):
                decay = yd[j, h : h + 1, :]
                state[h] = decay * state[h] + ys[j, h].astype(F32)
                span[h] = span[h] * decay
        for h in range(2):
            self.zb[h] = state[h].astype(BF16)
            self.zdb[h : h + 1, :] = span[h]
        for d in range(1, self.nz):

            @pl.when(self.z + d < self.nz)
            def _():
                for c in self.zcopy(d):
                    c.start()

    def zcopy(self, d):
        dev = {"sp": (self.z + d) * NY + self.y}
        return (
            remote(self.zb, self.zs.at[self.z], self.zs_s.at[d - 1], self.zs_r.at[self.z], dev),
            remote(self.zdb, self.zd.at[self.z], self.zd_s.at[d - 1], self.zd_r.at[self.z], dev),
        )

    def join_z(self):
        zs, zd, ys, yd = self.zs, self.zd, self.ys, self.yd
        dev = {"sp": self.sp}

        def earlier(j, carry):
            remote(zs.at[j], zs.at[j], self.zs_s.at[0], self.zs_r.at[j], dev).wait_recv()
            remote(zd.at[j], zd.at[j], self.zd_s.at[0], self.zd_r.at[j], dev).wait_recv()
            return tuple(zd[j, h : h + 1, :] * carry[h] + zs[j, h].astype(F32) for h in range(2))

        zero = jnp.zeros((self.vs, HEAD), F32)
        state = list(lax.fori_loop(0, self.z, earlier, (zero, zero)))
        for j in range(NY):
            for h in range(2):
                self.ib[j, h] = state[h].astype(BF16)
                state[h] = yd[j, h : h + 1, :] * state[h] + ys[j, h].astype(F32)
        for d in range(1, NY):
            self.icopy(d).start()
        for h in range(2):
            spot = pl.ds(pl.multiple_of(self.y * self.vs, self.vs), self.vs)
            self.into[h, spot, :] = self.ib[self.y, h]

    def icopy(self, d):
        spot = self.rows(self.into, self.y)
        return remote(self.ib.at[self.other(d)], spot, self.i_s.at[d - 1], self.i_r.at[d - 1], {"sp": self.at_y(d)})

    def finish(self):
        for d in range(1, NY):
            spot = self.rows(self.into, self.other(-d))
            remote(spot, spot, self.i_s.at[d - 1], self.i_r.at[d - 1], {"sp": self.sp}).wait_recv()

    def drain(self):
        for d in range(1, NY):
            for c in self.ycopy(d):
                c.wait_send()
            self.icopy(d).wait_send()
        for d in range(1, self.nz):

            @pl.when(self.z + d < self.nz)
            def _():
                for c in self.zcopy(d):
                    c.wait_send()


def mixer_kernel(
    nz, nx, hid, wq, wf, wi, wqdt, wkvdt, wkrt, wku, wvu, wqn, wqrt, qg, kvg, kcos, ksin, qcos, qsin,
    gap, dext, gain, worh, woah, out,
    hall, wa, wb, rall, kvin, racc, wrt, left, qn, lat, kvw, qw, wor, woa,
    lout, qx, into, key, cum, stb, decb, ys, yd, zb, zdb, zs, zd, ib,
    qblk, msc, acc, obuf, sbuf, orecv, srecv, mixed, pairs, got_pair, sums, got,
    loc, hs, hr, ks, kr, qs, qr, rs, rr, was, waz, way_, wbs, wbz, wby, ls, lz, ly,
    ys_s, ys_r, yd_s, yd_r, zs_s, zs_r, zd_s, zd_r, i_s, i_r,
    o_s, o_r, s_s, s_r, kv_s, kv_r, p_s, p_r, f_s, f_r,
):
    tpn, spn = 2 * nx, nz * NY
    tp, sp = lax.axis_index("tp"), lax.axis_index("sp")
    x, core = tp // 2, lax.rem(tp, 2)
    toks, feat = hid.shape
    tt = lat.shape[1]
    line_h, line_k = Line(hall, hs, hr, nx), Line(kvw, ks, kr, nx)
    line_q, line_r = Line(qw, qs, qr, nx), Line(rall, rs, rr, nx)
    plane_a = PlaneYZ(wa, was, waz, way_, nz)
    plane_b = PlaneZY(wb, wbs, wbz, wby, nz)
    plane_l = PlaneZY(lat, ls, lz, ly, nz)
    sems = (ys_s, ys_r, yd_s, yd_r, zs_s, zs_r, zd_s, zd_r, i_s, i_r)
    scan = Scan(nz, left, gap, dext, lout, qx, into, key, cum, stb, decb, ys, yd, zb, zdb, zs, zd, ib, sems)

    barrier = pltpu.get_barrier_semaphore()
    greet = [{"tp": lax.rem(tp + d, tpn)} for d in range(1, tpn)]
    greet += [{"sp": plane_a.slot(0, d)} for d in range(1, NY)]
    near = [d for d in range(1, nz) if d <= 2 or d >= nz - 2]
    greet += [{"sp": plane_a.slot(d, 0)} for d in near]
    for dev in greet:
        pl.semaphore_signal(barrier, inc=1, device_id=dev, device_id_type=MESH)

    own = [
        pltpu.make_async_copy(hid, hall.at[tp], loc.at[0]),
        pltpu.make_async_copy(wq, wa.at[sp], loc.at[1]),
        pltpu.make_async_copy(wf, wb.at[sp, :, pl.ds(0, wf.shape[1])], loc.at[2]),
        pltpu.make_async_copy(wi, wb.at[sp, :, pl.ds(wf.shape[1], wi.shape[1])], loc.at[3]),
        pltpu.make_async_copy(wku, kvw.at[tp, :, pl.ds(0, 128)], loc.at[4]),
        pltpu.make_async_copy(wvu, kvw.at[tp, :, pl.ds(128, 128)], loc.at[5]),
    ]
    late = [pltpu.make_async_copy(worh, wor, loc.at[6]), pltpu.make_async_copy(woah, woa, loc.at[7])]
    for c in own + late:
        c.start()
    wrt[0:64, :] = wqdt[...]
    wrt[64:96, :] = wkvdt[...]
    wrt[96:128, :] = wkrt[...]
    for c in own:
        c.wait()
    pl.semaphore_wait(barrier, len(greet))

    line_h.start()
    plane_a.start()
    plane_b.start()
    qw[tp, 0:128, :] = jnp.transpose(wqn[...].astype(F32)).astype(BF16)
    qw[tp, 128:192, :] = wqrt[...]
    qblk[...] = jnp.zeros(qblk.shape, BF16)
    plane_a.begin()

    def wstep(t):
        plane_b.step(t)
        plane_a.step(t)

    def kv_copy(to):
        mine = rall.at[tp, pl.ds(pl.multiple_of(to * tt, tt), tt)]
        return remote(mine, kvin.at[tp], kv_s.at[to], kv_r.at[tp], {"tp": to})

    def lora():
        line_h.finish()
        acc = None
        for i in range(tpn):
            part = dotg(hall[i], wrt[:, i * feat : (i + 1) * feat], NT)
            acc = part if acc is None else acc + part
        rall[tp] = acc.astype(BF16)
        for d in range(1, tpn):
            kv_copy(lax.rem(tp + d, tpn)).start()
        line_r.start()
        line_k.start()
        line_q.start()
        kvin[tp] = rall[tp, pl.ds(pl.multiple_of(tp * tt, tt), tt), :]
        racc[...] = acc
        mine = racc[pl.ds(pl.multiple_of(tp * tt, tt), tt), :]
        lane = lanes_of((tt, 128))
        other = jnp.where(
            lax.rem(lane, 32) < 16, pltpu.roll(mine, 128 - 16, 1), pltpu.roll(mine, 16, 1)
        )
        turned = mine * kcos[...] + other * ksin[...]
        lat[sp, :, 256:384] = jnp.where(lane < 32, pltpu.roll(turned, 32, 1), 0.0).astype(BF16)

    def latents():
        for d in range(1, tpn):
            src = lax.rem(tp + d, tpn)
            remote(kvin.at[src], kvin.at[src], kv_s.at[src], kv_r.at[src], {"tp": tp}).wait_recv()
        lane = lanes_of((tt, 128))
        tiles = []
        total = jnp.zeros((tt, 128), F32)
        width = 32 * tpn
        for j in range(2):
            tile = jnp.zeros((tt, 128), F32)
            for k in range(4):
                if 4 * j + k >= tpn:
                    continue
                piece = kvin[4 * j + k].astype(F32)
                moved = pltpu.roll(piece, (32 * k - 64) % 128, 1) if k != 2 else piece
                tile = jnp.where((lane >= 32 * k) & (lane < 32 * (k + 1)), moved, tile)
            tiles.append(tile)
            total = total + tile * tile
        scale = lax.rsqrt(jnp.sum(total, axis=1, keepdims=True) / width + NORM_EPS)
        for j in range(2):
            cols = slice(128 * j, 128 * (j + 1))
            lat[sp, :, cols] = (tiles[j] * scale * kvg[:, cols]).astype(BF16)

    def queries():
        line_r.finish()
        lane = lanes_of((toks, 128))
        total = jnp.zeros((toks, 128), F32)
        for i in range(tpn):
            piece = rall[i].astype(F32)
            total = total + jnp.where(lane < 64, piece * piece, 0.0)
        width = 64 * tpn
        scale = lax.rsqrt(jnp.sum(total, axis=1, keepdims=True) / width + NORM_EPS)
        for j in range(width // 128):
            one, two = rall[2 * j].astype(F32), rall[2 * j + 1].astype(F32)
            tile = jnp.where(lane < 64, one, pltpu.roll(two, 64, 1))
            cols = slice(128 * j, 128 * (j + 1))
            qn[:, cols] = (tile * scale * qg[:, cols]).astype(BF16)

    def project(w, cols, at):
        per = spn // tpn
        acc = None
        for i in range(tpn):
            block = w[i * per : (i + 1) * per, :, cols].reshape(feat, 256)
            part = dot(hall[i], block)
            acc = part if acc is None else acc + part
        left[:, at : at + 256] = acc.astype(BF16)

    jobs = {
        1: [line_h.forward],
        2: [lora],
        3: [latents, plane_l.start, line_r.forward],
        4: [line_k.forward, queries],
    }
    lsteps = list(range(1, plane_l.steps + 1))
    for t in range(1, max(plane_a.steps, 4) + 1):
        if t <= plane_a.steps:
            wstep(t)
        for job in jobs.get(t, []):
            job()
    if lsteps:
        plane_l.step(lsteps.pop(0))
    plane_b.finish()
    tail = [
        lambda: (project(wb, slice(0, 256), 256), project(wb, slice(256, 512), 512)),
        lambda: project(wa, slice(0, 256), 0),
        scan.prepare,
        scan.local,
        line_q.forward,
    ]
    while lsteps or tail:
        if tail:
            tail.pop(0)()
        if lsteps:
            plane_l.step(lsteps.pop(0))
    scan.join_y()
    line_k.finish()
    line_q.finish()
    plane_l.finish()

    per = CHUNK // tt
    base2 = math.log2(math.e) / math.sqrt(NOPE + ROPE)
    whole = sp // per

    def sent(p):
        dev = {"tp": p}
        return (
            remote(obuf.at[p], orecv.at[tp], o_s.at[p], o_r.at[tp], dev),
            remote(sbuf.at[p], srecv.at[tp], s_s.at[p], s_r.at[tp], dev),
        )

    def pair(i, _):
        p = lax.rem(tp + 1 + i, tpn)
        q = dotg(qw[p], qn[...], NT)
        for h in range(2):
            c = slice(h * toks, (h + 1) * toks)
            qblk[64 * h : 64 * (h + 1), c] = q[64 * h : 64 * (h + 1)].astype(BF16)
            a, b = q[128 + 32 * h : 144 + 32 * h], q[144 + 32 * h : 160 + 32 * h]
            qblk[128:144, c] = (a * qcos[...] - b * qsin[...]).astype(BF16)
            qblk[144:160, c] = (a * qsin[...] + b * qcos[...]).astype(BF16)
        msc[...] = jnp.full(msc.shape, NEG_BIG, F32)
        acc[...] = jnp.zeros(acc.shape, F32)

        def chunk(j, masked):
            part = lat[pl.ds(j * per, per)].reshape(CHUNK, 384)
            kv = dot(part[:, : kvw.shape[1]], kvw[p])
            keys = jnp.concatenate([kv[:, :128].astype(BF16), part[:, 256:]], axis=1)
            vals = jnp.transpose(kv[:, 128:]).astype(BF16)
            vals = jnp.concatenate([vals, jnp.ones((16, CHUNK), BF16)], axis=0)
            for h in range(2):
                c = slice(h * toks, (h + 1) * toks)
                s = dot(keys, qblk[:, c])
                if masked:
                    at = lax.broadcasted_iota(jnp.int32, (CHUNK, toks), 0)
                    kpos = (j * per + at // tt) * toks + tp * tt + lax.rem(at, tt)
                    ok = kpos <= sp * toks + lanes_of((CHUNK, toks))
                    s = jnp.where(ok, s, NEG_BIG)
                old = msc[0:1, c]
                new = jnp.maximum(old, jnp.max(s, axis=0, keepdims=True))
                w = jnp.exp2((s - new) * base2)
                if masked:
                    w = jnp.where(ok, w, 0.0)
                fade = jnp.exp2((old - new) * base2)
                acc[:, c] = acc[:, c] * fade + dot(vals, w.astype(BF16))
                msc[0:1, c] = new

        @pl.loop(0, whole)
        def _(j):
            chunk(j, False)

        chunk(whole, True)
        for h in range(2):
            c = slice(h * toks, (h + 1) * toks)
            total = acc[128:129, c]
            some = total > 0.0
            safe = jnp.where(some, total, 1.0)
            obuf[p, 64 * h : 64 * (h + 1), :] = (acc[64 * h : 64 * (h + 1), c] / safe).astype(BF16)
            sbuf[p, h : h + 1, :] = jnp.where(some, msc[0:1, c] * base2 + jnp.log2(safe), NEG_BIG)

        @pl.when(i < tpn - 1)
        def _():
            for c in sent(p):
                c.start()

        return 0

    lax.fori_loop(0, tpn - 2, pair, 0)
    scan.join_z()
    lax.fori_loop(tpn - 2, tpn, pair, 0)
    orecv[tp] = obuf[tp]
    srecv[tp] = sbuf[tp]

    scan.finish()
    cols = []
    for h in range(2):
        c = slice(HEAD * h, HEAD * (h + 1))
        raw = lout[:, c] + dotg(qx[:, c], into[h], NT)
        norm = lax.rsqrt(jnp.mean(raw * raw, axis=1, keepdims=True) + NORM_EPS)
        cols.append((raw * norm * gain[...]).astype(BF16))
    rec = jnp.concatenate(cols, axis=1)
    for c in late:
        c.wait()
    width = wor.shape[1]
    step = got.shape[3]
    for n in range(0, width, step):
        mixed[:, n : n + step] = dot(rec, wor[:, n : n + step])

    for d in range(1, tpn):
        src = lax.rem(tp + d, tpn)
        dev = {"tp": tp}
        remote(orecv.at[src], orecv.at[src], o_s.at[src], o_r.at[src], dev).wait_recv()
        remote(srecv.at[src], srecv.at[src], s_s.at[src], s_r.at[src], dev).wait_recv()
    halves = []
    for h in range(2):
        lse = [srecv[i, h : h + 1, :] for i in range(tpn)]
        top = functools.reduce(jnp.maximum, lse)
        total = jnp.zeros((1, toks), F32)
        merged = jnp.zeros((64, toks), F32)
        for i in range(tpn):
            weight = jnp.exp2(lse[i] - top)
            total = total + weight
            merged = merged + weight * orecv[i, 64 * h : 64 * (h + 1), :].astype(F32)
        halves.append((merged / total).astype(BF16))
    att = jnp.concatenate(halves, axis=0)

    sib = x * 2 + 1 - core

    def to_sib(k):
        return remote(pairs.at[k], got_pair.at[k], p_s.at[k], p_r.at[k], {"tp": sib})

    for k in range(width // step):
        n = slice(k * step, (k + 1) * step)
        mixed[:, n] += dotg(att, woa[:, n], TN)
        for i in range(nx):
            first = pl.multiple_of((2 * i + 1 - core) * tt, tt)
            pairs[k, i] = mixed[pl.ds(first, tt), n].astype(BF16)
        to_sib(k).start()

    def mine(i, k):
        first = pl.multiple_of((2 * i + core) * tt, tt)
        return mixed[pl.ds(first, tt), k * step : (k + 1) * step] + got_pair[k, i].astype(F32)

    def final(d, k):
        to = lax.rem(x + d, nx) * 2 + core
        return remote(sums.at[k, d - 1], got.at[k, d - 1], f_s.at[k, d - 1], f_r.at[k, d - 1], {"tp": to})

    for k in range(width // step):
        to_sib(k).wait_recv()
        for d in range(1, nx):
            sums[k, d - 1] = mine(lax.rem(x + d, nx), k).astype(BF16)
            final(d, k).start()
    for k in range(width // step):
        total = mine(x, k)
        for d in range(1, nx):
            final(d, k).wait_recv()
            total = total + got[k, d - 1].astype(F32)
        out[:, k * step : (k + 1) * step] = total.astype(BF16)
    for k in range(width // step):
        to_sib(k).wait_send()
        for d in range(1, nx):
            final(d, k).wait_send()
    for d in range(1, tpn):
        for c in sent(lax.rem(tp + d, tpn)):
            c.wait_send()
        kv_copy(lax.rem(tp + d, tpn)).wait_send()
    for part in (line_h, line_k, line_q, line_r, plane_a, plane_b, plane_l, scan):
        part.drain()


def shards(
    nz, nx,
    hidden_in, w_query_rec, w_forget, w_input, forget_gap, decay_extra, rec_gain,
    w_q_down, w_kv_down, w_key_rope, q_gain, kv_gain, w_q_nope, w_q_rope, w_k_up, w_v_up,
    w_out_rec, w_out_att,
):
    tpn, spn = 2 * nx, nz * NY
    toks, feat = hidden_in.shape
    tt = toks // tpn
    rw = w_query_rec.shape[0]
    qrank = w_q_down.shape[1] * tpn
    kvrank = w_k_up.shape[0]
    width = w_out_rec.shape[1]
    sp, tp = lax.axis_index("sp"), lax.axis_index("tp")

    frequency = 1.0 / ROPE_BASE ** (jnp.arange(0, ROPE, 2, dtype=F32) / ROPE)
    position = (sp * toks + jnp.arange(toks)).astype(F32)
    angle = frequency[:, None] * position[None, :]
    qcos, qsin = jnp.cos(angle), jnp.sin(angle)
    keyed = (sp * toks + tp * tt + jnp.arange(tt)).astype(F32)
    angle = keyed[:, None] * jnp.tile(frequency, 8)[None, :]
    sign = jnp.where(jnp.arange(128) % 32 < 16, -1.0, 1.0).astype(F32)
    kcos, ksin = jnp.cos(angle), jnp.sin(angle) * sign[None, :]
    kvg = jnp.pad(kv_gain, (0, 256 - kv_gain.shape[0]))

    vs = HEAD // NY
    step = width // SPLIT
    line = [DMA(()), DMA((2 * nx - 1,))]
    far = max(nx - 1, 1)
    scratch = [
        VM((tpn, toks, feat), BF16),
        VM((spn, rw, 256), BF16),
        VM((spn, rw, 512), BF16),
        VM((tpn, toks, 128), BF16),
        VM((tpn, tt, 128), BF16),
        VM((toks, 128), F32),
        VM((128, tpn * feat), BF16),
        VM((toks, 768), BF16),
        VM((toks, qrank), BF16),
        VM((spn, tt, 384), BF16),
        VM((tpn, kvrank, 256), BF16),
        VM((tpn, 192, qrank), BF16),
        VM(w_out_rec.shape, BF16),
        VM(w_out_att.shape, BF16),
        VM((toks, 256), F32),
        VM((toks, 256), BF16),
        VM((2, HEAD, HEAD), BF16),
        VM((toks, 256), F32),
        VM((toks, 256), F32),
        VM((2, HEAD, HEAD), BF16),
        VM((8, HEAD), F32),
        VM((NY, 2, vs, HEAD), BF16),
        VM((NY, 8, HEAD), F32),
        VM((2, vs, HEAD), BF16),
        VM((8, HEAD), F32),
        VM((nz, 2, vs, HEAD), BF16),
        VM((nz, 8, HEAD), F32),
        VM((NY, 2, vs, HEAD), BF16),
        VM((256, 2 * toks), BF16),
        VM((8, 2 * toks), F32),
        VM((144, 2 * toks), F32),
        VM((tpn, 128, toks), BF16),
        VM((tpn, 8, toks), F32),
        VM((tpn, 128, toks), BF16),
        VM((tpn, 8, toks), F32),
        VM((toks, width), F32),
        VM((SPLIT, nx, tt, step), BF16),
        VM((SPLIT, nx, tt, step), BF16),
        VM((SPLIT, far, tt, step), BF16),
        VM((SPLIT, far, tt, step), BF16),
        DMA((8,)),
        *line, *line, *line, *line,
        DMA(()), DMA((nz - 1, NY)), DMA((NY - 1,)),
        DMA(()), DMA((nz - 1,)), DMA(()),
        DMA(()), DMA((nz - 1,)), DMA(()),
        *([DMA((NY - 1,))] * 4),
        DMA((nz - 1,)), DMA((nz,)), DMA((nz - 1,)), DMA((nz,)),
        *([DMA((NY - 1,))] * 2),
        *([DMA((tpn,))] * 6),
        *([DMA((SPLIT,))] * 2),
        *([DMA((SPLIT, far))] * 2),
    ]
    args = (
        hidden_in, w_query_rec, w_forget, w_input, w_q_down.T, w_kv_down.T, w_key_rope.T,
        w_k_up, w_v_up, w_q_nope, w_q_rope.T, q_gain[None], kvg[None], kcos, ksin, qcos, qsin,
        forget_gap[None], decay_extra.T, rec_gain[None], w_out_rec, w_out_att,
    )
    whole, anywhere = pl.BlockSpec(memory_space=VM), pl.BlockSpec(memory_space=pl.ANY)
    return pl.pallas_call(
        functools.partial(mixer_kernel, nz, nx),
        out_shape=jax.ShapeDtypeStruct((tt, width), BF16),
        in_specs=[anywhere if i in (0, 1, 2, 3, 7, 8, 20, 21) else whole for i in range(len(args))],
        out_specs=whole,
        scratch_shapes=scratch,
        compiler_params=pltpu.CompilerParams(
            collective_id=0, has_side_effects=True, vmem_limit_bytes=60 * 2**20
        ),
        name="mixer",
    )(*args)


def solution(mesh):
    placed = (
        P("sp", "tp"),
        P("sp", "tp"),
        P("sp", "tp"),
        P("sp", "tp"),
        P("tp"),
        P("sp", "tp"),
        P(),
        P(None, "tp"),
        P(None, "tp"),
        P(),
        P(),
        P(),
        P(None, "tp"),
        P(None, "tp"),
        P(None, "tp"),
        P(None, "tp"),
        P("tp", None),
        P("tp", None),
    )
    nz, nx = mesh.shape["sp"] // NY, mesh.shape["tp"] // 2
    return jax.shard_map(
        functools.partial(shards, nz, nx),
        mesh=mesh,
        in_specs=placed,
        out_specs=P(("sp", "tp"), None),
        check_vma=False,
    )
```
